128 devices in a mesh: sp: 32 (over z, y, core), tp: 4 (over x).
Axes of the slice: x: 4, y: 4, z: 4, core: 2. Of those that a mesh axis runs over, the one named last changes fastest.
Arguments:
- moe_input: bfloat16 [8192, 2048], P('sp'), may hold values from -17.5 to 17.5
- cotangent: bfloat16 [8192, 2048], P('sp'), may hold values from -6 to 6
- routes: int32 [8192, 2], P('sp'), may hold values from 0 to 31, all different within a row; in each aligned block of 256 rows (0 to 255, 256 to 511, ...) at most 20 rows name the same one
- route_weights: float32 [8192, 2], P('sp'), may hold values from 0.2 to 1
- gate_weight: bfloat16 [32, 2048, 2048], P('sp', None, 'tp'), may hold values from -0.125 to 0.125
- up_weight: bfloat16 [32, 2048, 2048], P('sp', None, 'tp'), may hold values from -0.125 to 0.125
- down_weight: bfloat16 [32, 2048, 2048], P('sp', 'tp'), may hold values from -0.125 to 0.125
- out_weight: bfloat16 [2048, 2048], P(None, 'tp'), may hold values from -0.125 to 0.125
- mixer_output: bfloat16 [8192, 2048], P('sp', 'tp'), may hold values from -6 to 6
- queries: bfloat16 [8192, 2048], P('sp', 'tp'), may hold values from -6 to 6
- key_vectors: bfloat16 [8192, 2048], P('sp', 'tp'), may hold values from -0.75 to 0.75
- value_vectors: bfloat16 [8192, 2048], P('sp', 'tp'), may hold values from -6 to 6
- log_decay: float32 [8192, 32], P('sp', 'tp'), may hold values from -0.85 to 0
- block_states: bfloat16 [64, 32, 64, 64], P('sp', 'tp'), may hold values from -1.5 to 1.5
Outputs:
- grad_gate: float32 [32, 2048, 2048], P('sp', None, 'tp')
- grad_up: float32 [32, 2048, 2048], P('sp', None, 'tp')
- grad_down: float32 [32, 2048, 2048], P('sp', 'tp')
- grad_out: float32 [2048, 2048], P('sp', 'tp')
- grad_queries: bfloat16 [8192, 2048], P('sp', 'tp')
- grad_keys: bfloat16 [8192, 2048], P('sp', 'tp')
- grad_values: bfloat16 [8192, 2048], P('sp', 'tp')
The draws below stay inside these ranges and needn't reach their ends.
Inputs may be any that keep to these rules, and one draw needn't show every extreme that they name: `routes`: each row names 2 different experts. Among the rows of one device no expert is named by more than 20 rows, and in every draw some device's rows name some expert exactly 20 times.
All inputs are finite; a program needn't handle non-finite values.
Results may differ from the reference program's by a relative error of at most 0.02.
Values may be sent and summed in bfloat16 or wider, within the bound.
A program may use at most 128 MiB of HBM per device.

```python
import math
import jax
import jax.numpy as jnp
import numpy as np
from jax import lax

D = 2048
FF = 2048
HEADS = 32
HEAD_DIM = 64
EXPERTS = 32
TOP_K = 2
TOK_DEV = 256
TOKENS = 8192
CAP = 20
BLK = 128
NBLK = 64
N_SP = 32
N_TP = 4


def draw_moe_input(key, part):
    key_rows, key_values = jax.random.split(key)
    row_scale = jnp.exp(jax.random.uniform(key_rows, (TOKENS, 1), jnp.float32, jnp.log(0.25), jnp.log(3.0)))
    values = jnp.clip(jax.random.normal(key_values, (TOKENS, D), jnp.float32), -3.5, 3.5)
    return (values * row_scale).astype(jnp.bfloat16)


def draw_log_decay(key, part):
    subkeys = jax.random.split(key, 9)
    fast_edge = 0.3
    middle_edge = 0.55
    head_class = jax.random.uniform(subkeys[0], (HEADS,), jnp.float32)
    fast_rate = jax.random.uniform(subkeys[1], (HEADS,), jnp.float32, 1.0 / 50.0, 1.0 / 30.0)
    middle_rate = jnp.exp(jax.random.uniform(subkeys[8], (HEADS,), jnp.float32, jnp.log(1.0 / 2048.0), jnp.log(1.0 / 256.0)))
    chain_rate = jax.random.uniform(subkeys[2], (HEADS,), jnp.float32, 0.05, 0.15) / TOKENS
    base_rate = jnp.where(head_class < fast_edge, fast_rate, jnp.where(head_class < middle_edge, middle_rate, chain_rate))
    segment_factor = jax.random.uniform(subkeys[3], (TOKENS // TOK_DEV, 1, HEADS), jnp.float32, 1.0, 3.0)
    jitter = jax.random.uniform(subkeys[4], (TOKENS // TOK_DEV, TOK_DEV, HEADS), jnp.float32, 0.5, 1.5)
    forgetting_factor_matrix = (segment_factor * jitter).reshape(TOKENS, HEADS) * base_rate[None, :]
    primary_expert_index = jax.random.randint(subkeys[5], (HEADS,), 0, TOKENS)
    runner_expert_index = (primary_expert_index + 1 + jax.random.randint(subkeys[6], (HEADS,), 0, TOKENS - 1)) % TOKENS
    discarded_log_terms = jnp.log(jax.random.uniform(subkeys[7], (2, HEADS), jnp.float32, 0.5, 0.8))
    sequence_indices = jnp.arange(TOKENS, dtype=jnp.int32)[:, None]
    exchange_batches = jnp.where(sequence_indices == primary_expert_index[None, :], discarded_log_terms[0][None, :], 0.0)
    exchange_batches = exchange_batches + jnp.where(sequence_indices == runner_expert_index[None, :], discarded_log_terms[1][None, :], 0.0)
    return (exchange_batches - forgetting_factor_matrix).astype(jnp.float32)


def spiked(values, own_key, source, target, shards_of, factor):
    owner, partner = [(jnp.arange(values.shape[axis_at]) // (values.shape[axis_at] // shards_of)).reshape([-1 if axis == axis_at else 1 for axis in range(values.ndim)]) for axis_at in (source, target)]
    chosen = jax.random.permutation(own_key, shards_of)[partner]
    strong = (owner == chosen) | (owner == (partner + shards_of // 2) % shards_of)
    return jnp.where(strong, factor * values, values)


def level_of(rng, shape, cuts, low, top_value):
    loudness, own = 1.0, jax.random.fold_in(rng, 6)
    for position, shards_of in cuts:
        heights = jnp.exp(jax.random.uniform(jax.random.fold_in(own, position), (shards_of,), jnp.float32, low / len(cuts), top_value / len(cuts)))
        loudness = loudness * jnp.repeat(heights, shape[position] // shards_of).reshape([-1 if axis == position else 1 for axis in range(len(shape))])
    return loudness


def deal_out(own_key, own, number, rows, count, top, reach, slope):
    sequence = jax.random.permutation(own_key, count)
    packed, usual = shares(count, rows * top, reach, slope, True), shares(count, rows * top, reach, slope, False)
    places = jnp.arange(count)

    def named(lengths, offset_by):
        used = int((lengths > 0).sum())
        fixed = max(1, used // 4)
        passed = fixed + (places - fixed + offset_by * (used - fixed)) % max(1, count - fixed)
        return jnp.zeros((count,), jnp.int32).at[sequence[jnp.where(places < fixed, places, passed)]].set(jnp.asarray(lengths, jnp.int32))

    lengths = jnp.where(number % 4 == 0, named(packed, number // 4), named(usual, number - number // 4 - 1))
    mixed = jax.random.permutation(jax.random.fold_in(own, 3), count)
    donor, receiver = mixed[0:count // 2 * 2:2], mixed[1:count // 2 * 2:2]
    room = jnp.minimum(lengths[donor] - 1, reach - lengths[receiver]) // 2
    room = jnp.where((donor == sequence[0]) | (receiver == sequence[0]) | (lengths[receiver] == 0), 0, jnp.maximum(room, 0))
    passed = jax.random.randint(jax.random.fold_in(own, 4), (count // 2,), 0, 1 << 20) % (room + 1)
    lengths = lengths.at[donor].add(-passed).at[receiver].add(passed)
    members = jnp.searchsorted(jnp.cumsum(lengths), jnp.arange(rows * top), side="right").astype(jnp.int32)
    table = members.reshape(top, rows).T
    table = table[jax.random.permutation(jax.random.fold_in(own, 1), rows)]
    offset_by = jax.random.randint(jax.random.fold_in(own, 2), (rows, 1), 0, top)
    return jnp.take_along_axis(table, (jnp.arange(top)[None, :] + offset_by) % top, axis=1)


def shares(number_of, total, most, skew, full):
    portions = [(1 << 20) // math.isqrt(grade ** skew) + 1 for grade in range(1, number_of + 1)]
    largest = most if full else min(most, max(-(-total // number_of), total * portions[0] // sum(portions)))
    least = 1 if total - largest >= number_of - 1 else 0
    counts, rest = [largest] + [least] * (number_of - 1), total - largest - least * (number_of - 1)
    while rest > 0:
        free = [i for i in range(1, number_of) if counts[i] < largest] or [i for i in range(1, number_of) if counts[i] < most]
        mass, budget = sum([portions[i] for i in free]), rest
        for i in free:
            extra = min(most - counts[i], max(1, budget * portions[i] // mass), rest)
            counts[i] = counts[i] + extra
            rest = rest - extra
    return np.array(counts)


def gaussian(stream_key, shape, spread, limit, cuts=(), kind=jnp.bfloat16):
    entries = spread * jax.random.normal(stream_key, shape, jnp.float32)
    if cuts:
        entries = entries * level_of(stream_key, shape, cuts, -0.22, 0.18)
    return jnp.clip(entries, -limit, limit).astype(kind)


def noise_with(key, extent, spread, bound, cuts, heavy, held_as=jnp.bfloat16):
    values = spread * jax.random.normal(key, extent, jnp.float32)
    if cuts:
        values = values * level_of(key, extent, cuts, -0.22, 0.18)
    return jnp.clip(spiked(values, jax.random.fold_in(key, 3), *heavy), -bound, bound).astype(held_as)


def setup_inputs(seed: int = 0) -> dict:
    arg_keys = jax.random.split(jax.random.key(seed), 15)
    moe_input = draw_moe_input(jax.random.fold_in(arg_keys[14], 71), 0)
    cotangent = noise_with(arg_keys[1], (TOKENS, D), 1.0, 6.0, ((0, 32),), (0, 1, 32, 2.75))
    routes_keys = jax.random.split(jax.random.fold_in(arg_keys[2], 1), TOKENS // TOK_DEV)
    routes_turns = jax.random.permutation(jax.random.fold_in(arg_keys[2], 3), TOKENS // TOK_DEV)
    routes = jax.vmap(lambda own, number: deal_out(jax.random.fold_in(arg_keys[2], 2), own, number, TOK_DEV, EXPERTS, TOP_K, CAP, 1))(routes_keys, routes_turns).reshape((TOKENS, TOP_K))
    route_weights = jnp.clip(0.2 + 0.8 * jax.random.uniform(arg_keys[3], (TOKENS, TOP_K), jnp.float32) ** level_of(arg_keys[3], (TOKENS, TOP_K), ((0, 32),), -0.2, 0.2), 0.2, 1.0)
    gate_weight = gaussian(arg_keys[4], (EXPERTS, D, FF), D ** -0.5, 0.125, ((0, 32), (2, 4)))
    up_weight = gaussian(arg_keys[5], (EXPERTS, D, FF), D ** -0.5, 0.125, ((0, 32), (2, 4)))
    down_weight = gaussian(arg_keys[6], (EXPERTS, FF, D), FF ** -0.5, 0.125, ((0, 32), (1, 4)))
    out_weight = gaussian(arg_keys[7], (D, HEADS * HEAD_DIM), D ** -0.5, 0.125, ((1, 4),))
    mixer_output = gaussian(arg_keys[8], (TOKENS, HEADS * HEAD_DIM), 1.0, 6.0, ((0, 32), (1, 4)))
    queries = gaussian(arg_keys[9], (TOKENS, HEADS * HEAD_DIM), 1.0, 6.0, ((0, 32), (1, 4)))
    key_vectors = gaussian(arg_keys[10], (TOKENS, HEADS * HEAD_DIM), HEAD_DIM ** -0.5, 0.75, ((0, 32), (1, 4)))
    value_vectors = gaussian(arg_keys[11], (TOKENS, HEADS * HEAD_DIM), 1.0, 6.0, ((0, 32), (1, 4)))
    log_decay = draw_log_decay(jax.random.fold_in(arg_keys[14], 71), 0)
    block_states = gaussian(arg_keys[13], (NBLK, HEADS, HEAD_DIM, HEAD_DIM), 0.25, 1.5, ((0, 32), (1, 4)))
    return {"moe_input": moe_input, "cotangent": cotangent, "routes": routes, "route_weights": route_weights, "gate_weight": gate_weight, "up_weight": up_weight, "down_weight": down_weight, "out_weight": out_weight, "mixer_output": mixer_output, "queries": queries, "key_vectors": key_vectors, "value_vectors": value_vectors, "log_decay": log_decay, "block_states": block_states}


clamp_limit = 7.0
sigmoid_sharpness = 1.702


def round_keep(values):
    return lax.optimization_barrier(values.astype(jnp.bfloat16)).astype(jnp.float32)


def pair_slots(routes_blocks):
    flat_routes = routes_blocks.reshape(routes_blocks.shape[0], -1)
    onehot = (flat_routes[:, :, None] == jnp.arange(EXPERTS, dtype=jnp.int32)[None, None, :]).astype(jnp.int32)
    before = jnp.cumsum(onehot, axis=1) - onehot
    return (flat_routes * CAP + jnp.sum(before * onehot, axis=2)).astype(jnp.int32)


def expert_grads(expert_rows, expert_cotangent, w_gate, w_up, w_down):
    gate_pre = jnp.dot(expert_rows, w_gate, preferred_element_type=jnp.float32)
    up_pre = jnp.dot(expert_rows, w_up, preferred_element_type=jnp.float32)
    act_grad = jnp.dot(expert_cotangent, w_down.T, preferred_element_type=jnp.float32)
    clamped = jnp.minimum(gate_pre, clamp_limit)
    logistic = jax.nn.sigmoid(sigmoid_sharpness * clamped)
    linear = jnp.clip(up_pre, -clamp_limit, clamp_limit)
    activation = (clamped * logistic * (linear + 1.0)).astype(jnp.bfloat16)
    slope_term = logistic + sigmoid_sharpness * clamped * logistic * (1.0 - logistic)
    gate_grad = jnp.where(gate_pre < clamp_limit, act_grad * (linear + 1.0) * slope_term, 0.0).astype(jnp.bfloat16)
    up_grad = jnp.where(jnp.abs(up_pre) < clamp_limit, act_grad * clamped * logistic, 0.0).astype(jnp.bfloat16)
    group_width = w_gate.shape[1] // N_TP
    gate_split = gate_grad.astype(jnp.float32).reshape(-1, N_TP, group_width)
    up_split = up_grad.astype(jnp.float32).reshape(-1, N_TP, group_width)
    partials = jnp.einsum("rgf,dgf->grd", gate_split, w_gate.astype(jnp.float32).reshape(-1, N_TP, group_width))
    partials = partials + jnp.einsum("rgf,dgf->grd", up_split, w_up.astype(jnp.float32).reshape(-1, N_TP, group_width))
    pair_grad = jnp.sum(round_keep(partials), axis=0).astype(jnp.bfloat16)
    grad_gate = jnp.dot(expert_rows.T, gate_grad, preferred_element_type=jnp.float32)
    grad_up = jnp.dot(expert_rows.T, up_grad, preferred_element_type=jnp.float32)
    grad_down = jnp.dot(activation.T, expert_cotangent, preferred_element_type=jnp.float32)
    return pair_grad, grad_gate, grad_up, grad_down


def retention_grads(queries, key_vectors, value_vectors, grad_mix, log_decay, block_states):
    blocks = TOKENS // BLK
    block_shape = (blocks, BLK, HEADS, HEAD_DIM)
    query_blocks = queries.astype(jnp.float32).reshape(block_shape)
    key_blocks = key_vectors.astype(jnp.float32).reshape(block_shape)
    value_blocks = value_vectors.astype(jnp.float32).reshape(block_shape)
    grad_blocks = grad_mix.astype(jnp.float32).reshape(block_shape)
    states = block_states.astype(jnp.float32)
    cumulative = jnp.cumsum(log_decay.reshape(blocks, BLK, HEADS), axis=1)
    block_ends = cumulative[:, -1, :]
    to_end = jnp.exp(block_ends[:, None, :] - cumulative)
    from_start = jnp.exp(cumulative)
    per_attention_head = jnp.transpose(cumulative, (0, 2, 1))
    differences = per_attention_head[:, :, :, None] - per_attention_head[:, :, None, :]
    causal = jnp.arange(BLK, dtype=jnp.int32)[:, None] >= jnp.arange(BLK, dtype=jnp.int32)[None, :]
    decays = jnp.where(causal, jnp.exp(jnp.minimum(differences, 0.0)), 0.0)
    weighted_grad = round_keep(jnp.einsum("nthe,nshe->nhts", grad_blocks, value_blocks) * decays)
    weighted_score = round_keep(jnp.einsum("nthd,nshd->nhts", query_blocks, key_blocks) * decays)
    query_intra = jnp.einsum("nhts,nshd->nthd", weighted_grad, key_blocks)
    query_carry = jnp.einsum("nthe,nhde->nthd", grad_blocks, states) * from_start[..., None]
    grad_queries = (query_intra + query_carry).astype(jnp.bfloat16).reshape(TOKENS, HEADS * HEAD_DIM)
    scaled_queries = round_keep(query_blocks * from_start[..., None])
    outer_terms = jnp.einsum("nthd,nthe->nhde", scaled_queries, grad_blocks)
    end_factor = jnp.exp(block_ends)

    def suffix_step(state_grad, inputs):
        factor, outer_block = inputs
        return factor[:, None, None] * state_grad + outer_block, state_grad

    start_grad = jnp.zeros((HEADS, HEAD_DIM, HEAD_DIM), jnp.float32)
    _, leaving = lax.scan(suffix_step, start_grad, (end_factor, outer_terms), reverse=True)
    carried = round_keep(leaving)
    key_intra = jnp.einsum("nhts,nthd->nshd", weighted_grad, query_blocks)
    value_intra = jnp.einsum("nhts,nthe->nshe", weighted_score, grad_blocks)
    key_carry = jnp.einsum("nshe,nhde->nshd", value_blocks, carried) * to_end[..., None]
    value_carry = jnp.einsum("nshd,nhde->nshe", key_blocks, carried) * to_end[..., None]
    grad_keys = (key_intra + key_carry).astype(jnp.bfloat16).reshape(TOKENS, HEADS * HEAD_DIM)
    grad_values = (value_intra + value_carry).astype(jnp.bfloat16).reshape(TOKENS, HEADS * HEAD_DIM)
    return grad_queries, grad_keys, grad_values


def reference(moe_input, cotangent, routes, route_weights, gate_weight, up_weight, down_weight, out_weight, mixer_output, queries, key_vectors, value_vectors, log_decay, block_states):
    pair_count = TOK_DEV * TOP_K
    slot_index = pair_slots(routes.reshape(N_SP, TOK_DEV, TOP_K))
    source = jnp.arange(N_SP, dtype=jnp.int32)[:, None]
    pair_ids = (source * pair_count + jnp.arange(pair_count, dtype=jnp.int32)[None, :]).astype(jnp.int32)
    slot_pair = jnp.full((N_SP, EXPERTS * CAP), TOKENS * TOP_K, jnp.int32).at[source, slot_index].set(pair_ids)
    tables = jnp.transpose(slot_pair.reshape(N_SP, EXPERTS, CAP), (1, 0, 2)).reshape(EXPERTS, N_SP * CAP)
    zero_row = jnp.zeros((1, D), jnp.bfloat16)
    scaled = (route_weights[:, :, None] * cotangent.astype(jnp.float32)[:, None, :]).astype(jnp.bfloat16)
    scaled = jnp.concatenate([scaled.reshape(TOKENS * TOP_K, D), zero_row], axis=0)
    inputs_padded = jnp.concatenate([moe_input, zero_row], axis=0)

    def one_expert(operands):
        table, w_gate, w_up, w_down = operands
        return expert_grads(inputs_padded[table // TOP_K], scaled[table], w_gate, w_up, w_down)

    pair_rows, grad_gate, grad_up, grad_down = lax.map(one_expert, (tables, gate_weight, up_weight, down_weight))
    pair_sum = jnp.zeros((TOKENS * TOP_K + 1, D), jnp.float32).at[tables.reshape(-1)].add(pair_rows.reshape(-1, D).astype(jnp.float32))
    token_sum = jnp.sum(pair_sum[:TOKENS * TOP_K].reshape(TOKENS, TOP_K, D), axis=1)
    residual_grad = (cotangent.astype(jnp.float32) + token_sum).astype(jnp.bfloat16)
    grad_out = jnp.dot(residual_grad.T, mixer_output, preferred_element_type=jnp.float32)
    grad_mix = jnp.dot(residual_grad, out_weight, preferred_element_type=jnp.float32).astype(jnp.bfloat16)
    grad_queries, grad_keys, grad_values = retention_grads(queries, key_vectors, value_vectors, grad_mix, log_decay, block_states)
    return (grad_gate, grad_up, grad_down, grad_out, grad_queries, grad_keys, grad_values)
```

```python
import jax
import jax.numpy as jnp
from jax import lax
from jax.sharding import PartitionSpec as P
from jax.experimental import pallas as pl
from jax.experimental.pallas import tpu as pltpu

EXP_DEV = 1
TOP_K = 2
SP = "sp"


clamp_limit = 7.0
sigmoid_sharpness = 1.702


MAIN = 16
LEFT = 4
LANES = 128
BF = jnp.bfloat16
F32 = jnp.float32
MESH_ID = pl.DeviceIdType.MESH


def dot(a, b):
    return jnp.dot(a, b, preferred_element_type=F32)


def dot_t(a, b):
    return lax.dot_general(a, b, (((1,), (1,)), ((), ())), preferred_element_type=F32)


def t_dot(a, b):
    return lax.dot_general(a, b, (((0,), (0,)), ((), ())), preferred_element_type=F32)


def iota(shape, dim):
    return lax.broadcasted_iota(jnp.int32, shape, dim)


def select_groups(y, rows):
    group = (iota((rows, 1), 0) % MAIN) // LEFT
    return sum(
        jnp.where(group == g, y[:, g * LANES : (g + 1) * LANES], 0.0) for g in range(MAIN // LEFT)
    )


def prep_kernel(routes, weights, x_ref, c_ref, s_in, s_gr, pm_ref, pl_ref):
    toks = x_ref.shape[0]
    rows = s_in.shape[0]
    experts = rows // MAIN
    share = x_ref.shape[1] // lax.axis_size("tp")
    cols = pl.ds(pl.multiple_of(lax.axis_index("tp") * share, share), share)
    e = iota((experts, toks), 0)
    first = routes[0:1, :] == e
    second = routes[1:2, :] == e
    chosen = first | second
    tri = (iota((toks, toks), 0) < iota((toks, toks), 1)).astype(BF)
    rank = dot(chosen.astype(F32).astype(BF), tri)
    ranks = jnp.where(chosen, rank, -1.0).astype(BF)
    owner = (iota((rows, experts), 0) // MAIN == iota((rows, experts), 1)).astype(BF)
    spread = dot(owner, ranks).astype(jnp.int32)
    place = iota((rows, toks), 0) % MAIN
    is_main = spread == place
    is_left = spread == MAIN + place % LEFT
    w = jnp.where(first, weights[0:1, :], 0.0) + jnp.where(second, weights[1:2, :], 0.0)
    w_rows = jnp.zeros((rows, toks), F32)
    for _ in range(3):
        piece = w.astype(BF)
        w_rows = w_rows + dot(owner, piece)
        w = w - piece.astype(F32)
    w_main = jnp.sum(jnp.where(is_main, w_rows, 0.0), axis=1, keepdims=True)
    w_left = jnp.sum(jnp.where(is_left, w_rows, 0.0), axis=1, keepdims=True)
    p_main = is_main.astype(F32).astype(BF)
    p_left = is_left.astype(F32).astype(BF)
    pm_ref[...] = p_main
    pl_ref[...] = p_left
    x = x_ref[:, cols]
    c = c_ref[:, cols]
    s_in[:, :share] = dot(p_main, x).astype(BF)
    s_in[:, share:] = select_groups(dot(p_left, x), rows).astype(BF)
    s_gr[:, :share] = (w_main * dot(p_main, c)).astype(BF)
    s_gr[:, share:] = (w_left * select_groups(dot(p_left, c), rows)).astype(BF)


def prep(routes, weights, x, c, experts):
    share = x.shape[1] // lax.axis_size("tp")
    rows = experts * MAIN
    sent = jax.ShapeDtypeStruct((rows, share + LANES), BF)
    table = jax.ShapeDtypeStruct((rows, x.shape[0]), BF)
    return pl.pallas_call(
        prep_kernel,
        out_shape=(sent, sent, table, table),
        in_specs=[pl.BlockSpec(memory_space=pltpu.VMEM)] * 4,
        out_specs=[pl.BlockSpec(memory_space=pltpu.VMEM)] * 4,
        compiler_params=pltpu.CompilerParams(vmem_limit_bytes=40 << 20),
        cost_estimate=pl.CostEstimate(flops=10**9, bytes_accessed=5 << 20, transcendentals=0),
        name="prep",
    )(routes, weights, x, c)


def expert_kernel(
    s_in, s_gr, wg_h, wu_h, wd_h, pm_ref, pl_ref, cot_ref,
    x_out, c_out, gg_out, ug_out, act_out, res_out,
    recv, xs, wg, wu, wd, acc, half_out, ip, far_in, near_in, ret_t, ret_q, res,
    w_sem, a_send, a_recv, g_send, g_recv, rs_send, rs_recv, t_send, t_recv, r_send, r_recv, o_sem,
):
    n_sp, n_tp = lax.axis_size("sp"), lax.axis_size("tp")
    me, tp = lax.axis_index("sp"), lax.axis_index("tp")
    nxt, prv, far = lax.rem(tp + 1, n_tp), lax.rem(tp + n_tp - 1, n_tp), lax.rem(tp + 2, n_tp)
    share = wg.shape[0] // n_tp
    wide = share + LANES
    hidden = wg.shape[1]
    hs = n_sp // 2 * MAIN
    hx = n_sp // 2 * (MAIN + LEFT)
    hl = n_sp // 2 * LEFT

    def at(k, width):
        return pl.ds(pl.multiple_of(k * width, LANES), width)

    def slab(k):
        return pl.ds(pl.multiple_of(k * MAIN, MAIN), MAIN)

    loads = [
        pltpu.make_async_copy(src, dst, w_sem.at[i])
        for i, (src, dst) in enumerate(((wg_h, wg), (wu_h, wu), (wd_h, wd)))
    ]
    for load in loads:
        load.start()

    barrier = pltpu.get_barrier_semaphore()

    def greet(i, carry):
        pl.semaphore_signal(
            barrier, inc=1, device_id={"sp": lax.rem(me + i, n_sp)}, device_id_type=MESH_ID
        )
        return carry

    lax.fori_loop(1, n_sp, greet, 0)
    for k in (nxt, prv):
        pl.semaphore_signal(barrier, inc=1, device_id={"tp": k}, device_id_type=MESH_ID)
    pl.semaphore_wait(barrier, n_sp + 1)

    for a, src in ((0, s_in), (1, s_gr)):
        landing = recv.at[a, slab(me), at(tp, wide)]
        pltpu.make_async_copy(src.at[slab(me), :], landing, a_recv.at[a, me // (n_sp // 2)]).start()

        def deliver(i, carry):
            e = lax.rem(me + i, n_sp)
            pltpu.make_async_remote_copy(
                src_ref=src.at[slab(e), :],
                dst_ref=landing,
                send_sem=a_send.at[a],
                recv_sem=a_recv.at[a, me // (n_sp // 2)],
                device_id={"sp": e},
                device_id_type=MESH_ID,
            ).start()
            return carry

        lax.fori_loop(1, n_sp, deliver, 0)

    def tp_copy(ref, dst, sends, recvs, i, k):
        return pltpu.make_async_remote_copy(
            src_ref=ref, dst_ref=dst, send_sem=sends.at[i], recv_sem=recvs.at[i],
            device_id={"tp": k}, device_id_type=MESH_ID,
        )

    def ring_copies(view, sends, recvs):
        def move(h, k, i, to):
            return tp_copy(view(h, k), view(h, k), sends, recvs, i, to)

        return [
            move(0, tp, 0, nxt), move(1, tp, 1, nxt), move(0, tp, 2, prv), move(1, tp, 3, prv),
            move(0, prv, 4, nxt), move(1, nxt, 5, prv),
        ]

    jj = iota((hs, hs), 0)
    qq = iota((hs, hs), 1)
    unpick = (
        qq == ((jj % hl) // LEFT) * MAIN + (jj // hl) * LEFT + jj % LEFT
    ).astype(F32).astype(BF)
    pick = (
        qq == ((jj % MAIN) // LEFT) * hl + (jj // MAIN) * LEFT + jj % LEFT
    ).astype(F32).astype(BF)
    groups = MAIN // LEFT

    def unpack(a, k):
        for h in range(2):
            rows = pl.ds(h * hs, hs)
            xs[a, h * hx : h * hx + hs, at(k, share)] = recv[a, rows, pl.ds(pl.multiple_of(k * wide, LANES), share)]
            tail = recv[a, rows, pl.ds(pl.multiple_of(k * wide + share, LANES), LANES)]
            spread = dot(unpick, tail).astype(BF)
            left = jnp.concatenate([spread[g * hl : (g + 1) * hl] for g in range(groups)], axis=1)
            xs[a, h * hx + hs : (h + 1) * hx, at(k, share)] = left

    def piece_in(k, fresh):
        unpack(0, k)

        @pl.loop(0, 2)
        def _(h):
            rows = pl.ds(pl.multiple_of(h * hx, MAIN), hx)
            x = xs[0, rows, at(k, share)]
            g = dot(x, wg[at(k, share), :])
            u = dot(x, wu[at(k, share), :])
            if fresh:
                acc[0, rows, :] = g
                acc[1, rows, :] = u
            else:
                acc[0, rows, :] += g
                acc[1, rows, :] += u

    def piece_gr(k, fresh):
        unpack(1, k)

        @pl.loop(0, 2)
        def _(h):
            rows = pl.ds(pl.multiple_of(h * hx, MAIN), hx)
            d = dot_t(xs[1, rows, at(k, share)], wd[:, at(k, share)])
            if fresh:
                acc[2, rows, :] = d
            else:
                acc[2, rows, :] += d

    rings = [
        ring_copies(
            lambda h, k, a=a: recv.at[a, pl.ds(h * hs, hs), at(k, wide)],
            g_send.at[a], g_recv.at[a],
        )
        for a in range(2)
    ]

    def wait_arrivals(a, h):
        ref = recv.at[a, pl.ds(h * hs, hs), at(tp, wide)]
        pltpu.make_async_copy(ref, ref, a_recv.at[a, h]).wait()

    def ring_begin(ring, ready):
        ready(0)
        ring[0].start()
        ring[2].start()
        ready(1)
        ring[3].start()
        ring[1].start()

    def ring_relay(ring):
        ring[0].wait_recv()
        ring[4].start()
        ring[3].wait_recv()
        ring[5].start()

    ring_begin(rings[0], lambda h: wait_arrivals(0, h))
    loads[0].wait()
    loads[1].wait()
    piece_in(tp, True)
    ring_relay(rings[0])
    ring_begin(rings[1], lambda h: wait_arrivals(1, h))
    rings[0][1].wait_recv()
    piece_in(prv, False)
    rings[0][2].wait_recv()
    piece_in(nxt, False)
    loads[2].wait()
    piece_gr(tp, True)
    rings[0][4].wait_recv()
    rings[0][5].wait_recv()
    piece_in(far, False)
    x_copy = pltpu.make_async_copy(xs.at[0], x_out, o_sem.at[0])
    x_copy.start()

    step = 2 * MAIN

    @pl.loop(0, 2 * hx // step)
    def _(i):
        rows = pl.ds(pl.multiple_of(i * step, step), step)
        gate, up = acc[0, rows, :], acc[1, rows, :]
        clamped = jnp.minimum(gate, clamp_limit)
        logistic = 1.0 / (1.0 + jnp.exp(-sigmoid_sharpness * clamped))
        linear = jnp.clip(up, -clamp_limit, clamp_limit) + 1.0
        swish = clamped * logistic
        half_out[2, rows, :] = (swish * linear).astype(BF)
        slope = logistic + sigmoid_sharpness * swish * (1.0 - logistic)
        acc[0, rows, :] = jnp.where(gate < clamp_limit, linear * slope, 0.0)
        acc[1, rows, :] = jnp.where(jnp.abs(up) < clamp_limit, swish, 0.0)

    act_copy = pltpu.make_async_copy(half_out.at[2], act_out, o_sem.at[1])
    act_copy.start()

    ring_relay(rings[1])
    rings[1][1].wait_recv()
    piece_gr(prv, False)
    rings[1][2].wait_recv()
    piece_gr(nxt, False)
    rings[1][4].wait_recv()
    rings[1][5].wait_recv()
    piece_gr(far, False)
    c_copy = pltpu.make_async_copy(xs.at[1], c_out, o_sem.at[2])
    c_copy.start()

    @pl.loop(0, 2 * hx // step)
    def _(i):
        rows = pl.ds(pl.multiple_of(i * step, step), step)
        act_grad = acc[2, rows, :]
        half_out[0, rows, :] = (act_grad * acc[0, rows, :]).astype(BF)
        half_out[1, rows, :] = (act_grad * acc[1, rows, :]).astype(BF)

    gg_copy = pltpu.make_async_copy(half_out.at[0], gg_out, o_sem.at[3])
    ug_copy = pltpu.make_async_copy(half_out.at[1], ug_out, o_sem.at[4])
    gg_copy.start()
    ug_copy.start()

    def part(k, slot):
        @pl.loop(0, 2)
        def _(h):
            rows = pl.ds(pl.multiple_of(h * hx, MAIN), hx)
            y = dot_t(half_out[0, rows, :], wg[at(k, share), :])
            y = y + dot_t(half_out[1, rows, :], wu[at(k, share), :])
            ip[slot, rows, :] = y.astype(BF)

    halves = [pl.ds(0, hx), pl.ds(hx, hx)]

    def rs_copy(src, dst, i, k):
        return tp_copy(src, dst, rs_send, rs_recv, i, k)

    rs = [
        rs_copy(ip.at[0, halves[0]], far_in.at[0], 0, nxt),
        rs_copy(ip.at[0, halves[1]], far_in.at[1], 1, prv),
        rs_copy(ip.at[1, halves[1]], near_in.at[0, halves[1]], 2, nxt),
        rs_copy(ip.at[2, halves[0]], near_in.at[1, halves[0]], 3, prv),
        rs_copy(ip.at[1, halves[0]], near_in.at[0, halves[0]], 4, nxt),
        rs_copy(ip.at[2, halves[1]], near_in.at[1, halves[1]], 5, prv),
    ]
    part(far, 0)
    rs[0].start()
    rs[1].start()
    part(nxt, 1)
    rs[2].start()
    part(prv, 2)
    rs[3].start()
    rs[0].wait_recv()
    ip[1, halves[0], :] = (ip[1, halves[0], :].astype(F32) + far_in[0].astype(F32)).astype(BF)
    rs[4].start()
    rs[1].wait_recv()
    ip[2, halves[1], :] = (ip[2, halves[1], :].astype(F32) + far_in[1].astype(F32)).astype(BF)
    rs[5].start()
    part(tp, 3)

    for h in range(2):
        rs[(4, 2)[h]].wait_recv()
        rs[(3, 5)[h]].wait_recv()
        total = (
            ip[3, halves[h], :].astype(F32)
            + near_in[0, halves[h], :].astype(F32)
            + near_in[1, halves[h], :].astype(F32)
        ).astype(BF)
        ret_t[h * hs : (h + 1) * hs, :share] = total[:hs]
        stacked = jnp.concatenate(
            [total[hs:, g * LANES : (g + 1) * LANES] for g in range(groups)], axis=0
        )
        ret_t[h * hs : (h + 1) * hs, share:] = dot(pick, stacked).astype(BF)

        def give_back(i, carry):
            s = h * (n_sp // 2) + lax.rem(me + i, n_sp // 2)

            @pl.when(s != me)
            def _():
                pltpu.make_async_remote_copy(
                    src_ref=ret_t.at[slab(s), :],
                    dst_ref=ret_q.at[slab(me), :],
                    send_sem=t_send.at[0],
                    recv_sem=t_recv.at[0],
                    device_id={"sp": s},
                    device_id_type=MESH_ID,
                ).start()

            return carry

        lax.fori_loop(0, n_sp // 2, give_back, 0)
    ret_q[slab(me), :] = ret_t[slab(me), :]
    others = pl.ds(0, (n_sp - 1) * MAIN)
    pltpu.make_async_copy(ret_q.at[others, :], ret_q.at[others, :], t_recv.at[0]).wait()

    p_left = pl_ref[...]
    y = t_dot(pm_ref[...], ret_q[:, :share])
    tails = ret_q[:, share:]
    group = (iota(p_left.shape, 0) % MAIN) // LEFT
    y = y + jnp.concatenate(
        [t_dot(jnp.where(group == g, p_left, jnp.zeros_like(p_left)), tails) for g in range(groups)],
        axis=1,
    )
    res[:, at(tp, share)] = (cot_ref[:, at(tp, share)].astype(F32) + y).astype(BF)
    toks = res.shape[0]
    ring = ring_copies(
        lambda h, k: res.at[pl.ds(h * (toks // 2), toks // 2), at(k, share)], r_send, r_recv
    )
    ring_begin(ring, lambda h: None)
    ring_relay(ring)
    for i in (1, 2, 4, 5):
        ring[i].wait_recv()
    res_out[...] = res[...]

    for a in range(2):
        ref = recv.at[a, others, at(tp, wide)]
        pltpu.make_async_copy(ref, ref, a_send.at[a]).wait()
        for copy in rings[a]:
            copy.wait_send()
    for copy in rs + ring:
        copy.wait_send()
    pltpu.make_async_copy(ret_q.at[others, :], ret_q.at[others, :], t_send.at[0]).wait()
    for copy in (x_copy, act_copy, c_copy, gg_copy, ug_copy):
        copy.wait()


def expert_call(s_in, s_gr, w_gate, w_up, w_down, p_main, p_left, cotangent):
    n_sp, n_tp = lax.axis_size("sp"), lax.axis_size("tp")
    width, hidden = w_gate.shape
    rows, wide = s_in.shape
    share = width // n_tp
    full = n_sp * (MAIN + LEFT)
    toks = cotangent.shape[0]
    anyspace = pl.BlockSpec(memory_space=pl.ANY)
    vmem = pl.BlockSpec(memory_space=pltpu.VMEM)
    dma = pltpu.SemaphoreType.DMA
    return pl.pallas_call(
        expert_kernel,
        out_shape=(
            jax.ShapeDtypeStruct((full, width), BF),
            jax.ShapeDtypeStruct((full, width), BF),
            jax.ShapeDtypeStruct((full, hidden), BF),
            jax.ShapeDtypeStruct((full, hidden), BF),
            jax.ShapeDtypeStruct((full, hidden), BF),
            jax.ShapeDtypeStruct((toks, width), BF),
        ),
        in_specs=[anyspace] * 5 + [vmem] * 3,
        out_specs=[anyspace] * 5 + [vmem],
        scratch_shapes=[
            pltpu.VMEM((2, rows, n_tp * wide), BF),
            pltpu.VMEM((2, full, width), BF),
            pltpu.VMEM(w_gate.shape, BF),
            pltpu.VMEM(w_up.shape, BF),
            pltpu.VMEM(w_down.shape, BF),
            pltpu.VMEM((3, full, hidden), F32),
            pltpu.VMEM((3, full, hidden), BF),
            pltpu.VMEM((4, full, share), BF),
            pltpu.VMEM((2, full // 2, share), BF),
            pltpu.VMEM((2, full, share), BF),
            pltpu.VMEM((rows, wide), BF),
            pltpu.VMEM((rows, wide), BF),
            pltpu.VMEM((toks, width), BF),
            dma((3,)), dma((2,)), dma((2, 2)), dma((2, 6)), dma((2, 6)),
            dma((6,)), dma((6,)), dma((1,)), dma((1,)), dma((6,)), dma((6,)), dma((5,)),
        ],
        compiler_params=pltpu.CompilerParams(
            collective_id=0, has_side_effects=True, vmem_limit_bytes=60 << 20
        ),
        cost_estimate=pl.CostEstimate(flops=10**10, bytes_accessed=20 << 20, transcendentals=0),
        name="experts",
    )(s_in, s_gr, w_gate, w_up, w_down, p_main, p_left, cotangent)


def nothing_yet(x, identity):
    return jax.tree.map(
        lambda part, zero: jnp.zeros_like(part) + jnp.asarray(zero, part.dtype), x, identity
    )


def entering(x, axes, combine, identity):
    before = start = nothing_yet(x, identity)
    subtotal = x
    for axis in reversed(axes):
        peers, place = (lax.axis_size(axis), lax.axis_index(axis))
        pieces = jax.tree.map(
            lambda part, kind: lax.all_gather(part.astype(kind), axis),
            subtotal,
            (jnp.bfloat16, jnp.bfloat16),
        )
        inside, subtotal = (start, start)
        for k in reversed(range(peers)):
            passed = k > place
            subtotal = combine(
                subtotal, jax.tree.map(lambda part, own: part[k].astype(own.dtype), pieces, x)
            )
            inside = jax.tree.map(lambda new, old: jnp.where(passed, new, old), subtotal, inside)
        before = combine(inside, before)
    return before


def contract_rows(left, right):
    return lax.dot_general(
        left, right, (((0,), (0,)), ((), ())), preferred_element_type=jnp.float32
    )


def combine_suffix(earlier, later):
    return (earlier[0] * later[0], later[0][:, None, None] * earlier[1] + later[1])


def retention_grads(queries, key_vectors, value_vectors, grad_mix, log_decay, block_states):
    tok_dev = queries.shape[0]
    heads_local = log_decay.shape[1]
    head_dim = queries.shape[1] // heads_local
    blocks = block_states.shape[0]
    block_rows = tok_dev // blocks
    block_shape = (blocks, block_rows, heads_local, head_dim)
    query_blocks = queries.reshape(block_shape)
    key_blocks = key_vectors.reshape(block_shape)
    value_blocks = value_vectors.reshape(block_shape)
    grad_blocks = grad_mix.reshape(block_shape)
    cumulative = jnp.cumsum(log_decay.reshape(blocks, block_rows, heads_local), axis=1)
    block_ends = cumulative[:, -1, :]
    to_end = jnp.exp(block_ends[:, None, :] - cumulative)
    from_start = jnp.exp(cumulative)
    per_attention_head = jnp.transpose(cumulative, (0, 2, 1))
    differences = per_attention_head[:, :, :, None] - per_attention_head[:, :, None, :]
    causal = (
        jnp.arange(block_rows, dtype=jnp.int32)[:, None]
        >= jnp.arange(block_rows, dtype=jnp.int32)[None, :]
    )
    decays = jnp.where(causal, jnp.exp(jnp.minimum(differences, 0.0)), 0.0)
    grad_dot = jnp.einsum(
        "nthe,nshe->nhts", grad_blocks, value_blocks, preferred_element_type=jnp.float32
    )
    weighted_grad = (grad_dot * decays).astype(jnp.bfloat16)
    score_dot = jnp.einsum(
        "nthd,nshd->nhts", query_blocks, key_blocks, preferred_element_type=jnp.float32
    )
    weighted_score = (score_dot * decays).astype(jnp.bfloat16)
    scaled_queries = (query_blocks * from_start[..., None]).astype(jnp.bfloat16)
    outer_terms = jnp.einsum(
        "nthd,nthe->nhde", scaled_queries, grad_blocks, preferred_element_type=jnp.float32
    )
    end_factor = jnp.exp(block_ends)
    local_total = jnp.zeros((heads_local, head_dim, head_dim), jnp.float32)
    for block_id in reversed(range(blocks)):
        local_total = end_factor[block_id][:, None, None] * local_total + outer_terms[block_id]
    device_factor = jnp.exp(jnp.sum(block_ends, axis=0))
    identity = (
        jnp.ones((heads_local,), jnp.float32),
        jnp.zeros((heads_local, head_dim, head_dim), jnp.float32),
    )
    suffix = entering((device_factor, local_total), ("sp",), combine_suffix, identity)
    query_intra = jnp.einsum(
        "nhts,nshd->nthd", weighted_grad, key_blocks, preferred_element_type=jnp.float32
    )
    query_carry = jnp.einsum(
        "nthe,nhde->nthd", grad_blocks, block_states, preferred_element_type=jnp.float32
    )
    grad_queries = (
        (query_intra + query_carry * from_start[..., None])
        .astype(jnp.bfloat16)
        .reshape(tok_dev, -1)
    )
    key_intra = jnp.einsum(
        "nhts,nthd->nshd", weighted_grad, query_blocks, preferred_element_type=jnp.float32
    )
    value_intra = jnp.einsum(
        "nhts,nthe->nshe", weighted_score, grad_blocks, preferred_element_type=jnp.float32
    )
    state_grad = suffix[1]
    leaving = []
    for block_id in reversed(range(blocks)):
        leaving.append(state_grad)
        state_grad = end_factor[block_id][:, None, None] * state_grad + outer_terms[block_id]
    carried = jnp.stack(leaving[::-1], axis=0).astype(jnp.bfloat16)
    key_carry = jnp.einsum(
        "nshe,nhde->nshd", value_blocks, carried, preferred_element_type=jnp.float32
    )
    value_carry = jnp.einsum(
        "nshd,nhde->nshe", key_blocks, carried, preferred_element_type=jnp.float32
    )
    grad_keys = (
        (key_intra + key_carry * to_end[..., None]).astype(jnp.bfloat16).reshape(tok_dev, -1)
    )
    grad_values = (
        (value_intra + value_carry * to_end[..., None]).astype(jnp.bfloat16).reshape(tok_dev, -1)
    )
    return (grad_queries, grad_keys, grad_values)


def shards(
    moe_input,
    cotangent,
    routes,
    route_weights,
    gate_weight,
    up_weight,
    down_weight,
    out_weight,
    mixer_output,
    queries,
    key_vectors,
    value_vectors,
    log_decay,
    block_states,
):
    experts_total = EXP_DEV * lax.axis_size("sp")
    s_in, s_gr, p_main, p_left = prep(
        routes.T, route_weights.T, moe_input, cotangent, experts_total
    )
    rows, row_grads, gate_grad, up_grad, activation, residual_grad = expert_call(
        s_in, s_gr, gate_weight[0], up_weight[0], down_weight[0], p_main, p_left, cotangent
    )
    grad_gate = contract_rows(rows, gate_grad)[None]
    grad_up = contract_rows(rows, up_grad)[None]
    grad_down = contract_rows(activation, row_grads)[None]
    grad_out = lax.psum_scatter(
        contract_rows(residual_grad, mixer_output).astype(jnp.bfloat16),
        SP,
        scatter_dimension=0,
        tiled=True,
    ).astype(jnp.float32)
    grad_mix = jnp.dot(residual_grad, out_weight, preferred_element_type=jnp.float32).astype(
        jnp.bfloat16
    )
    grad_queries, grad_keys, grad_values = retention_grads(
        queries, key_vectors, value_vectors, grad_mix, log_decay, block_states
    )
    return (grad_gate, grad_up, grad_down, grad_out, grad_queries, grad_keys, grad_values)


def solution(mesh):
    return jax.shard_map(
        shards,
        mesh=mesh,
        in_specs=(
            P(SP, None),
            P(SP, None),
            P(SP, None),
            P(SP, None),
            P(SP, None, "tp"),
            P(SP, None, "tp"),
            P(SP, "tp", None),
            P(None, "tp"),
            P(SP, "tp"),
            P(SP, "tp"),
            P(SP, "tp"),
            P(SP, "tp"),
            P(SP, "tp"),
            P(SP, "tp", None, None),
        ),
        out_specs=(
            P(SP, None, "tp"),
            P(SP, None, "tp"),
            P(SP, "tp", None),
            P(SP, "tp"),
            P(SP, "tp"),
            P(SP, "tp"),
            P(SP, "tp"),
        ),
        check_vma=False,
    )
```

```python
import jax
import jax.numpy as jnp
from jax import lax
from jax.sharding import PartitionSpec as P
from jax.experimental import pallas as pl
from jax.experimental.pallas import tpu as pltpu

SP = "sp"


clamp_limit = 7.0
sigmoid_sharpness = 1.702


MAIN = 16
LEFT = 4
LANES = 128
BF = jnp.bfloat16
F32 = jnp.float32
MESH_ID = pl.DeviceIdType.MESH


def dot(a, b):
    return jnp.dot(a, b, preferred_element_type=F32)


def dot_t(a, b):
    return lax.dot_general(a, b, (((1,), (1,)), ((), ())), preferred_element_type=F32)


def t_dot(a, b):
    return lax.dot_general(a, b, (((0,), (0,)), ((), ())), preferred_element_type=F32)


def iota(shape, dim):
    return lax.broadcasted_iota(jnp.int32, shape, dim)


def select_groups(y, rows):
    group = (iota((rows, 1), 0) % MAIN) // LEFT
    return sum(
        jnp.where(group == g, y[:, g * LANES : (g + 1) * LANES], 0.0) for g in range(MAIN // LEFT)
    )


def prep_kernel(routes, weights, x_ref, c_ref, s_in, s_gr, pm_ref, pl_ref):
    toks = x_ref.shape[0]
    rows = s_in.shape[0]
    experts = rows // MAIN
    share = x_ref.shape[1] // lax.axis_size("tp")
    cols = pl.ds(pl.multiple_of(lax.axis_index("tp") * share, share), share)
    e = iota((experts, toks), 0)
    first = routes[0:1, :] == e
    second = routes[1:2, :] == e
    chosen = first | second
    tri = (iota((toks, toks), 0) < iota((toks, toks), 1)).astype(BF)
    rank = dot(chosen.astype(F32).astype(BF), tri)
    ranks = jnp.where(chosen, rank, -1.0).astype(BF)
    owner = (iota((rows, experts), 0) // MAIN == iota((rows, experts), 1)).astype(BF)
    spread = dot(owner, ranks).astype(jnp.int32)
    place = iota((rows, toks), 0) % MAIN
    is_main = spread == place
    is_left = spread == MAIN + place % LEFT
    w = jnp.where(first, weights[0:1, :], 0.0) + jnp.where(second, weights[1:2, :], 0.0)
    w_rows = jnp.zeros((rows, toks), F32)
    for _ in range(3):
        piece = w.astype(BF)
        w_rows = w_rows + dot(owner, piece)
        w = w - piece.astype(F32)
    w_main = jnp.sum(jnp.where(is_main, w_rows, 0.0), axis=1, keepdims=True)
    w_left = jnp.sum(jnp.where(is_left, w_rows, 0.0), axis=1, keepdims=True)
    p_main = is_main.astype(F32).astype(BF)
    p_left = is_left.astype(F32).astype(BF)
    pm_ref[...] = p_main
    pl_ref[...] = p_left
    x = x_ref[:, cols]
    c = c_ref[:, cols]
    s_in[:, :share] = dot(p_main, x).astype(BF)
    s_in[:, share:] = select_groups(dot(p_left, x), rows).astype(BF)
    s_gr[:, :share] = (w_main * dot(p_main, c)).astype(BF)
    s_gr[:, share:] = (w_left * select_groups(dot(p_left, c), rows)).astype(BF)


def prep(routes, weights, x, c, experts):
    share = x.shape[1] // lax.axis_size("tp")
    rows = experts * MAIN
    sent = jax.ShapeDtypeStruct((rows, share + LANES), BF)
    table = jax.ShapeDtypeStruct((rows, x.shape[0]), BF)
    return pl.pallas_call(
        prep_kernel,
        out_shape=(sent, sent, table, table),
        in_specs=[pl.BlockSpec(memory_space=pltpu.VMEM)] * 4,
        out_specs=[pl.BlockSpec(memory_space=pltpu.VMEM)] * 4,
        compiler_params=pltpu.CompilerParams(vmem_limit_bytes=40 << 20),
        cost_estimate=pl.CostEstimate(flops=10**9, bytes_accessed=5 << 20, transcendentals=0),
        name="prep",
    )(routes, weights, x, c)


def expert_kernel(
    s_in, s_gr, wg_h, wu_h, wd_h, ow_h, mix_h, q_h, k_h, v_h, pm_ref, pl_ref, cot_ref,
    ld_ref, st_ref,
    x_out, c_out, gg_out, ug_out, act_out, go_out, gq_out, gk_out, gv_out,
    recv, xs, wg, wu, wd, acc, half_out, ip, far_in, near_in, ret_t, ret_q, res,
    w_sem, a_send, a_recv, g_send, g_recv, rs_send, rs_recv, t_send, t_recv, r_send, r_recv, o_sem,
    ow, mix, qkv, cum, cum_t, decay, score, logs, gm, gmb, outer, local, part, peer, got,
    ybuf, zbuf, lt_send, lt_recv, d_send, d_recv, b_send, b_recv, sc_send, sc_recv,
    sy_send, sy_recv, sz_send, sz_recv, cbuf,
):
    n_sp, n_tp = lax.axis_size("sp"), lax.axis_size("tp")
    me, tp = lax.axis_index("sp"), lax.axis_index("tp")
    nxt, prv, far = lax.rem(tp + 1, n_tp), lax.rem(tp + n_tp - 1, n_tp), lax.rem(tp + 2, n_tp)
    share = wg.shape[0] // n_tp
    wide = share + LANES
    hidden = wg.shape[1]
    hs = n_sp // 2 * MAIN
    hx = n_sp // 2 * (MAIN + LEFT)
    hl = n_sp // 2 * LEFT

    def at(k, width):
        return pl.ds(pl.multiple_of(k * width, LANES), width)

    def slab(k):
        return pl.ds(pl.multiple_of(k * MAIN, MAIN), MAIN)

    loads = [
        pltpu.make_async_copy(src, dst, w_sem.at[i])
        for i, (src, dst) in enumerate(
            ((wg_h, wg), (wu_h, wu), (wd_h, wd), (ow_h, ow), (mix_h, mix))
            + tuple((src, qkv.at[j]) for j, src in enumerate((q_h, k_h, v_h)))
        )
    ]
    for load in loads:
        load.start()

    barrier = pltpu.get_barrier_semaphore()

    def greet(i, carry):
        pl.semaphore_signal(
            barrier, inc=1, device_id={"sp": lax.rem(me + i, n_sp)}, device_id_type=MESH_ID
        )
        return carry

    lax.fori_loop(1, n_sp, greet, 0)
    for k in (nxt, prv):
        pl.semaphore_signal(barrier, inc=1, device_id={"tp": k}, device_id_type=MESH_ID)
    pl.semaphore_wait(barrier, n_sp + 1)

    for a, src in ((0, s_in), (1, s_gr)):
        landing = recv.at[a, slab(me), at(tp, wide)]
        pltpu.make_async_copy(src.at[slab(me), :], landing, a_recv.at[a, me // (n_sp // 2)]).start()

        def deliver(i, carry):
            e = lax.rem(me + i, n_sp)
            pltpu.make_async_remote_copy(
                src_ref=src.at[slab(e), :],
                dst_ref=landing,
                send_sem=a_send.at[a],
                recv_sem=a_recv.at[a, me // (n_sp // 2)],
                device_id={"sp": e},
                device_id_type=MESH_ID,
            ).start()
            return carry

        lax.fori_loop(1, n_sp, deliver, 0)

    toks = res.shape[0]
    blk = toks // 2
    pairs = share // LANES
    core, y_at, z_at = lax.rem(me, 2), lax.rem(me // 2, 4), me // 8

    def pieces(v):
        out = []
        for _ in range(3):
            p = v.astype(BF)
            out.append(p)
            v = v - p.astype(F32)
        return out

    heads = ld_ref.shape[1]
    lane_head = (iota((heads, share), 1) // (share // heads) == iota((heads, share), 0)).astype(
        F32
    ).astype(BF)
    lower = (iota((blk, blk), 0) >= iota((blk, blk), 1)).astype(F32).astype(BF)
    upper = (iota((blk, blk), 0) <= iota((blk, blk), 1)).astype(F32).astype(BF)
    for b in range(2):
        steps = pieces(ld_ref[b * blk : (b + 1) * blk, :])
        cum_t[b * heads : (b + 1) * heads, :] = sum(t_dot(p, upper) for p in steps)
        cum[b * blk : (b + 1) * blk, :] = sum(
            dot(lower, dot(p, lane_head).astype(BF)) for p in steps
        )
    ends = [cum[(b + 1) * blk - 1 : (b + 1) * blk, :] for b in range(2)]

    def by_pair(row):
        return jnp.concatenate(
            [row[:, p * LANES : (p + 1) * LANES] for p in range(pairs)], axis=0
        )

    both_ends = by_pair(ends[0] + ends[1])
    logs[me] = jnp.concatenate([both_ends, jnp.zeros_like(both_ends)], axis=0)

    def tell(i, carry):
        pltpu.make_async_remote_copy(
            src_ref=logs.at[me],
            dst_ref=logs.at[me],
            send_sem=lt_send.at[0],
            recv_sem=lt_recv.at[0],
            device_id={"sp": lax.rem(me + i, n_sp)},
            device_id_type=MESH_ID,
        ).start()
        return carry

    lax.fori_loop(1, n_sp, tell, 0)
    for load in loads[4:]:
        load.wait()
    low_lane = iota((1, LANES), 1) < LANES // 2
    causal = iota((blk, blk), 0) >= iota((blk, blk), 1)

    def spot(i):
        b, p = i // pairs, lax.rem(i, pairs)
        return pl.ds(pl.multiple_of(b * blk, blk), blk), at(p, LANES), b, p

    def side(v, hh):
        return jnp.where(low_lane if hh == 0 else ~low_lane, v, jnp.zeros_like(v))

    @pl.loop(0, 2 * pairs)
    def _(i):
        rows, cols, b, p = spot(i)
        q, k = qkv[0, rows, cols], qkv[1, rows, cols]
        c = cum[rows, cols]
        for hh in range(2):
            column = c[:, hh * (LANES // 2) : hh * (LANES // 2) + 1]
            row = cum_t[pl.ds(b * heads + p * 2 + hh, 1), :]
            d = jnp.where(causal, jnp.exp(jnp.minimum(column - row, 0.0)), 0.0)
            decay[i * 2 + hh] = d
            score[i * 2 + hh] = (dot_t(q, side(k, hh)) * d).astype(BF)

    def tp_copy(ref, dst, sends, recvs, i, k):
        return pltpu.make_async_remote_copy(
            src_ref=ref, dst_ref=dst, send_sem=sends.at[i], recv_sem=recvs.at[i],
            device_id={"tp": k}, device_id_type=MESH_ID,
        )

    def ring_copies(view, sends, recvs):
        def move(h, k, i, to):
            return tp_copy(view(h, k), view(h, k), sends, recvs, i, to)

        return [
            move(0, tp, 0, nxt), move(1, tp, 1, nxt), move(0, tp, 2, prv), move(1, tp, 3, prv),
            move(0, prv, 4, nxt), move(1, nxt, 5, prv),
        ]

    jj = iota((hs, hs), 0)
    qq = iota((hs, hs), 1)
    unpick = (
        qq == ((jj % hl) // LEFT) * MAIN + (jj // hl) * LEFT + jj % LEFT
    ).astype(F32).astype(BF)
    pick = (
        qq == ((jj % MAIN) // LEFT) * hl + (jj // MAIN) * LEFT + jj % LEFT
    ).astype(F32).astype(BF)
    groups = MAIN // LEFT

    def unpack(a, k):
        for h in range(2):
            rows = pl.ds(h * hs, hs)
            xs[a, h * hx : h * hx + hs, at(k, share)] = recv[a, rows, pl.ds(pl.multiple_of(k * wide, LANES), share)]
            tail = recv[a, rows, pl.ds(pl.multiple_of(k * wide + share, LANES), LANES)]
            spread = dot(unpick, tail).astype(BF)
            left = jnp.concatenate([spread[g * hl : (g + 1) * hl] for g in range(groups)], axis=1)
            xs[a, h * hx + hs : (h + 1) * hx, at(k, share)] = left

    def piece_in(k, fresh):
        unpack(0, k)

        @pl.loop(0, 2)
        def _(h):
            rows = pl.ds(pl.multiple_of(h * hx, MAIN), hx)
            x = xs[0, rows, at(k, share)]
            g = dot(x, wg[at(k, share), :])
            u = dot(x, wu[at(k, share), :])
            if fresh:
                acc[0, rows, :] = g
                acc[1, rows, :] = u
            else:
                acc[0, rows, :] += g
                acc[1, rows, :] += u

    def piece_gr(k, fresh):
        unpack(1, k)

        @pl.loop(0, 2)
        def _(h):
            rows = pl.ds(pl.multiple_of(h * hx, MAIN), hx)
            d = dot_t(xs[1, rows, at(k, share)], wd[:, at(k, share)])
            if fresh:
                acc[2, rows, :] = d
            else:
                acc[2, rows, :] += d

    rings = [
        ring_copies(
            lambda h, k, a=a: recv.at[a, pl.ds(h * hs, hs), at(k, wide)],
            g_send.at[a], g_recv.at[a],
        )
        for a in range(2)
    ]

    def wait_arrivals(a, h):
        ref = recv.at[a, pl.ds(h * hs, hs), at(tp, wide)]
        pltpu.make_async_copy(ref, ref, a_recv.at[a, h]).wait()

    def ring_begin(ring, ready):
        ready(0)
        ring[0].start()
        ring[2].start()
        ready(1)
        ring[3].start()
        ring[1].start()

    def ring_relay(ring):
        ring[0].wait_recv()
        ring[4].start()
        ring[3].wait_recv()
        ring[5].start()

    ring_begin(rings[0], lambda h: wait_arrivals(0, h))
    loads[0].wait()
    loads[1].wait()
    piece_in(tp, True)
    ring_relay(rings[0])
    ring_begin(rings[1], lambda h: wait_arrivals(1, h))
    rings[0][1].wait_recv()
    piece_in(prv, False)
    rings[0][2].wait_recv()
    piece_in(nxt, False)
    loads[2].wait()
    piece_gr(tp, True)
    rings[0][4].wait_recv()
    rings[0][5].wait_recv()
    piece_in(far, False)
    x_copy = pltpu.make_async_copy(xs.at[0], x_out, o_sem.at[0])
    x_copy.start()

    step = 2 * MAIN

    @pl.loop(0, 2 * hx // step)
    def _(i):
        rows = pl.ds(pl.multiple_of(i * step, step), step)
        gate, up = acc[0, rows, :], acc[1, rows, :]
        clamped = jnp.minimum(gate, clamp_limit)
        logistic = 1.0 / (1.0 + jnp.exp(-sigmoid_sharpness * clamped))
        linear = jnp.clip(up, -clamp_limit, clamp_limit) + 1.0
        swish = clamped * logistic
        half_out[2, rows, :] = (swish * linear).astype(BF)
        slope = logistic + sigmoid_sharpness * swish * (1.0 - logistic)
        acc[0, rows, :] = jnp.where(gate < clamp_limit, linear * slope, 0.0)
        acc[1, rows, :] = jnp.where(jnp.abs(up) < clamp_limit, swish, 0.0)

    act_copy = pltpu.make_async_copy(half_out.at[2], act_out, o_sem.at[1])
    act_copy.start()

    ring_relay(rings[1])
    rings[1][1].wait_recv()
    piece_gr(prv, False)
    rings[1][2].wait_recv()
    piece_gr(nxt, False)
    rings[1][4].wait_recv()
    rings[1][5].wait_recv()
    piece_gr(far, False)
    c_copy = pltpu.make_async_copy(xs.at[1], c_out, o_sem.at[2])
    c_copy.start()

    @pl.loop(0, 2 * hx // step)
    def _(i):
        rows = pl.ds(pl.multiple_of(i * step, step), step)
        act_grad = acc[2, rows, :]
        half_out[0, rows, :] = (act_grad * acc[0, rows, :]).astype(BF)
        half_out[1, rows, :] = (act_grad * acc[1, rows, :]).astype(BF)

    gg_copy = pltpu.make_async_copy(half_out.at[0], gg_out, o_sem.at[3])
    ug_copy = pltpu.make_async_copy(half_out.at[1], ug_out, o_sem.at[4])
    gg_copy.start()
    ug_copy.start()

    def expert_part(k, slot):
        @pl.loop(0, 2)
        def _(h):
            rows = pl.ds(pl.multiple_of(h * hx, MAIN), hx)
            y = dot_t(half_out[0, rows, :], wg[at(k, share), :])
            y = y + dot_t(half_out[1, rows, :], wu[at(k, share), :])
            ip[slot, rows, :] = y.astype(BF)

    halves = [pl.ds(0, hx), pl.ds(hx, hx)]

    def rs_copy(src, dst, i, k):
        return tp_copy(src, dst, rs_send, rs_recv, i, k)

    rs = [
        rs_copy(ip.at[0, halves[0]], far_in.at[0], 0, nxt),
        rs_copy(ip.at[0, halves[1]], far_in.at[1], 1, prv),
        rs_copy(ip.at[1, halves[1]], near_in.at[0, halves[1]], 2, nxt),
        rs_copy(ip.at[2, halves[0]], near_in.at[1, halves[0]], 3, prv),
        rs_copy(ip.at[1, halves[0]], near_in.at[0, halves[0]], 4, nxt),
        rs_copy(ip.at[2, halves[1]], near_in.at[1, halves[1]], 5, prv),
    ]
    expert_part(far, 0)
    rs[0].start()
    rs[1].start()
    expert_part(nxt, 1)
    rs[2].start()
    expert_part(prv, 2)
    rs[3].start()
    rs[0].wait_recv()
    ip[1, halves[0], :] = (ip[1, halves[0], :].astype(F32) + far_in[0].astype(F32)).astype(BF)
    rs[4].start()
    rs[1].wait_recv()
    ip[2, halves[1], :] = (ip[2, halves[1], :].astype(F32) + far_in[1].astype(F32)).astype(BF)
    rs[5].start()
    expert_part(tp, 3)

    for h in range(2):
        rs[(4, 2)[h]].wait_recv()
        rs[(3, 5)[h]].wait_recv()
        total = (
            ip[3, halves[h], :].astype(F32)
            + near_in[0, halves[h], :].astype(F32)
            + near_in[1, halves[h], :].astype(F32)
        ).astype(BF)
        ret_t[h * hs : (h + 1) * hs, :share] = total[:hs]
        stacked = jnp.concatenate(
            [total[hs:, g * LANES : (g + 1) * LANES] for g in range(groups)], axis=0
        )
        ret_t[h * hs : (h + 1) * hs, share:] = dot(pick, stacked).astype(BF)

        def give_back(i, carry):
            s = h * (n_sp // 2) + lax.rem(me + i, n_sp // 2)

            @pl.when(s != me)
            def _():
                pltpu.make_async_remote_copy(
                    src_ref=ret_t.at[slab(s), :],
                    dst_ref=ret_q.at[slab(me), :],
                    send_sem=t_send.at[0],
                    recv_sem=t_recv.at[0],
                    device_id={"sp": s},
                    device_id_type=MESH_ID,
                ).start()

            return carry

        lax.fori_loop(0, n_sp // 2, give_back, 0)
    ret_q[slab(me), :] = ret_t[slab(me), :]
    others = pl.ds(0, (n_sp - 1) * MAIN)
    pltpu.make_async_copy(ret_q.at[others, :], ret_q.at[others, :], t_recv.at[0]).wait()

    p_left = pl_ref[...]
    y = t_dot(pm_ref[...], ret_q[:, :share])
    tails = ret_q[:, share:]
    group = (iota(p_left.shape, 0) % MAIN) // LEFT
    y = y + jnp.concatenate(
        [t_dot(jnp.where(group == g, p_left, jnp.zeros_like(p_left)), tails) for g in range(groups)],
        axis=1,
    )
    res[:, at(tp, share)] = (cot_ref[:, at(tp, share)].astype(F32) + y).astype(BF)
    ring = ring_copies(
        lambda h, k: res.at[pl.ds(h * (toks // 2), toks // 2), at(k, share)], r_send, r_recv
    )
    ring_begin(ring, lambda h: None)
    block = share // (2 * pairs)
    plane = pairs * block
    partner = me + 1 - 2 * core

    def sp_copy(src, dst, send_sem, recv_sem, e):
        return pltpu.make_async_remote_copy(
            src_ref=src, dst_ref=dst, send_sem=send_sem, recv_sem=recv_sem,
            device_id={"sp": e}, device_id_type=MESH_ID,
        )

    order = (tp, prv, nxt, far)

    def plane_rows(k):
        return pl.ds(pl.multiple_of(k * plane, plane), plane)

    swaps = [
        sp_copy(
            part.at[1 - core, plane_rows(k), :], peer.at[plane_rows(k), :],
            d_send.at[i], d_recv.at[i], partner,
        )
        for i, k in enumerate(order)
    ]

    def piece_res(i):
        k = order[i]
        r = res[:, at(k, share)]
        y = dot(r, ow[at(k, share), :])
        if i == 0:
            gm[...] = y
        else:
            gm[...] += y
        for j in range(pairs):
            g = t_dot(r[:, j * LANES : (j + 1) * LANES], mix[...]).astype(BF)
            for c in range(2):
                part[c, pl.ds(pl.multiple_of(k * plane + j * block, block), block), :] = g[
                    c * block : (c + 1) * block
                ]
        swaps[i].start()

    loads[3].wait()
    piece_res(0)
    ring_relay(ring)
    ring[1].wait_recv()
    piece_res(1)
    ring[2].wait_recv()
    piece_res(2)
    ring[4].wait_recv()
    ring[5].wait_recv()
    piece_res(3)
    gmb[...] = gm[...].astype(BF)

    half = LANES // 2

    @pl.loop(0, 2 * pairs)
    def _(i):
        rows, cols, b, p = spot(i)
        q = (qkv[0, rows, cols].astype(F32) * jnp.exp(cum[rows, cols])).astype(BF)
        o = t_dot(q, gmb[rows, cols])
        outer[b, p] = jnp.where(low_lane, o[:half], o[half:])

    def pair_rows(tile):
        return tile[:pairs][:, None, :]

    block_factor = [jnp.exp(by_pair(e))[:, None, :] for e in ends]
    total = block_factor[0] * outer[1] + outer[0]
    local[0] = total.astype(BF)
    swap_state = sp_copy(local.at[0], cbuf, sc_send.at[0], sc_recv.at[0], partner)
    swap_state.start()
    tiles = pl.ds(0, n_sp - 1)
    pltpu.make_async_copy(logs.at[tiles], logs.at[tiles], lt_recv.at[0]).wait()

    def chip_log(z, y):
        return logs[z * 8 + y * 2] + logs[z * 8 + y * 2 + 1]

    later_core_log = logs[me - core + 1]
    earlier_core_log = logs[me - core]

    swap_state.wait_recv()
    mine, others_total = local[0].astype(F32), cbuf[...].astype(F32)
    early = jnp.where(core == 0, mine, others_total)
    late = jnp.where(core == 0, others_total, mine)
    chip_total = jnp.exp(pair_rows(earlier_core_log)) * late + early
    ybuf[y_at] = chip_total.astype(BF)
    y_sends = [
        sp_copy(
            ybuf.at[y_at], ybuf.at[y_at], sy_send.at[i - 1], sy_recv.at[i - 1],
            z_at * 8 + lax.rem(y_at + i, 4) * 2 + core,
        )
        for i in range(1, 4)
    ]
    for copy in y_sends:
        copy.start()

    my_block = me // 2

    def send_plane(i):
        k = order[i]
        swaps[i].wait_recv()
        rows = plane_rows(k)
        part[core, rows, :] = (
            part[core, rows, :].astype(F32) + peer[rows, :].astype(F32)
        ).astype(BF)
        for j in range(4):
            zy = k * 4 + lax.rem(y_at + j, 4)

            @pl.when(zy != my_block)
            def _():
                sp_copy(
                    part.at[core, pl.ds(pl.multiple_of(zy * block, block), block), :],
                    got.at[my_block], b_send.at[0], b_recv.at[0], zy * 2 + core,
                ).start()

    send_plane(0)
    send_plane(1)
    for copy in y_sends:
        copy.wait_recv()
    inside_y = jnp.zeros_like(total)
    plane_total = jnp.zeros_like(total)
    later_y = jnp.zeros((2 * pairs, LANES), F32)
    for y in (3, 2, 1, 0):
        log = chip_log(z_at, y)
        factor = jnp.exp(pair_rows(log))
        t = ybuf[y].astype(F32)
        inside_y = jnp.where(y > y_at, factor * inside_y + t, inside_y)
        later_y = jnp.where(y > y_at, later_y + log, later_y)
        plane_total = factor * plane_total + t
    local[1] = plane_total.astype(BF)
    z_sends = [
        sp_copy(local.at[1], zbuf.at[i - 1], sz_send.at[i - 1], sz_recv.at[i - 1], me - i * 8)
        for i in range(1, 4)
    ]
    for i, copy in enumerate(z_sends, 1):

        @pl.when(z_at >= i)
        def _():
            copy.start()

    send_plane(2)
    send_plane(3)

    @pl.loop(0, 2 * pairs)
    def _(i):
        rows, cols, b, p = spot(i)
        q, k, v, g = qkv[0, rows, cols], qkv[1, rows, cols], qkv[2, rows, cols], gmb[rows, cols]
        outs = []
        for hh in range(2):
            wg_ts = (dot_t(g, side(v, hh)) * decay[i * 2 + hh]).astype(BF)
            outs.append((dot(wg_ts, k), t_dot(wg_ts, q), t_dot(score[i * 2 + hh], g)))
        intra = [jnp.where(low_lane, lo, hi) for lo, hi in zip(*outs)]
        st = st_ref[b, p]
        full = jnp.concatenate([side(st, 0), side(st, 1)], axis=0)
        carry = dot_t(g, full) * jnp.exp(cum[rows, cols])
        gq_out[rows, cols] = (intra[0] + carry).astype(BF)
        gm[rows, cols] = intra[1]
        acc[0, rows, cols] = intra[2]

    beyond = jnp.zeros_like(total)
    local_state = acc.at[1, pl.ds(0, pairs * half), pl.ds(0, LANES)]
    local_state[...] = jnp.zeros((pairs * half, LANES), F32)
    for i in (3, 2, 1):

        @pl.when(z_at + i < 4)
        def _():
            z_sends[i - 1].wait_recv()
            log = sum(chip_log(z_at + i, y) for y in range(4))
            now = local_state[...].reshape(pairs, half, LANES)
            now = jnp.exp(pair_rows(log)) * now + zbuf[i - 1].astype(F32)
            local_state[...] = now.reshape(pairs * half, LANES)

    beyond = local_state[...].reshape(pairs, half, LANES)
    entering_state = jnp.exp(pair_rows(later_y)) * beyond + inside_y
    entering_state = jnp.where(
        core == 0, jnp.exp(pair_rows(later_core_log)) * entering_state + late, entering_state
    )
    carried = (block_factor[1] * entering_state + outer[1], entering_state)
    for b in range(2):
        outer[b] = carried[b]

    @pl.loop(0, 2 * pairs)
    def _(i):
        rows, cols, b, p = spot(i)
        k, v = qkv[1, rows, cols], qkv[2, rows, cols]
        st = outer[b, p].astype(BF)
        full = jnp.concatenate([side(st, 0), side(st, 1)], axis=0)
        c = cum[rows, cols]
        to_end = jnp.exp(c[blk - 1 : blk, :] - c)
        gk_out[rows, cols] = (gm[rows, cols] + dot_t(v, full) * to_end).astype(BF)
        gv_out[rows, cols] = (acc[0, rows, cols] + dot(k, full) * to_end).astype(BF)

    blocks = pl.ds(0, 15)
    pltpu.make_async_copy(got.at[blocks], got.at[blocks], b_recv.at[0]).wait()
    got[my_block] = part[core, pl.ds(pl.multiple_of(my_block * block, block), block), :]
    sums = got[0].astype(F32)
    for i in range(1, 16):
        sums = sums + got[i].astype(F32)
    go_out[...] = sums

    pltpu.make_async_copy(got.at[blocks], got.at[blocks], b_send.at[0]).wait()
    pltpu.make_async_copy(logs.at[tiles], logs.at[tiles], lt_send.at[0]).wait()
    for copy in swaps + [swap_state] + y_sends:
        copy.wait_send()
    for i, copy in enumerate(z_sends, 1):

        @pl.when(z_at >= i)
        def _():
            copy.wait_send()

    for a in range(2):
        ref = recv.at[a, others, at(tp, wide)]
        pltpu.make_async_copy(ref, ref, a_send.at[a]).wait()
        for copy in rings[a]:
            copy.wait_send()
    for copy in rs + ring:
        copy.wait_send()
    pltpu.make_async_copy(ret_q.at[others, :], ret_q.at[others, :], t_send.at[0]).wait()
    for copy in (x_copy, act_copy, c_copy, gg_copy, ug_copy):
        copy.wait()


def expert_call(
    s_in, s_gr, w_gate, w_up, w_down, w_out, mixer, queries, key_vectors, value_vectors,
    p_main, p_left, cotangent, log_decay, states,
):
    n_sp, n_tp = lax.axis_size("sp"), lax.axis_size("tp")
    width, hidden = w_gate.shape
    rows, wide = s_in.shape
    share = width // n_tp
    full = n_sp * (MAIN + LEFT)
    toks = cotangent.shape[0]
    anyspace = pl.BlockSpec(memory_space=pl.ANY)
    vmem = pl.BlockSpec(memory_space=pltpu.VMEM)
    dma = pltpu.SemaphoreType.DMA
    return pl.pallas_call(
        expert_kernel,
        out_shape=(
            jax.ShapeDtypeStruct((full, width), BF),
            jax.ShapeDtypeStruct((full, width), BF),
            jax.ShapeDtypeStruct((full, hidden), BF),
            jax.ShapeDtypeStruct((full, hidden), BF),
            jax.ShapeDtypeStruct((full, hidden), BF),
            jax.ShapeDtypeStruct((width // n_sp, share), F32),
            jax.ShapeDtypeStruct((toks, share), BF),
            jax.ShapeDtypeStruct((toks, share), BF),
            jax.ShapeDtypeStruct((toks, share), BF),
        ),
        in_specs=[anyspace] * 10 + [vmem] * 5,
        out_specs=[anyspace] * 5 + [vmem] * 4,
        scratch_shapes=[
            pltpu.VMEM((2, rows, n_tp * wide), BF),
            pltpu.VMEM((2, full, width), BF),
            pltpu.VMEM(w_gate.shape, BF),
            pltpu.VMEM(w_up.shape, BF),
            pltpu.VMEM(w_down.shape, BF),
            pltpu.VMEM((3, full, hidden), F32),
            pltpu.VMEM((3, full, hidden), BF),
            pltpu.VMEM((4, full, share), BF),
            pltpu.VMEM((2, full // 2, share), BF),
            pltpu.VMEM((2, full, share), BF),
            pltpu.VMEM((rows, wide), BF),
            pltpu.VMEM((rows, wide), BF),
            pltpu.VMEM((toks, width), BF),
            dma((8,)), dma((2,)), dma((2, 2)), dma((2, 6)), dma((2, 6)),
            dma((6,)), dma((6,)), dma((1,)), dma((1,)), dma((6,)), dma((6,)), dma((5,)),
            pltpu.VMEM(w_out.shape, BF),
            pltpu.VMEM(mixer.shape, BF),
            pltpu.VMEM((3, toks, share), BF),
            pltpu.VMEM((toks, share), F32),
            pltpu.VMEM((2 * log_decay.shape[1], toks // 2), F32),
            pltpu.VMEM((16, toks // 2, toks // 2), F32),
            pltpu.VMEM((16, toks // 2, toks // 2), BF),
            pltpu.VMEM((n_sp, 8, LANES), F32),
            pltpu.VMEM((toks, share), F32),
            pltpu.VMEM((toks, share), BF),
            pltpu.VMEM((2, 4, 64, LANES), F32),
            pltpu.VMEM((2, 4, 64, LANES), BF),
            pltpu.VMEM((2, width // 2, share), BF),
            pltpu.VMEM((width // 2, share), BF),
            pltpu.VMEM((16, width // n_sp, share), BF),
            pltpu.VMEM((4, 4, 64, LANES), BF),
            pltpu.VMEM((3, 4, 64, LANES), BF),
            dma((1,)), dma((1,)), dma((4,)), dma((4,)), dma((1,)), dma((1,)), dma((1,)),
            dma((1,)), dma((3,)), dma((3,)), dma((3,)), dma((3,)),
            pltpu.VMEM((4, 64, LANES), BF),
        ],
        compiler_params=pltpu.CompilerParams(
            collective_id=0, has_side_effects=True, vmem_limit_bytes=60 << 20
        ),
        cost_estimate=pl.CostEstimate(flops=10**10, bytes_accessed=20 << 20, transcendentals=0),
        name="experts",
    )(
        s_in, s_gr, w_gate, w_up, w_down, w_out, mixer, queries, key_vectors, value_vectors,
        p_main, p_left, cotangent, log_decay, states,
    )


def contract_rows(left, right):
    return lax.dot_general(
        left, right, (((0,), (0,)), ((), ())), preferred_element_type=jnp.float32
    )


def shards(
    moe_input,
    cotangent,
    routes,
    route_weights,
    gate_weight,
    up_weight,
    down_weight,
    out_weight,
    mixer_output,
    queries,
    key_vectors,
    value_vectors,
    log_decay,
    block_states,
):
    s_in, s_gr, p_main, p_left = prep(
        routes.T, route_weights.T, moe_input, cotangent, lax.axis_size("sp")
    )
    blocks, heads, dim, _ = block_states.shape
    states = block_states.reshape(blocks, heads // 2, 2, dim, dim)
    states = jnp.swapaxes(states, 2, 3).reshape(blocks, heads // 2, dim, 2 * dim)
    rows, row_grads, gate_grad, up_grad, activation, grad_out, grad_queries, grad_keys, grad_values = (
        expert_call(
            s_in, s_gr, gate_weight[0], up_weight[0], down_weight[0], out_weight, mixer_output,
            queries, key_vectors, value_vectors, p_main, p_left, cotangent, log_decay, states,
        )
    )
    grad_gate = contract_rows(rows, gate_grad)[None]
    grad_up = contract_rows(rows, up_grad)[None]
    grad_down = contract_rows(activation, row_grads)[None]
    return (grad_gate, grad_up, grad_down, grad_out, grad_queries, grad_keys, grad_values)


def solution(mesh):
    return jax.shard_map(
        shards,
        mesh=mesh,
        in_specs=(
            P(SP, None),
            P(SP, None),
            P(SP, None),
            P(SP, None),
            P(SP, None, "tp"),
            P(SP, None, "tp"),
            P(SP, "tp", None),
            P(None, "tp"),
            P(SP, "tp"),
            P(SP, "tp"),
            P(SP, "tp"),
            P(SP, "tp"),
            P(SP, "tp"),
            P(SP, "tp", None, None),
        ),
        out_specs=(
            P(SP, None, "tp"),
            P(SP, None, "tp"),
            P(SP, "tp", None),
            P(SP, "tp"),
            P(SP, "tp"),
            P(SP, "tp"),
            P(SP, "tp"),
        ),
        check_vma=False,
    )
```

```python
import jax
import jax.numpy as jnp
from jax import lax
from jax.sharding import PartitionSpec as P
from jax.experimental import pallas as pl
from jax.experimental.pallas import tpu as pltpu

SP = "sp"
WEIGHT_STEPS = 8


clamp_limit = 7.0
sigmoid_sharpness = 1.702


MAIN = 16
LEFT = 4
LANES = 128
BF = jnp.bfloat16
F32 = jnp.float32
MESH_ID = pl.DeviceIdType.MESH


def dot(a, b):
    return jnp.dot(a, b, preferred_element_type=F32)


def dot_t(a, b):
    return lax.dot_general(a, b, (((1,), (1,)), ((), ())), preferred_element_type=F32)


def t_dot(a, b):
    return lax.dot_general(a, b, (((0,), (0,)), ((), ())), preferred_element_type=F32)


def iota(shape, dim):
    return lax.broadcasted_iota(jnp.int32, shape, dim)


def expert_kernel(
    routes_h, weights_h, x_h, cot_h, ld_h, st_h, wg_h, wu_h, wd_h, ow_h, mix_h, q_h, k_h, v_h,
    xt_h, c_h, gg_h, ug_h, act_h, go_out, gq_out, gk_out, gv_out,
    xt_out, act_out, gg_out, ug_out, o_sem, tails, xs, wg, wu, wd, acc, half_out, ip, far_in, near_in, ret_t, ret_q, res,
    w_sem, a_send, a_recv, l_send, l_recv, g_send, g_recv, rs_send, rs_recv, t_send, t_recv, r_send, r_recv,
    ow, mix, qkv, cum, cum_t, decay, score, logs, gm, gmb, outer, local, part, peer, got,
    ybuf, zbuf, lt_send, lt_recv, d_send, d_recv, b_send, b_recv, sc_send, sc_recv,
    sy_send, sy_recv, sz_send, sz_recv, cbuf,
    routes, weights, xq, cq, ld_ref, st_ref, sent, sent_left, stacks, pm_ref, pl_ref, e_sem,
    stack_sem,
):
    n_sp, n_tp = lax.axis_size("sp"), lax.axis_size("tp")
    me, tp = lax.axis_index("sp"), lax.axis_index("tp")
    nxt, prv, far = lax.rem(tp + 1, n_tp), lax.rem(tp + n_tp - 1, n_tp), lax.rem(tp + 2, n_tp)
    share = wg.shape[0] // n_tp
    wide = share + LANES
    hidden = wg.shape[1]
    hs = n_sp // 2 * MAIN
    hx = n_sp // 2 * (MAIN + LEFT)
    hl = n_sp // 2 * LEFT

    def at(k, width):
        return pl.ds(pl.multiple_of(k * width, LANES), width)

    def slab(k):
        return pl.ds(pl.multiple_of(k * MAIN, MAIN), MAIN)

    def main_slab(k):
        return pl.ds(pl.multiple_of(k * MAIN + k // (n_sp // 2) * hl, MAIN), MAIN)

    groups = MAIN // LEFT

    mine_cols = at(tp, share)
    early = [
        pltpu.make_async_copy(src, dst, e_sem.at[i])
        for i, (src, dst) in enumerate(
            (
                (routes_h, routes), (x_h.at[:, mine_cols], xq), (weights_h, weights),
                (cot_h.at[:, mine_cols], cq), (ld_h, ld_ref), (st_h, st_ref),
            )
        )
    ]
    for load in early:
        load.start()
    toks = pm_ref.shape[1]
    stack_loads = [
        pltpu.make_async_copy(
            src.at[:, pl.ds(k * share + g * LANES, LANES)],
            stacks.at[a, pl.ds(g * toks, toks), pl.ds(k * LANES, LANES)],
            stack_sem.at[a, k * groups + g],
        )
        for a, src in enumerate((x_h, cot_h))
        for k in range(n_tp)
        for g in range(groups)
    ]
    for load in stack_loads:
        load.start()
    loads = [
        pltpu.make_async_copy(src, dst, w_sem.at[i])
        for i, (src, dst) in enumerate(
            ((wg_h, wg), (wu_h, wu), (wd_h, wd), (ow_h, ow), (mix_h, mix))
            + tuple((src, qkv.at[j]) for j, src in enumerate((q_h, k_h, v_h)))
        )
    ]
    for load in loads:
        load.start()

    barrier = pltpu.get_barrier_semaphore()

    def greet(i, carry):
        pl.semaphore_signal(
            barrier, inc=1, device_id={"sp": lax.rem(me + i, n_sp)}, device_id_type=MESH_ID
        )
        return carry

    lax.fori_loop(1, n_sp, greet, 0)
    for k in (nxt, prv):
        pl.semaphore_signal(barrier, inc=1, device_id={"tp": k}, device_id_type=MESH_ID)

    rows_all = pm_ref.shape[0]
    e = iota((n_sp, toks), 0)
    early[0].wait()
    first = routes[0:1, :] == e
    second = routes[1:2, :] == e
    chosen = first | second
    before = (iota((toks, toks), 0) < iota((toks, toks), 1)).astype(F32).astype(BF)
    ranks = jnp.where(chosen, dot(chosen.astype(F32).astype(BF), before), -1.0).astype(BF)
    owner = (iota((rows_all, n_sp), 0) // MAIN == iota((rows_all, n_sp), 1)).astype(F32).astype(BF)
    spread = dot(owner, ranks).astype(jnp.int32)
    place = iota((rows_all, toks), 0) % MAIN
    is_main = spread == place
    is_left = spread == MAIN + place % LEFT
    pm_ref[...] = is_main.astype(F32).astype(BF)
    pl_ref[...] = is_left.astype(F32).astype(BF)
    early[1].wait()
    sent[0] = dot(pm_ref[...], xq[...]).astype(BF)
    pl.semaphore_wait(barrier, n_sp + 1)

    def spread_out(src, landing, send_sem, recv_sem):
        def deliver(i, carry):
            e = lax.rem(me + i, n_sp)
            pltpu.make_async_remote_copy(
                src_ref=src.at[slab(e), :],
                dst_ref=landing,
                send_sem=send_sem,
                recv_sem=recv_sem,
                device_id={"sp": e},
                device_id_type=MESH_ID,
            ).start()
            return carry

        lax.fori_loop(1, n_sp, deliver, 0)

    def dispatch(a):
        landing = xs.at[a, main_slab(me), at(tp, share)]
        spread_out(sent.at[a], landing, a_send.at[a], a_recv.at[a, me // (n_sp // 2)])
        xs[a, main_slab(me), at(tp, share)] = sent[a, slab(me), :]

    def dispatch_left(a):
        spread_out(sent_left.at[a], tails.at[a, slab(me), :], l_send.at[a], l_recv.at[a])
        tails[a, slab(me), :] = sent_left[a, slab(me), :]

    dispatch(0)
    early[2].wait()
    early[3].wait()
    w = jnp.where(first, weights[0:1, :], 0.0) + jnp.where(second, weights[1:2, :], 0.0)
    w_rows = jnp.zeros((rows_all, toks), F32)
    for _ in range(3):
        piece = w.astype(BF)
        w_rows = w_rows + dot(owner, piece)
        w = w - piece.astype(F32)
    w_main = jnp.sum(jnp.where(is_main, w_rows, 0.0), axis=1, keepdims=True)
    w_left = jnp.sum(jnp.where(is_left, w_rows, 0.0), axis=1, keepdims=True)
    sent[1] = (w_main * dot(pm_ref[...], cq[...])).astype(BF)
    dispatch(1)
    row_group = (iota((rows_all, toks), 0) % MAIN) // LEFT
    p_left = pl_ref[...]
    p_wide = jnp.concatenate(
        [jnp.where(row_group == g, p_left, jnp.zeros_like(p_left)) for g in range(groups)], axis=1
    )
    for load in stack_loads:
        load.wait()
    sent_left[0] = dot(p_wide, stacks[0]).astype(BF)
    dispatch_left(0)
    sent_left[1] = (w_left * dot(p_wide, stacks[1])).astype(BF)
    dispatch_left(1)
    early[4].wait()
    early[5].wait()

    blk = toks // 2
    pairs = share // LANES
    core, y_at, z_at = lax.rem(me, 2), lax.rem(me // 2, 4), me // 8

    def pieces(v):
        out = []
        for _ in range(3):
            p = v.astype(BF)
            out.append(p)
            v = v - p.astype(F32)
        return out

    heads = ld_ref.shape[0]
    lane_head = (iota((heads, share), 1) // (share // heads) == iota((heads, share), 0)).astype(
        F32
    ).astype(BF)
    lower = (iota((blk, blk), 0) >= iota((blk, blk), 1)).astype(F32).astype(BF)
    upper = (iota((blk, blk), 0) <= iota((blk, blk), 1)).astype(F32).astype(BF)
    for b in range(2):
        steps = pieces(ld_ref[:, b * blk : (b + 1) * blk])
        cum_t[b * heads : (b + 1) * heads, :] = sum(dot(p, upper) for p in steps)
        cum[b * blk : (b + 1) * blk, :] = sum(
            dot(lower, t_dot(p, lane_head).astype(BF)) for p in steps
        )
    ends = [cum[(b + 1) * blk - 1 : (b + 1) * blk, :] for b in range(2)]

    def by_pair(row):
        return jnp.concatenate(
            [row[:, p * LANES : (p + 1) * LANES] for p in range(pairs)], axis=0
        )

    both_ends = by_pair(ends[0] + ends[1])
    logs[me] = jnp.concatenate([both_ends, jnp.zeros_like(both_ends)], axis=0)

    def tell(i, carry):
        pltpu.make_async_remote_copy(
            src_ref=logs.at[me],
            dst_ref=logs.at[me],
            send_sem=lt_send.at[0],
            recv_sem=lt_recv.at[0],
            device_id={"sp": lax.rem(me + i, n_sp)},
            device_id_type=MESH_ID,
        ).start()
        return carry

    lax.fori_loop(1, n_sp, tell, 0)
    for load in loads[4:]:
        load.wait()
    low_lane = iota((1, LANES), 1) < LANES // 2
    causal = iota((blk, blk), 0) >= iota((blk, blk), 1)

    def spot(i):
        b, p = i // pairs, lax.rem(i, pairs)
        return pl.ds(pl.multiple_of(b * blk, blk), blk), at(p, LANES), b, p

    def side(v, hh):
        return jnp.where(low_lane if hh == 0 else ~low_lane, v, jnp.zeros_like(v))

    @pl.loop(0, 2 * pairs)
    def _(i):
        rows, cols, b, p = spot(i)
        q, k = qkv[0, rows, cols], qkv[1, rows, cols]
        c = cum[rows, cols]
        for hh in range(2):
            column = c[:, hh * (LANES // 2) : hh * (LANES // 2) + 1]
            row = cum_t[pl.ds(b * heads + p * 2 + hh, 1), :]
            d = jnp.where(causal, jnp.exp(jnp.minimum(column - row, 0.0)), 0.0)
            decay[i * 2 + hh] = d
            score[i * 2 + hh] = (dot_t(q, side(k, hh)) * d).astype(BF)

    def tp_copy(ref, dst, sends, recvs, i, k):
        return pltpu.make_async_remote_copy(
            src_ref=ref, dst_ref=dst, send_sem=sends.at[i], recv_sem=recvs.at[i],
            device_id={"tp": k}, device_id_type=MESH_ID,
        )

    def ring_copies(view, sends, recvs):
        def move(h, k, i, to):
            return tp_copy(view(h, k), view(h, k), sends, recvs, i, to)

        return [
            move(0, tp, 0, nxt), move(1, tp, 1, nxt), move(0, tp, 2, prv), move(1, tp, 3, prv),
            move(0, prv, 4, nxt), move(1, nxt, 5, prv),
        ]

    jj = iota((hs, hs), 0)
    qq = iota((hs, hs), 1)
    unpick = (
        qq == ((jj % hl) // LEFT) * MAIN + (jj // hl) * LEFT + jj % LEFT
    ).astype(F32).astype(BF)
    pick = (
        qq == ((jj % MAIN) // LEFT) * hl + (jj // MAIN) * LEFT + jj % LEFT
    ).astype(F32).astype(BF)
    def unpack(a):
        ref = tails.at[a, pl.ds(0, (n_sp - 1) * MAIN), :]
        pltpu.make_async_copy(ref, ref, l_recv.at[a]).wait()
        for h in range(2):
            spread = dot(unpick, tails[a, h * hs : (h + 1) * hs, :]).astype(BF)
            for k in range(n_tp):
                for g in range(groups):
                    lanes = pl.ds(k * share + g * LANES, LANES)
                    xs[a, h * hx + hs : (h + 1) * hx, lanes] = spread[
                        g * hl : (g + 1) * hl, k * LANES : (k + 1) * LANES
                    ]

    def piece_in(k, fresh):
        @pl.loop(0, 2)
        def _(h):
            rows = pl.ds(pl.multiple_of(h * hx, MAIN), hs)
            x = xs[0, rows, at(k, share)]
            g = dot(x, wg[at(k, share), :])
            u = dot(x, wu[at(k, share), :])
            if fresh:
                acc[0, rows, :] = g
                acc[1, rows, :] = u
            else:
                acc[0, rows, :] += g
                acc[1, rows, :] += u

    def left_in():
        unpack(0)

        @pl.loop(0, 2)
        def _(h):
            rows = pl.ds(pl.multiple_of(h * hx + hs, MAIN), hl)
            x = xs[0, rows, :]
            acc[0, rows, :] = dot(x, wg[...])
            acc[1, rows, :] = dot(x, wu[...])

    def piece_gr(k, fresh):
        @pl.loop(0, 2)
        def _(h):
            rows = pl.ds(pl.multiple_of(h * hx, MAIN), hs)
            d = dot_t(xs[1, rows, at(k, share)], wd[:, at(k, share)])
            if fresh:
                acc[2, rows, :] = d
            else:
                acc[2, rows, :] += d

    def left_gr():
        unpack(1)

        @pl.loop(0, 2)
        def _(h):
            rows = pl.ds(pl.multiple_of(h * hx + hs, MAIN), hl)
            acc[2, rows, :] = dot_t(xs[1, rows, :], wd[...])

    rings = [
        ring_copies(
            lambda h, k, a=a: xs.at[a, pl.ds(h * hx, hs), at(k, share)],
            g_send.at[a], g_recv.at[a],
        )
        for a in range(2)
    ]

    def wait_arrivals(a, h):
        for inside in range(2):

            @pl.when((me // (n_sp // 2) == h) == (inside == 1))
            def _():
                ref = xs.at[a, pl.ds(h * hx, hs - inside * MAIN), at(tp, share)]
                pltpu.make_async_copy(ref, ref, a_recv.at[a, h]).wait()

    def ring_begin(ring, ready):
        ready(0)
        ring[0].start()
        ring[2].start()
        ready(1)
        ring[3].start()
        ring[1].start()

    def ring_relay(ring):
        ring[0].wait_recv()
        ring[4].start()
        ring[3].wait_recv()
        ring[5].start()

    ring_begin(rings[0], lambda h: wait_arrivals(0, h))
    loads[0].wait()
    loads[1].wait()
    piece_in(tp, True)
    ring_relay(rings[0])
    ring_begin(rings[1], lambda h: wait_arrivals(1, h))
    rings[0][1].wait_recv()
    piece_in(prv, False)
    rings[0][2].wait_recv()
    piece_in(nxt, False)
    loads[2].wait()
    piece_gr(tp, True)
    rings[0][4].wait_recv()
    rings[0][5].wait_recv()
    piece_in(far, False)
    left_in()

    step = 2 * MAIN

    @pl.loop(0, 2 * hx // step)
    def _(i):
        rows = pl.ds(pl.multiple_of(i * step, step), step)
        gate, up = acc[0, rows, :], acc[1, rows, :]
        clamped = jnp.minimum(gate, clamp_limit)
        logistic = 1.0 / (1.0 + jnp.exp(-sigmoid_sharpness * clamped))
        linear = jnp.clip(up, -clamp_limit, clamp_limit) + 1.0
        swish = clamped * logistic
        half_out[rows, :] = (swish * linear).astype(BF)
        slope = logistic + sigmoid_sharpness * swish * (1.0 - logistic)
        acc[0, rows, :] = jnp.where(gate < clamp_limit, linear * slope, 0.0)
        acc[1, rows, :] = jnp.where(jnp.abs(up) < clamp_limit, swish, 0.0)

    left_gr()
    ring_relay(rings[1])
    rings[1][1].wait_recv()
    piece_gr(prv, False)
    rings[1][2].wait_recv()
    piece_gr(nxt, False)
    rings[1][4].wait_recv()
    rings[1][5].wait_recv()
    piece_gr(far, False)

    @pl.loop(0, 2 * hx // step)
    def _(i):
        rows = pl.ds(pl.multiple_of(i * step, step), step)
        act_grad = acc[2, rows, :]
        gg_out[rows, :] = (act_grad * acc[0, rows, :]).astype(BF)
        ug_out[rows, :] = (act_grad * acc[1, rows, :]).astype(BF)

    def expert_part(k, slot):
        @pl.loop(0, 2)
        def _(h):
            rows = pl.ds(pl.multiple_of(h * hx, MAIN), hx)
            y = dot_t(gg_out[rows, :], wg[at(k, share), :])
            y = y + dot_t(ug_out[rows, :], wu[at(k, share), :])
            ip[slot, rows, :] = y.astype(BF)

    halves = [pl.ds(0, hx), pl.ds(hx, hx)]

    def rs_copy(src, dst, i, k):
        return tp_copy(src, dst, rs_send, rs_recv, i, k)

    rs = [
        rs_copy(ip.at[0, halves[0]], far_in.at[0], 0, nxt),
        rs_copy(ip.at[0, halves[1]], far_in.at[1], 1, prv),
        rs_copy(ip.at[1, halves[1]], near_in.at[0, halves[1]], 2, nxt),
        rs_copy(ip.at[2, halves[0]], near_in.at[1, halves[0]], 3, prv),
        rs_copy(ip.at[1, halves[0]], near_in.at[0, halves[0]], 4, nxt),
        rs_copy(ip.at[2, halves[1]], near_in.at[1, halves[1]], 5, prv),
    ]
    expert_part(far, 0)
    rs[0].start()
    rs[1].start()
    expert_part(nxt, 1)
    rs[2].start()
    expert_part(prv, 2)
    rs[3].start()

    @pl.loop(0, n_tp * groups)
    def _(i):
        xt_out[at(i, LANES), :] = xs[0, :, at(i, LANES)].T

    @pl.loop(0, hidden // LANES)
    def _(i):
        act_out[at(i, LANES), :] = half_out[:, at(i, LANES)].T

    saves = [
        pltpu.make_async_copy(src, dst, o_sem.at[i])
        for i, (src, dst) in enumerate(
            ((xt_out, xt_h), (xs.at[1], c_h), (gg_out, gg_h), (ug_out, ug_h), (act_out, act_h))
        )
    ]
    for save in saves:
        save.start()
    rs[0].wait_recv()
    ip[1, halves[0], :] = (ip[1, halves[0], :].astype(F32) + far_in[0].astype(F32)).astype(BF)
    rs[4].start()
    rs[1].wait_recv()
    ip[2, halves[1], :] = (ip[2, halves[1], :].astype(F32) + far_in[1].astype(F32)).astype(BF)
    rs[5].start()
    expert_part(tp, 3)

    for h in range(2):
        rs[(4, 2)[h]].wait_recv()
        rs[(3, 5)[h]].wait_recv()
        total = (
            ip[3, halves[h], :].astype(F32)
            + near_in[0, halves[h], :].astype(F32)
            + near_in[1, halves[h], :].astype(F32)
        ).astype(BF)
        ret_t[h * hs : (h + 1) * hs, :share] = total[:hs]
        stacked = jnp.concatenate(
            [total[hs:, g * LANES : (g + 1) * LANES] for g in range(groups)], axis=0
        )
        ret_t[h * hs : (h + 1) * hs, share:] = dot(pick, stacked).astype(BF)

        def give_back(i, carry):
            s = h * (n_sp // 2) + lax.rem(me + i, n_sp // 2)

            @pl.when(s != me)
            def _():
                pltpu.make_async_remote_copy(
                    src_ref=ret_t.at[slab(s), :],
                    dst_ref=ret_q.at[slab(me), :],
                    send_sem=t_send.at[0],
                    recv_sem=t_recv.at[0],
                    device_id={"sp": s},
                    device_id_type=MESH_ID,
                ).start()

            return carry

        lax.fori_loop(0, n_sp // 2, give_back, 0)
    ret_q[slab(me), :] = ret_t[slab(me), :]
    others = pl.ds(0, (n_sp - 1) * MAIN)
    pltpu.make_async_copy(ret_q.at[others, :], ret_q.at[others, :], t_recv.at[0]).wait()

    p_left = pl_ref[...]
    y = t_dot(pm_ref[...], ret_q[:, :share])
    back = ret_q[:, share:]
    group = (iota(p_left.shape, 0) % MAIN) // LEFT
    y = y + jnp.concatenate(
        [t_dot(jnp.where(group == g, p_left, jnp.zeros_like(p_left)), back) for g in range(groups)],
        axis=1,
    )
    res[:, at(tp, share)] = (cq[...].astype(F32) + y).astype(BF)
    ring = ring_copies(
        lambda h, k: res.at[pl.ds(h * (toks // 2), toks // 2), at(k, share)], r_send, r_recv
    )
    ring_begin(ring, lambda h: None)
    block = share // (2 * pairs)
    plane = pairs * block
    partner = me + 1 - 2 * core

    def sp_copy(src, dst, send_sem, recv_sem, e):
        return pltpu.make_async_remote_copy(
            src_ref=src, dst_ref=dst, send_sem=send_sem, recv_sem=recv_sem,
            device_id={"sp": e}, device_id_type=MESH_ID,
        )

    order = (tp, prv, nxt, far)

    def plane_rows(k):
        return pl.ds(pl.multiple_of(k * plane, plane), plane)

    swaps = [
        sp_copy(
            part.at[1 - core, plane_rows(k), :], peer.at[plane_rows(k), :],
            d_send.at[i], d_recv.at[i], partner,
        )
        for i, k in enumerate(order)
    ]

    def piece_res(i):
        k = order[i]
        r = res[:, at(k, share)]
        y = dot(r, ow[at(k, share), :])
        if i == 0:
            gm[...] = y
        else:
            gm[...] += y
        for j in range(pairs):
            g = t_dot(r[:, j * LANES : (j + 1) * LANES], mix[...]).astype(BF)
            for c in range(2):
                part[c, pl.ds(pl.multiple_of(k * plane + j * block, block), block), :] = g[
                    c * block : (c + 1) * block
                ]
        swaps[i].start()

    my_block = me // 2

    def send_plane(i):
        k = order[i]
        swaps[i].wait_recv()
        rows = plane_rows(k)
        part[core, rows, :] = (
            part[core, rows, :].astype(F32) + peer[rows, :].astype(F32)
        ).astype(BF)
        for j in range(4):
            zy = k * 4 + lax.rem(y_at + j, 4)

            @pl.when(zy != my_block)
            def _():
                sp_copy(
                    part.at[core, pl.ds(pl.multiple_of(zy * block, block), block), :],
                    got.at[my_block], b_send.at[0], b_recv.at[0], zy * 2 + core,
                ).start()

    loads[3].wait()
    piece_res(0)
    ring_relay(ring)
    ring[1].wait_recv()
    piece_res(1)
    send_plane(0)
    ring[2].wait_recv()
    piece_res(2)
    send_plane(1)
    ring[4].wait_recv()
    ring[5].wait_recv()
    piece_res(3)
    send_plane(2)
    gmb[...] = gm[...].astype(BF)

    half = LANES // 2

    @pl.loop(0, 2 * pairs)
    def _(i):
        rows, cols, b, p = spot(i)
        q = (qkv[0, rows, cols].astype(F32) * jnp.exp(cum[rows, cols])).astype(BF)
        o = t_dot(q, gmb[rows, cols])
        outer[b, p] = jnp.where(low_lane, o[:half], o[half:])

    def pair_rows(tile):
        return tile[:pairs][:, None, :]

    block_factor = [jnp.exp(by_pair(e))[:, None, :] for e in ends]
    total = block_factor[0] * outer[1] + outer[0]
    local[0] = total.astype(BF)
    swap_state = sp_copy(local.at[0], cbuf, sc_send.at[0], sc_recv.at[0], partner)
    swap_state.start()
    tiles = pl.ds(0, n_sp - 1)
    pltpu.make_async_copy(logs.at[tiles], logs.at[tiles], lt_recv.at[0]).wait()

    def chip_log(z, y):
        return logs[z * 8 + y * 2] + logs[z * 8 + y * 2 + 1]

    later_core_log = logs[me - core + 1]
    earlier_core_log = logs[me - core]

    swap_state.wait_recv()
    mine, others_total = local[0].astype(F32), cbuf[...].astype(F32)
    early = jnp.where(core == 0, mine, others_total)
    late = jnp.where(core == 0, others_total, mine)
    chip_total = jnp.exp(pair_rows(earlier_core_log)) * late + early
    ybuf[y_at] = chip_total.astype(BF)
    y_sends = [
        sp_copy(
            ybuf.at[y_at], ybuf.at[y_at], sy_send.at[i - 1], sy_recv.at[i - 1],
            z_at * 8 + lax.rem(y_at + i, 4) * 2 + core,
        )
        for i in range(1, 4)
    ]
    for copy in y_sends:
        copy.start()

    send_plane(3)
    for copy in y_sends:
        copy.wait_recv()
    inside_y = jnp.zeros_like(total)
    plane_total = jnp.zeros_like(total)
    later_y = jnp.zeros((2 * pairs, LANES), F32)
    for y in (3, 2, 1, 0):
        log = chip_log(z_at, y)
        factor = jnp.exp(pair_rows(log))
        t = ybuf[y].astype(F32)
        inside_y = jnp.where(y > y_at, factor * inside_y + t, inside_y)
        later_y = jnp.where(y > y_at, later_y + log, later_y)
        plane_total = factor * plane_total + t
    local[1] = plane_total.astype(BF)
    z_sends = [
        sp_copy(local.at[1], zbuf.at[i - 1], sz_send.at[i - 1], sz_recv.at[i - 1], me - i * 8)
        for i in range(1, 4)
    ]
    for i, copy in enumerate(z_sends, 1):

        @pl.when(z_at >= i)
        def _():
            copy.start()

    @pl.loop(0, 2 * pairs)
    def _(i):
        rows, cols, b, p = spot(i)
        q, k, v, g = qkv[0, rows, cols], qkv[1, rows, cols], qkv[2, rows, cols], gmb[rows, cols]
        outs = []
        for hh in range(2):
            wg_ts = (dot_t(g, side(v, hh)) * decay[i * 2 + hh]).astype(BF)
            outs.append((dot(wg_ts, k), t_dot(wg_ts, q), t_dot(score[i * 2 + hh], g)))
        intra = [jnp.where(low_lane, lo, hi) for lo, hi in zip(*outs)]
        st = [st_ref[b, 2 * p + hh] for hh in range(2)]
        none = jnp.zeros_like(st[0])
        full = jnp.concatenate(
            [
                jnp.concatenate([st[0], none], axis=1),
                jnp.concatenate([none, st[1]], axis=1),
            ],
            axis=0,
        )
        carry = dot_t(g, full) * jnp.exp(cum[rows, cols])
        gq_out[rows, cols] = (intra[0] + carry).astype(BF)
        gm[rows, cols] = intra[1]
        acc[0, rows, cols] = intra[2]

    beyond = jnp.zeros_like(total)
    local_state = acc.at[1, pl.ds(0, pairs * half), pl.ds(0, LANES)]
    local_state[...] = jnp.zeros((pairs * half, LANES), F32)
    for i in (3, 2, 1):

        @pl.when(z_at + i < 4)
        def _():
            z_sends[i - 1].wait_recv()
            log = sum(chip_log(z_at + i, y) for y in range(4))
            now = local_state[...].reshape(pairs, half, LANES)
            now = jnp.exp(pair_rows(log)) * now + zbuf[i - 1].astype(F32)
            local_state[...] = now.reshape(pairs * half, LANES)

    beyond = local_state[...].reshape(pairs, half, LANES)
    entering_state = jnp.exp(pair_rows(later_y)) * beyond + inside_y
    entering_state = jnp.where(
        core == 0, jnp.exp(pair_rows(later_core_log)) * entering_state + late, entering_state
    )
    carried = (block_factor[1] * entering_state + outer[1], entering_state)
    for b in range(2):
        outer[b] = carried[b]

    @pl.loop(0, 2 * pairs)
    def _(i):
        rows, cols, b, p = spot(i)
        k, v = qkv[1, rows, cols], qkv[2, rows, cols]
        st = outer[b, p].astype(BF)
        full = jnp.concatenate([side(st, 0), side(st, 1)], axis=0)
        c = cum[rows, cols]
        to_end = jnp.exp(c[blk - 1 : blk, :] - c)
        gk_out[rows, cols] = (gm[rows, cols] + dot_t(v, full) * to_end).astype(BF)
        gv_out[rows, cols] = (acc[0, rows, cols] + dot(k, full) * to_end).astype(BF)

    blocks = pl.ds(0, 15)
    pltpu.make_async_copy(got.at[blocks], got.at[blocks], b_recv.at[0]).wait()
    got[my_block] = part[core, pl.ds(pl.multiple_of(my_block * block, block), block), :]
    sums = got[0].astype(F32)
    for i in range(1, 16):
        sums = sums + got[i].astype(F32)
    go_out[...] = sums

    pltpu.make_async_copy(got.at[blocks], got.at[blocks], b_send.at[0]).wait()
    pltpu.make_async_copy(logs.at[tiles], logs.at[tiles], lt_send.at[0]).wait()
    for copy in swaps + [swap_state] + y_sends:
        copy.wait_send()
    for i, copy in enumerate(z_sends, 1):

        @pl.when(z_at >= i)
        def _():
            copy.wait_send()

    for a in range(2):
        for ref, sem in ((sent.at[a, others, :], a_send), (sent_left.at[a, others, :], l_send)):
            pltpu.make_async_copy(ref, ref, sem.at[a]).wait()
        for copy in rings[a]:
            copy.wait_send()
    for copy in rs + ring:
        copy.wait_send()
    for save in saves:
        save.wait()
    pltpu.make_async_copy(ret_q.at[others, :], ret_q.at[others, :], t_send.at[0]).wait()


def expert_call(
    routes, weights, x, cotangent, log_decay, states, w_gate, w_up, w_down, w_out, mixer,
    queries, key_vectors, value_vectors,
):
    n_sp, n_tp = lax.axis_size("sp"), lax.axis_size("tp")
    width, hidden = w_gate.shape
    share = width // n_tp
    wide = share + LANES
    rows = n_sp * MAIN
    full = n_sp * (MAIN + LEFT)
    toks = cotangent.shape[0]
    anyspace = pl.BlockSpec(memory_space=pl.ANY)
    vmem = pl.BlockSpec(memory_space=pltpu.VMEM)
    dma = pltpu.SemaphoreType.DMA
    return pl.pallas_call(
        expert_kernel,
        out_shape=(
            jax.ShapeDtypeStruct((width, full), BF),
            jax.ShapeDtypeStruct((full, width), BF),
            jax.ShapeDtypeStruct((full, hidden), BF),
            jax.ShapeDtypeStruct((full, hidden), BF),
            jax.ShapeDtypeStruct((hidden, full), BF),
            jax.ShapeDtypeStruct((width // n_sp, share), F32),
            jax.ShapeDtypeStruct((toks, share), BF),
            jax.ShapeDtypeStruct((toks, share), BF),
            jax.ShapeDtypeStruct((toks, share), BF),
        ),
        in_specs=[anyspace] * 14,
        out_specs=[anyspace] * 5 + [vmem] * 4,
        scratch_shapes=[
            pltpu.VMEM((width, full), BF),
            pltpu.VMEM((hidden, full), BF),
            pltpu.VMEM((full, hidden), BF),
            pltpu.VMEM((full, hidden), BF),
            dma((5,)),
            pltpu.VMEM((2, rows, n_tp * LANES), BF),
            pltpu.VMEM((2, full, width), BF),
            pltpu.VMEM(w_gate.shape, BF),
            pltpu.VMEM(w_up.shape, BF),
            pltpu.VMEM(w_down.shape, BF),
            pltpu.VMEM((3, full, hidden), F32),
            pltpu.VMEM((full, hidden), BF),
            pltpu.VMEM((4, full, share), BF),
            pltpu.VMEM((2, full // 2, share), BF),
            pltpu.VMEM((2, full, share), BF),
            pltpu.VMEM((rows, wide), BF),
            pltpu.VMEM((rows, wide), BF),
            pltpu.VMEM((toks, width), BF),
            dma((8,)), dma((2,)), dma((2, 2)), dma((2,)), dma((2,)), dma((2, 6)), dma((2, 6)),
            dma((6,)), dma((6,)), dma((1,)), dma((1,)), dma((6,)), dma((6,)),
            pltpu.VMEM(w_out.shape, BF),
            pltpu.VMEM(mixer.shape, BF),
            pltpu.VMEM((3, toks, share), BF),
            pltpu.VMEM((toks, share), F32),
            pltpu.VMEM((2 * log_decay.shape[0], toks // 2), F32),
            pltpu.VMEM((16, toks // 2, toks // 2), F32),
            pltpu.VMEM((16, toks // 2, toks // 2), BF),
            pltpu.VMEM((n_sp, 8, LANES), F32),
            pltpu.VMEM((toks, share), F32),
            pltpu.VMEM((toks, share), BF),
            pltpu.VMEM((2, 4, 64, LANES), F32),
            pltpu.VMEM((2, 4, 64, LANES), BF),
            pltpu.VMEM((2, width // 2, share), BF),
            pltpu.VMEM((width // 2, share), BF),
            pltpu.VMEM((16, width // n_sp, share), BF),
            pltpu.VMEM((4, 4, 64, LANES), BF),
            pltpu.VMEM((3, 4, 64, LANES), BF),
            dma((1,)), dma((1,)), dma((4,)), dma((4,)), dma((1,)), dma((1,)), dma((1,)),
            dma((1,)), dma((3,)), dma((3,)), dma((3,)), dma((3,)),
            pltpu.VMEM((4, 64, LANES), BF),
            pltpu.VMEM(routes.shape, jnp.int32),
            pltpu.VMEM(weights.shape, F32),
            pltpu.VMEM((toks, share), BF),
            pltpu.VMEM((toks, share), BF),
            pltpu.VMEM(log_decay.shape, F32),
            pltpu.VMEM(states.shape, BF),
            pltpu.VMEM((2, rows, share), BF),
            pltpu.VMEM((2, rows, n_tp * LANES), BF),
            pltpu.VMEM((2, MAIN // LEFT * toks, n_tp * LANES), BF),
            pltpu.VMEM((rows, toks), BF),
            pltpu.VMEM((rows, toks), BF),
            dma((6,)),
            dma((2, 16)),
        ],
        compiler_params=pltpu.CompilerParams(
            collective_id=0, has_side_effects=True, vmem_limit_bytes=62 << 20
        ),
        cost_estimate=pl.CostEstimate(flops=10**10, bytes_accessed=20 << 20, transcendentals=0),
        name="experts",
    )(
        routes, weights, x, cotangent, log_decay, states, w_gate, w_up, w_down, w_out, mixer,
        queries, key_vectors, value_vectors,
    )


def weight_kernel(
    xt, c, gg, ug, act, go, gq, gk, gv, gate_out, up_out, down_out, go_out, gq_out, gk_out, gv_out
):
    gate_out[...] = dot(xt[...], gg[...])
    up_out[...] = dot(xt[...], ug[...])
    down_out[...] = dot(act[...], c[...])
    go_out[...] = go[...]
    gq_out[...] = gq[...]
    gk_out[...] = gk[...]
    gv_out[...] = gv[...]


def weight_call(xt, c, gg, ug, act, go, gq, gk, gv, steps):
    width, rows = xt.shape
    hidden = gg.shape[1]
    tile = width // steps
    slice_in = pl.BlockSpec((rows, tile), lambda i: (0, i))
    slice_x = pl.BlockSpec((tile, rows), lambda i: (i, 0))
    whole = pl.BlockSpec((rows, hidden), lambda i: (0, 0))
    whole_t = pl.BlockSpec((hidden, rows), lambda i: (0, 0))
    tall = pl.BlockSpec((tile, hidden), lambda i: (i, 0))

    def banded(v):
        return pl.BlockSpec((v.shape[0] // steps, v.shape[1]), lambda i: (i, 0))

    small = [banded(v) for v in (go, gq, gk, gv)]
    return pl.pallas_call(
        weight_kernel,
        grid=(steps,),
        out_shape=(
            jax.ShapeDtypeStruct((width, hidden), F32),
            jax.ShapeDtypeStruct((width, hidden), F32),
            jax.ShapeDtypeStruct((hidden, width), F32),
        )
        + tuple(jax.ShapeDtypeStruct(v.shape, v.dtype) for v in (go, gq, gk, gv)),
        in_specs=[slice_x, slice_in, whole, whole, whole_t] + small,
        out_specs=[tall, tall, pl.BlockSpec((hidden, tile), lambda i: (0, i))] + small,
        compiler_params=pltpu.CompilerParams(vmem_limit_bytes=62 << 20),
        name="weights",
    )(xt, c, gg, ug, act, go, gq, gk, gv)


def shards(
    moe_input,
    cotangent,
    routes,
    route_weights,
    gate_weight,
    up_weight,
    down_weight,
    out_weight,
    mixer_output,
    queries,
    key_vectors,
    value_vectors,
    log_decay,
    block_states,
):
    outs = expert_call(
        routes.T, route_weights.T, moe_input, cotangent, log_decay.T, block_states,
        gate_weight[0], up_weight[0], down_weight[0], out_weight, mixer_output,
        queries, key_vectors, value_vectors,
    )
    grads = weight_call(*outs, steps=WEIGHT_STEPS)
    return tuple(g[None] for g in grads[:3]) + tuple(grads[3:])


def solution(mesh):
    return jax.shard_map(
        shards,
        mesh=mesh,
        in_specs=(
            P(SP, None),
            P(SP, None),
            P(SP, None),
            P(SP, None),
            P(SP, None, "tp"),
            P(SP, None, "tp"),
            P(SP, "tp", None),
            P(None, "tp"),
            P(SP, "tp"),
            P(SP, "tp"),
            P(SP, "tp"),
            P(SP, "tp"),
            P(SP, "tp"),
            P(SP, "tp", None, None),
        ),
        out_specs=(
            P(SP, None, "tp"),
            P(SP, None, "tp"),
            P(SP, "tp", None),
            P(SP, "tp"),
            P(SP, "tp"),
            P(SP, "tp"),
            P(SP, "tp"),
        ),
        check_vma=False,
    )
```

```python
import jax
import jax.numpy as jnp
from jax import lax
from jax.sharding import PartitionSpec as P
from jax.experimental import pallas as pl
from jax.experimental.pallas import tpu as pltpu

SP = "sp"
WEIGHT_STEPS = 4


clamp_limit = 7.0
sigmoid_sharpness = 1.702


MAIN = 16
LEFT = 4
LANES = 128
BF = jnp.bfloat16
F32 = jnp.float32
MESH_ID = pl.DeviceIdType.MESH


def dot(a, b):
    return jnp.dot(a, b, preferred_element_type=F32)


def dot_t(a, b):
    return lax.dot_general(a, b, (((1,), (1,)), ((), ())), preferred_element_type=F32)


def t_dot(a, b):
    return lax.dot_general(a, b, (((0,), (0,)), ((), ())), preferred_element_type=F32)


def iota(shape, dim):
    return lax.broadcasted_iota(jnp.int32, shape, dim)


def expert_kernel(
    routes_h, weights_h, x_h, cot_h, ld_h, st_h, wg_h, wu_h, wd_h, ow_h, mix_h, q_h, k_h, v_h,
    xt_h, c_h, gg_h, ug_h, act_h, go_out, gq_out, gk_out, gv_out,
    xt_out, act_out, gg_out, ug_out, o_sem, tails, xs, wg, wu, wd, acc, half_out, ip, far_in, near_in, ret_t, ret_q, res,
    w_sem, a_send, a_recv, l_send, l_recv, g_send, g_recv, rs_send, rs_recv, t_send, t_recv, r_send, r_recv,
    ow, mix, qkv, cum, cum_t, decay, score, logs, gm, gmb, outer, local, part, peer, got,
    ybuf, zbuf, lt_send, lt_recv, d_send, d_recv, b_send, b_recv, sc_send, sc_recv,
    sy_send, sy_recv, sz_send, sz_recv, cbuf,
    routes, weights, xq, cq, ld_ref, st_ref, sent, sent_left, stacks, pm_ref, pl_ref, e_sem,
    stack_sem,
):
    n_sp, n_tp = lax.axis_size("sp"), lax.axis_size("tp")
    me, tp = lax.axis_index("sp"), lax.axis_index("tp")
    nxt, prv, far = lax.rem(tp + 1, n_tp), lax.rem(tp + n_tp - 1, n_tp), lax.rem(tp + 2, n_tp)
    share = wg.shape[0] // n_tp
    wide = share + LANES
    hidden = wg.shape[1]
    hs = n_sp // 2 * MAIN
    hx = n_sp // 2 * (MAIN + LEFT)
    hl = n_sp // 2 * LEFT

    def at(k, width):
        return pl.ds(pl.multiple_of(k * width, LANES), width)

    def slab(k):
        return pl.ds(pl.multiple_of(k * MAIN, MAIN), MAIN)

    def main_slab(k):
        return pl.ds(pl.multiple_of(k * MAIN + k // (n_sp // 2) * hl, MAIN), MAIN)

    groups = MAIN // LEFT

    mine_cols = at(tp, share)
    early = [
        pltpu.make_async_copy(src, dst, e_sem.at[i])
        for i, (src, dst) in enumerate(
            (
                (routes_h, routes), (x_h.at[:, mine_cols], xq), (weights_h, weights),
                (cot_h.at[:, mine_cols], cq), (ld_h, ld_ref), (st_h, st_ref),
            )
        )
    ]
    for load in early:
        load.start()
    toks = pm_ref.shape[1]
    stack_loads = [
        pltpu.make_async_copy(
            src.at[:, pl.ds(k * share + g * LANES, LANES)],
            stacks.at[a, pl.ds(g * toks, toks), pl.ds(k * LANES, LANES)],
            stack_sem.at[a, k * groups + g],
        )
        for a, src in enumerate((x_h, cot_h))
        for k in range(n_tp)
        for g in range(groups)
    ]
    for load in stack_loads:
        load.start()
    loads = [
        pltpu.make_async_copy(src, dst, w_sem.at[i])
        for i, (src, dst) in enumerate(
            ((wg_h, wg), (wu_h, wu), (wd_h, wd), (ow_h, ow), (mix_h, mix))
            + tuple((src, qkv.at[j]) for j, src in enumerate((q_h, k_h, v_h)))
        )
    ]
    for load in loads:
        load.start()

    barrier = pltpu.get_barrier_semaphore()

    def greet(i, carry):
        pl.semaphore_signal(
            barrier, inc=1, device_id={"sp": lax.rem(me + i, n_sp)}, device_id_type=MESH_ID
        )
        return carry

    lax.fori_loop(1, n_sp, greet, 0)
    for k in (nxt, prv):
        pl.semaphore_signal(barrier, inc=1, device_id={"tp": k}, device_id_type=MESH_ID)

    rows_all = pm_ref.shape[0]
    e = iota((n_sp, toks), 0)
    early[0].wait()
    first = routes[0:1, :] == e
    second = routes[1:2, :] == e
    chosen = first | second
    before = (iota((toks, toks), 0) < iota((toks, toks), 1)).astype(F32).astype(BF)
    ranks = jnp.where(chosen, dot(chosen.astype(F32).astype(BF), before), -1.0).astype(BF)
    owner = (iota((rows_all, n_sp), 0) // MAIN == iota((rows_all, n_sp), 1)).astype(F32).astype(BF)
    spread = dot(owner, ranks).astype(jnp.int32)
    place = iota((rows_all, toks), 0) % MAIN
    is_main = spread == place
    is_left = spread == MAIN + place % LEFT
    pm_ref[...] = is_main.astype(F32).astype(BF)
    pl_ref[...] = is_left.astype(F32).astype(BF)
    early[1].wait()
    sent[0] = dot(pm_ref[...], xq[...]).astype(BF)
    pl.semaphore_wait(barrier, n_sp + 1)

    def spread_out(src, landing, send_sem, recv_sem):
        def deliver(i, carry):
            e = lax.rem(me + i, n_sp)
            pltpu.make_async_remote_copy(
                src_ref=src.at[slab(e), :],
                dst_ref=landing,
                send_sem=send_sem,
                recv_sem=recv_sem,
                device_id={"sp": e},
                device_id_type=MESH_ID,
            ).start()
            return carry

        lax.fori_loop(1, n_sp, deliver, 0)

    def dispatch(a):
        landing = xs.at[a, main_slab(me), at(tp, share)]
        spread_out(sent.at[a], landing, a_send.at[a], a_recv.at[a, me // (n_sp // 2)])
        xs[a, main_slab(me), at(tp, share)] = sent[a, slab(me), :]

    def dispatch_left(a):
        spread_out(sent_left.at[a], tails.at[a, slab(me), :], l_send.at[a], l_recv.at[a])
        tails[a, slab(me), :] = sent_left[a, slab(me), :]

    dispatch(0)
    early[2].wait()
    early[3].wait()
    w = jnp.where(first, weights[0:1, :], 0.0) + jnp.where(second, weights[1:2, :], 0.0)
    w_rows = jnp.zeros((rows_all, toks), F32)
    for _ in range(3):
        piece = w.astype(BF)
        w_rows = w_rows + dot(owner, piece)
        w = w - piece.astype(F32)
    w_main = jnp.sum(jnp.where(is_main, w_rows, 0.0), axis=1, keepdims=True)
    w_left = jnp.sum(jnp.where(is_left, w_rows, 0.0), axis=1, keepdims=True)
    sent[1] = (w_main * dot(pm_ref[...], cq[...])).astype(BF)
    dispatch(1)
    row_group = (iota((rows_all, toks), 0) % MAIN) // LEFT
    p_left = pl_ref[...]
    p_wide = jnp.concatenate(
        [jnp.where(row_group == g, p_left, jnp.zeros_like(p_left)) for g in range(groups)], axis=1
    )
    for load in stack_loads:
        load.wait()
    sent_left[0] = dot(p_wide, stacks[0]).astype(BF)
    dispatch_left(0)
    sent_left[1] = (w_left * dot(p_wide, stacks[1])).astype(BF)
    dispatch_left(1)
    early[4].wait()
    early[5].wait()

    blk = toks // 2
    pairs = share // LANES
    core, y_at, z_at = lax.rem(me, 2), lax.rem(me // 2, 4), me // 8

    def pieces(v):
        out = []
        for _ in range(3):
            p = v.astype(BF)
            out.append(p)
            v = v - p.astype(F32)
        return out

    heads = ld_ref.shape[0]
    lane_head = (iota((heads, share), 1) // (share // heads) == iota((heads, share), 0)).astype(
        F32
    ).astype(BF)
    lower = (iota((blk, blk), 0) >= iota((blk, blk), 1)).astype(F32).astype(BF)
    upper = (iota((blk, blk), 0) <= iota((blk, blk), 1)).astype(F32).astype(BF)
    for b in range(2):
        steps = pieces(ld_ref[:, b * blk : (b + 1) * blk])
        cum_t[b * heads : (b + 1) * heads, :] = sum(dot(p, upper) for p in steps)
        cum[b * blk : (b + 1) * blk, :] = sum(
            dot(lower, t_dot(p, lane_head).astype(BF)) for p in steps
        )
    ends = [cum[(b + 1) * blk - 1 : (b + 1) * blk, :] for b in range(2)]

    def by_pair(row):
        return jnp.concatenate(
            [row[:, p * LANES : (p + 1) * LANES] for p in range(pairs)], axis=0
        )

    both_ends = by_pair(ends[0] + ends[1])
    logs[me] = jnp.concatenate([both_ends, jnp.zeros_like(both_ends)], axis=0)

    def tell(i, carry):
        pltpu.make_async_remote_copy(
            src_ref=logs.at[me],
            dst_ref=logs.at[me],
            send_sem=lt_send.at[0],
            recv_sem=lt_recv.at[0],
            device_id={"sp": lax.rem(me + i, n_sp)},
            device_id_type=MESH_ID,
        ).start()
        return carry

    lax.fori_loop(1, n_sp, tell, 0)
    for load in loads[4:]:
        load.wait()
    low_lane = iota((1, LANES), 1) < LANES // 2
    causal = iota((blk, blk), 0) >= iota((blk, blk), 1)

    def spot(i):
        b, p = i // pairs, lax.rem(i, pairs)
        return pl.ds(pl.multiple_of(b * blk, blk), blk), at(p, LANES), b, p

    def side(v, hh):
        return jnp.where(low_lane if hh == 0 else ~low_lane, v, jnp.zeros_like(v))

    @pl.loop(0, 2 * pairs)
    def _(i):
        rows, cols, b, p = spot(i)
        q, k = qkv[0, rows, cols], qkv[1, rows, cols]
        c = cum[rows, cols]
        for hh in range(2):
            column = c[:, hh * (LANES // 2) : hh * (LANES // 2) + 1]
            row = cum_t[pl.ds(b * heads + p * 2 + hh, 1), :]
            d = jnp.where(causal, jnp.exp(jnp.minimum(column - row, 0.0)), 0.0)
            decay[i * 2 + hh] = d
            score[i * 2 + hh] = (dot_t(q, side(k, hh)) * d).astype(BF)

    def tp_copy(ref, dst, sends, recvs, i, k):
        return pltpu.make_async_remote_copy(
            src_ref=ref, dst_ref=dst, send_sem=sends.at[i], recv_sem=recvs.at[i],
            device_id={"tp": k}, device_id_type=MESH_ID,
        )

    def ring_copies(view, sends, recvs):
        def move(h, k, i, to):
            return tp_copy(view(h, k), view(h, k), sends, recvs, i, to)

        return [
            move(0, tp, 0, nxt), move(1, tp, 1, nxt), move(0, tp, 2, prv), move(1, tp, 3, prv),
            move(0, prv, 4, nxt), move(1, nxt, 5, prv),
        ]

    jj = iota((hs, hs), 0)
    qq = iota((hs, hs), 1)
    unpick = (
        qq == ((jj % hl) // LEFT) * MAIN + (jj // hl) * LEFT + jj % LEFT
    ).astype(F32).astype(BF)
    pick = (
        qq == ((jj % MAIN) // LEFT) * hl + (jj // MAIN) * LEFT + jj % LEFT
    ).astype(F32).astype(BF)
    def unpack(a):
        ref = tails.at[a, pl.ds(0, (n_sp - 1) * MAIN), :]
        pltpu.make_async_copy(ref, ref, l_recv.at[a]).wait()
        for h in range(2):
            spread = dot(unpick, tails[a, h * hs : (h + 1) * hs, :]).astype(BF)
            for k in range(n_tp):
                for g in range(groups):
                    lanes = pl.ds(k * share + g * LANES, LANES)
                    xs[a, h * hx + hs : (h + 1) * hx, lanes] = spread[
                        g * hl : (g + 1) * hl, k * LANES : (k + 1) * LANES
                    ]

    def piece_in(k, h):
        rows = pl.ds(h * hx, hs)
        x = xs[0, rows, at(k, share)]
        for i, w in ((0, wg), (1, wu)):
            y = dot(x, w[at(k, share), :])
            acc[i, rows, :] = y if k is tp else acc[i, rows, :] + y

    def left_in():
        unpack(0)
        for h in range(2):
            rows = pl.ds(h * hx + hs, hl)
            x = xs[0, rows, :]
            acc[0, rows, :] = dot(x, wg[...])
            acc[1, rows, :] = dot(x, wu[...])

    def piece_gr(k, h):
        rows = pl.ds(h * hx, hs)
        y = dot_t(xs[1, rows, at(k, share)], wd[:, at(k, share)])
        acc[2, rows, :] = y if k is tp else acc[2, rows, :] + y

    def left_gr():
        unpack(1)
        for h in range(2):
            rows = pl.ds(h * hx + hs, hl)
            acc[2, rows, :] = dot_t(xs[1, rows, :], wd[...])

    rings = [
        [
            ring_copies(
                lambda sub, k, a=a, h=h: xs.at[
                    a, pl.ds(h * hx + sub * (hs // 2), hs // 2), at(k, share)
                ],
                g_send.at[a, h], g_recv.at[a, h],
            )
            for h in range(2)
        ]
        for a in range(2)
    ]

    def wait_arrivals(a, h):
        for inside in range(2):

            @pl.when((me // (n_sp // 2) == h) == (inside == 1))
            def _():
                ref = xs.at[a, pl.ds(h * hx, hs - inside * MAIN), at(tp, share)]
                pltpu.make_async_copy(ref, ref, a_recv.at[a, h]).wait()

    def ring_begin(ring):
        for i in (0, 3, 1, 2):
            ring[i].start()

    def ring_relay(ring):
        ring[0].wait_recv()
        ring[4].start()
        ring[3].wait_recv()
        ring[5].start()

    def begin(a, h):
        wait_arrivals(a, h)
        ring_begin(rings[a][h])

    def near_pieces(a, h):
        rings[a][h][1].wait_recv()
        (piece_in, piece_gr)[a](prv, h)
        rings[a][h][2].wait_recv()
        (piece_in, piece_gr)[a](nxt, h)

    def far_piece(a, h):
        rings[a][h][4].wait_recv()
        rings[a][h][5].wait_recv()
        (piece_in, piece_gr)[a](far, h)

    step = 2 * MAIN

    def forward_half(h):
        @pl.loop(0, hx // step)
        def _(i):
            rows = pl.ds(pl.multiple_of(h * hx + i * step, step), step)
            gate, up = acc[0, rows, :], acc[1, rows, :]
            clamped = jnp.minimum(gate, clamp_limit)
            logistic = 1.0 / (1.0 + jnp.exp(-sigmoid_sharpness * clamped))
            linear = jnp.clip(up, -clamp_limit, clamp_limit) + 1.0
            swish = clamped * logistic
            half_out[rows, :] = (swish * linear).astype(BF)
            slope = logistic + sigmoid_sharpness * swish * (1.0 - logistic)
            acc[0, rows, :] = jnp.where(gate < clamp_limit, linear * slope, 0.0)
            acc[1, rows, :] = jnp.where(jnp.abs(up) < clamp_limit, swish, 0.0)

    def backward_half(h):
        @pl.loop(0, hx // step)
        def _(i):
            rows = pl.ds(pl.multiple_of(h * hx + i * step, step), step)
            act_grad = acc[2, rows, :]
            gg_out[rows, :] = (act_grad * acc[0, rows, :]).astype(BF)
            ug_out[rows, :] = (act_grad * acc[1, rows, :]).astype(BF)

    def expert_part(k, slot, h):
        rows = pl.ds(h * hx, hx)
        y = dot_t(gg_out[rows, :], wg[at(k, share), :])
        y = y + dot_t(ug_out[rows, :], wu[at(k, share), :])
        ip[slot, rows, :] = y.astype(BF)

    def sums(h):
        subs = [pl.ds(h * hx + sub * (hx // 2), hx // 2) for sub in range(2)]

        def rs_copy(src, dst, i, k):
            return tp_copy(src, dst, rs_send.at[h], rs_recv.at[h], i, k)

        return subs, [
            rs_copy(ip.at[0, subs[0]], far_in.at[h, 0], 0, nxt),
            rs_copy(ip.at[0, subs[1]], far_in.at[h, 1], 1, prv),
            rs_copy(ip.at[1, subs[1]], near_in.at[0, subs[1]], 2, nxt),
            rs_copy(ip.at[2, subs[0]], near_in.at[1, subs[0]], 3, prv),
            rs_copy(ip.at[1, subs[0]], near_in.at[0, subs[0]], 4, nxt),
            rs_copy(ip.at[2, subs[1]], near_in.at[1, subs[1]], 5, prv),
        ]

    reduces = [sums(h) for h in range(2)]

    def parts(h):
        for slot, k in enumerate((far, nxt, prv)):
            expert_part(k, slot, h)

    def send_parts(h):
        for copy in reduces[h][1][:4]:
            copy.start()

    def augment(h):
        subs, rs = reduces[h]
        for i in range(2):
            rs[i].wait_recv()
            ip[1 + i, subs[i], :] = (
                ip[1 + i, subs[i], :].astype(F32) + far_in[h, i].astype(F32)
            ).astype(BF)
            rs[4 + i].start()

    def finish(h):
        for i in range(2, 6):
            reduces[h][1][i].wait_recv()
        rows = pl.ds(h * hx, hx)
        total = (
            ip[3, rows, :].astype(F32)
            + near_in[0, rows, :].astype(F32)
            + near_in[1, rows, :].astype(F32)
        ).astype(BF)
        ret_t[h * hs : (h + 1) * hs, :share] = total[:hs]
        stacked = jnp.concatenate(
            [total[hs:, g * LANES : (g + 1) * LANES] for g in range(groups)], axis=0
        )
        ret_t[h * hs : (h + 1) * hs, share:] = dot(pick, stacked).astype(BF)

        def give_back(i, carry):
            s = h * (n_sp // 2) + lax.rem(me + i, n_sp // 2)

            @pl.when(s != me)
            def _():
                pltpu.make_async_remote_copy(
                    src_ref=ret_t.at[slab(s), :],
                    dst_ref=ret_q.at[slab(me), :],
                    send_sem=t_send.at[0],
                    recv_sem=t_recv.at[0],
                    device_id={"sp": s},
                    device_id_type=MESH_ID,
                ).start()

            return carry

        lax.fori_loop(0, n_sp // 2, give_back, 0)

    begin(0, 0)
    loads[0].wait()
    loads[1].wait()
    piece_in(tp, 0)
    ring_relay(rings[0][0])
    begin(1, 0)
    loads[2].wait()
    piece_gr(tp, 0)
    near_pieces(0, 0)
    ring_relay(rings[1][0])
    begin(0, 1)
    far_piece(0, 0)
    piece_in(tp, 1)
    left_in()
    forward_half(0)
    ring_relay(rings[0][1])
    begin(1, 1)
    near_pieces(1, 0)
    left_gr()
    far_piece(1, 0)
    backward_half(0)
    parts(0)
    ring_relay(rings[1][1])
    send_parts(0)
    piece_gr(tp, 1)
    near_pieces(0, 1)
    far_piece(0, 1)
    forward_half(1)
    expert_part(tp, 3, 0)
    near_pieces(1, 1)
    far_piece(1, 1)
    backward_half(1)
    parts(1)
    augment(0)
    send_parts(1)
    expert_part(tp, 3, 1)

    @pl.loop(0, hidden // LANES)
    def _(i):
        act_out[at(i, LANES), :] = half_out[:, at(i, LANES)].T

    finish(0)

    @pl.loop(0, n_tp * groups)
    def _(i):
        xt_out[at(i, LANES), :] = xs[0, :, at(i, LANES)].T

    augment(1)
    saves = [
        pltpu.make_async_copy(src, dst, o_sem.at[i])
        for i, (src, dst) in enumerate(
            ((xt_out, xt_h), (xs.at[1], c_h), (gg_out, gg_h), (ug_out, ug_h), (act_out, act_h))
        )
    ]
    for save in saves:
        save.start()
    finish(1)
    ret_q[slab(me), :] = ret_t[slab(me), :]
    others = pl.ds(0, (n_sp - 1) * MAIN)
    pltpu.make_async_copy(ret_q.at[others, :], ret_q.at[others, :], t_recv.at[0]).wait()

    p_left = pl_ref[...]
    y = t_dot(pm_ref[...], ret_q[:, :share])
    back = ret_q[:, share:]
    group = (iota(p_left.shape, 0) % MAIN) // LEFT
    y = y + jnp.concatenate(
        [t_dot(jnp.where(group == g, p_left, jnp.zeros_like(p_left)), back) for g in range(groups)],
        axis=1,
    )
    res[:, at(tp, share)] = (cq[...].astype(F32) + y).astype(BF)
    ring = ring_copies(
        lambda h, k: res.at[pl.ds(h * (toks // 2), toks // 2), at(k, share)], r_send, r_recv
    )
    ring_begin(ring)
    block = share // (2 * pairs)
    plane = pairs * block
    partner = me + 1 - 2 * core

    def sp_copy(src, dst, send_sem, recv_sem, e):
        return pltpu.make_async_remote_copy(
            src_ref=src, dst_ref=dst, send_sem=send_sem, recv_sem=recv_sem,
            device_id={"sp": e}, device_id_type=MESH_ID,
        )

    order = (tp, prv, nxt, far)

    def plane_rows(k):
        return pl.ds(pl.multiple_of(k * plane, plane), plane)

    swaps = [
        sp_copy(
            part.at[1 - core, plane_rows(k), :], peer.at[plane_rows(k), :],
            d_send.at[i], d_recv.at[i], partner,
        )
        for i, k in enumerate(order)
    ]

    def piece_mix(i):
        k = order[i]
        y = dot(res[:, at(k, share)], ow[at(k, share), :])
        gm[...] = y if i == 0 else gm[...] + y

    def piece_out(i):
        k = order[i]
        r = res[:, at(k, share)]
        for j in range(pairs):
            g = t_dot(r[:, j * LANES : (j + 1) * LANES], mix[...]).astype(BF)
            for c in range(2):
                part[c, pl.ds(pl.multiple_of(k * plane + j * block, block), block), :] = g[
                    c * block : (c + 1) * block
                ]
        swaps[i].start()

    def piece_res(i):
        piece_out(i)
        piece_mix(i)

    my_block = me // 2

    def send_plane(i):
        k = order[i]
        swaps[i].wait_recv()
        rows = plane_rows(k)
        part[core, rows, :] = (
            part[core, rows, :].astype(F32) + peer[rows, :].astype(F32)
        ).astype(BF)
        for j in range(4):
            zy = k * 4 + lax.rem(y_at + j, 4)

            @pl.when(zy != my_block)
            def _():
                sp_copy(
                    part.at[core, pl.ds(pl.multiple_of(zy * block, block), block), :],
                    got.at[my_block], b_send.at[0], b_recv.at[0], zy * 2 + core,
                ).start()

    loads[3].wait()
    piece_res(0)
    ring_relay(ring)
    send_plane(0)
    ring[1].wait_recv()
    piece_res(1)
    ring[2].wait_recv()
    piece_res(2)
    send_plane(1)
    ring[4].wait_recv()
    ring[5].wait_recv()
    piece_mix(3)
    gmb[...] = gm[...].astype(BF)

    half = LANES // 2

    @pl.loop(0, 2 * pairs)
    def _(i):
        rows, cols, b, p = spot(i)
        q = (qkv[0, rows, cols].astype(F32) * jnp.exp(cum[rows, cols])).astype(BF)
        o = t_dot(q, gmb[rows, cols])
        outer[b, p] = jnp.where(low_lane, o[:half], o[half:])

    def pair_rows(tile):
        return tile[:pairs][:, None, :]

    block_factor = [jnp.exp(by_pair(e))[:, None, :] for e in ends]
    total = block_factor[0] * outer[1] + outer[0]
    local[0] = total.astype(BF)
    swap_state = sp_copy(local.at[0], cbuf, sc_send.at[0], sc_recv.at[0], partner)
    swap_state.start()
    send_plane(2)
    piece_out(3)
    tiles = pl.ds(0, n_sp - 1)
    pltpu.make_async_copy(logs.at[tiles], logs.at[tiles], lt_recv.at[0]).wait()

    def chip_log(z, y):
        return logs[z * 8 + y * 2] + logs[z * 8 + y * 2 + 1]

    later_core_log = logs[me - core + 1]
    earlier_core_log = logs[me - core]

    swap_state.wait_recv()
    mine, others_total = local[0].astype(F32), cbuf[...].astype(F32)
    early = jnp.where(core == 0, mine, others_total)
    late = jnp.where(core == 0, others_total, mine)
    chip_total = jnp.exp(pair_rows(earlier_core_log)) * late + early
    ybuf[y_at] = chip_total.astype(BF)
    y_sends = [
        sp_copy(
            ybuf.at[y_at], ybuf.at[y_at], sy_send.at[i - 1], sy_recv.at[i - 1],
            z_at * 8 + lax.rem(y_at + i, 4) * 2 + core,
        )
        for i in range(1, 4)
    ]
    for copy in y_sends:
        copy.start()

    send_plane(3)
    for copy in y_sends:
        copy.wait_recv()
    inside_y = jnp.zeros_like(total)
    plane_total = jnp.zeros_like(total)
    later_y = jnp.zeros((2 * pairs, LANES), F32)
    for y in (3, 2, 1, 0):
        log = chip_log(z_at, y)
        factor = jnp.exp(pair_rows(log))
        t = ybuf[y].astype(F32)
        inside_y = jnp.where(y > y_at, factor * inside_y + t, inside_y)
        later_y = jnp.where(y > y_at, later_y + log, later_y)
        plane_total = factor * plane_total + t
    local[1] = plane_total.astype(BF)
    z_sends = [
        sp_copy(local.at[1], zbuf.at[i - 1], sz_send.at[i - 1], sz_recv.at[i - 1], me - i * 8)
        for i in range(1, 4)
    ]
    for i, copy in enumerate(z_sends, 1):

        @pl.when(z_at >= i)
        def _():
            copy.start()

    @pl.loop(0, 2 * pairs)
    def _(i):
        rows, cols, b, p = spot(i)
        q, k, v, g = qkv[0, rows, cols], qkv[1, rows, cols], qkv[2, rows, cols], gmb[rows, cols]
        outs = []
        for hh in range(2):
            wg_ts = (dot_t(g, side(v, hh)) * decay[i * 2 + hh]).astype(BF)
            outs.append((dot(wg_ts, k), t_dot(wg_ts, q), t_dot(score[i * 2 + hh], g)))
        intra = [jnp.where(low_lane, lo, hi) for lo, hi in zip(*outs)]
        st = [st_ref[b, 2 * p + hh] for hh in range(2)]
        none = jnp.zeros_like(st[0])
        full = jnp.concatenate(
            [
                jnp.concatenate([st[0], none], axis=1),
                jnp.concatenate([none, st[1]], axis=1),
            ],
            axis=0,
        )
        carry = dot_t(g, full) * jnp.exp(cum[rows, cols])
        gq_out[rows, cols] = (intra[0] + carry).astype(BF)
        gm[rows, cols] = intra[1]
        acc[0, rows, cols] = intra[2]

    beyond = jnp.zeros_like(total)
    local_state = acc.at[1, pl.ds(0, pairs * half), pl.ds(0, LANES)]
    local_state[...] = jnp.zeros((pairs * half, LANES), F32)
    for i in (3, 2, 1):

        @pl.when(z_at + i < 4)
        def _():
            z_sends[i - 1].wait_recv()
            log = sum(chip_log(z_at + i, y) for y in range(4))
            now = local_state[...].reshape(pairs, half, LANES)
            now = jnp.exp(pair_rows(log)) * now + zbuf[i - 1].astype(F32)
            local_state[...] = now.reshape(pairs * half, LANES)

    beyond = local_state[...].reshape(pairs, half, LANES)
    entering_state = jnp.exp(pair_rows(later_y)) * beyond + inside_y
    entering_state = jnp.where(
        core == 0, jnp.exp(pair_rows(later_core_log)) * entering_state + late, entering_state
    )
    carried = (block_factor[1] * entering_state + outer[1], entering_state)
    for b in range(2):
        outer[b] = carried[b]

    @pl.loop(0, 2 * pairs)
    def _(i):
        rows, cols, b, p = spot(i)
        k, v = qkv[1, rows, cols], qkv[2, rows, cols]
        st = outer[b, p].astype(BF)
        full = jnp.concatenate([side(st, 0), side(st, 1)], axis=0)
        c = cum[rows, cols]
        to_end = jnp.exp(c[blk - 1 : blk, :] - c)
        gk_out[rows, cols] = (gm[rows, cols] + dot_t(v, full) * to_end).astype(BF)
        gv_out[rows, cols] = (acc[0, rows, cols] + dot(k, full) * to_end).astype(BF)

    blocks = pl.ds(0, 15)
    pltpu.make_async_copy(got.at[blocks], got.at[blocks], b_recv.at[0]).wait()
    got[my_block] = part[core, pl.ds(pl.multiple_of(my_block * block, block), block), :]
    sums = got[0].astype(F32)
    for i in range(1, 16):
        sums = sums + got[i].astype(F32)
    go_out[...] = sums

    pltpu.make_async_copy(got.at[blocks], got.at[blocks], b_send.at[0]).wait()
    pltpu.make_async_copy(logs.at[tiles], logs.at[tiles], lt_send.at[0]).wait()
    for copy in swaps + [swap_state] + y_sends:
        copy.wait_send()
    for i, copy in enumerate(z_sends, 1):

        @pl.when(z_at >= i)
        def _():
            copy.wait_send()

    for a in range(2):
        for ref, sem in ((sent.at[a, others, :], a_send), (sent_left.at[a, others, :], l_send)):
            pltpu.make_async_copy(ref, ref, sem.at[a]).wait()
        for copy in rings[a][0] + rings[a][1]:
            copy.wait_send()
    for copy in reduces[0][1] + reduces[1][1] + ring:
        copy.wait_send()
    for save in saves:
        save.wait()
    pltpu.make_async_copy(ret_q.at[others, :], ret_q.at[others, :], t_send.at[0]).wait()


def expert_call(
    routes, weights, x, cotangent, log_decay, states, w_gate, w_up, w_down, w_out, mixer,
    queries, key_vectors, value_vectors,
):
    n_sp, n_tp = lax.axis_size("sp"), lax.axis_size("tp")
    width, hidden = w_gate.shape
    share = width // n_tp
    wide = share + LANES
    rows = n_sp * MAIN
    full = n_sp * (MAIN + LEFT)
    toks = cotangent.shape[0]
    anyspace = pl.BlockSpec(memory_space=pl.ANY)
    vmem = pl.BlockSpec(memory_space=pltpu.VMEM)
    dma = pltpu.SemaphoreType.DMA
    return pl.pallas_call(
        expert_kernel,
        out_shape=(
            jax.ShapeDtypeStruct((width, full), BF),
            jax.ShapeDtypeStruct((full, width), BF),
            jax.ShapeDtypeStruct((full, hidden), BF),
            jax.ShapeDtypeStruct((full, hidden), BF),
            jax.ShapeDtypeStruct((hidden, full), BF),
            jax.ShapeDtypeStruct((width // n_sp, share), F32),
            jax.ShapeDtypeStruct((toks, share), BF),
            jax.ShapeDtypeStruct((toks, share), BF),
            jax.ShapeDtypeStruct((toks, share), BF),
        ),
        in_specs=[anyspace] * 14,
        out_specs=[anyspace] * 5 + [vmem] * 4,
        scratch_shapes=[
            pltpu.VMEM((width, full), BF),
            pltpu.VMEM((hidden, full), BF),
            pltpu.VMEM((full, hidden), BF),
            pltpu.VMEM((full, hidden), BF),
            dma((5,)),
            pltpu.VMEM((2, rows, n_tp * LANES), BF),
            pltpu.VMEM((2, full, width), BF),
            pltpu.VMEM(w_gate.shape, BF),
            pltpu.VMEM(w_up.shape, BF),
            pltpu.VMEM(w_down.shape, BF),
            pltpu.VMEM((3, full, hidden), F32),
            pltpu.VMEM((full, hidden), BF),
            pltpu.VMEM((4, full, share), BF),
            pltpu.VMEM((2, 2, full // 4, share), BF),
            pltpu.VMEM((2, full, share), BF),
            pltpu.VMEM((rows, wide), BF),
            pltpu.VMEM((rows, wide), BF),
            pltpu.VMEM((toks, width), BF),
            dma((8,)), dma((2,)), dma((2, 2)), dma((2,)), dma((2,)), dma((2, 2, 6)), dma((2, 2, 6)),
            dma((2, 6)), dma((2, 6)), dma((1,)), dma((1,)), dma((6,)), dma((6,)),
            pltpu.VMEM(w_out.shape, BF),
            pltpu.VMEM(mixer.shape, BF),
            pltpu.VMEM((3, toks, share), BF),
            pltpu.VMEM((toks, share), F32),
            pltpu.VMEM((2 * log_decay.shape[0], toks // 2), F32),
            pltpu.VMEM((16, toks // 2, toks // 2), F32),
            pltpu.VMEM((16, toks // 2, toks // 2), BF),
            pltpu.VMEM((n_sp, 8, LANES), F32),
            pltpu.VMEM((toks, share), F32),
            pltpu.VMEM((toks, share), BF),
            pltpu.VMEM((2, 4, 64, LANES), F32),
            pltpu.VMEM((2, 4, 64, LANES), BF),
            pltpu.VMEM((2, width // 2, share), BF),
            pltpu.VMEM((width // 2, share), BF),
            pltpu.VMEM((16, width // n_sp, share), BF),
            pltpu.VMEM((4, 4, 64, LANES), BF),
            pltpu.VMEM((3, 4, 64, LANES), BF),
            dma((1,)), dma((1,)), dma((4,)), dma((4,)), dma((1,)), dma((1,)), dma((1,)),
            dma((1,)), dma((3,)), dma((3,)), dma((3,)), dma((3,)),
            pltpu.VMEM((4, 64, LANES), BF),
            pltpu.VMEM(routes.shape, jnp.int32),
            pltpu.VMEM(weights.shape, F32),
            pltpu.VMEM((toks, share), BF),
            pltpu.VMEM((toks, share), BF),
            pltpu.VMEM(log_decay.shape, F32),
            pltpu.VMEM(states.shape, BF),
            pltpu.VMEM((2, rows, share), BF),
            pltpu.VMEM((2, rows, n_tp * LANES), BF),
            pltpu.VMEM((2, MAIN // LEFT * toks, n_tp * LANES), BF),
            pltpu.VMEM((rows, toks), BF),
            pltpu.VMEM((rows, toks), BF),
            dma((6,)),
            dma((2, 16)),
        ],
        compiler_params=pltpu.CompilerParams(
            collective_id=0, has_side_effects=True, vmem_limit_bytes=62 << 20
        ),
        cost_estimate=pl.CostEstimate(flops=10**10, bytes_accessed=20 << 20, transcendentals=0),
        name="experts",
    )(
        routes, weights, x, cotangent, log_decay, states, w_gate, w_up, w_down, w_out, mixer,
        queries, key_vectors, value_vectors,
    )


def weight_kernel(
    xt, c, gg, ug, act, go, gq, gk, gv, gate_out, up_out, down_out, go_out, gq_out, gk_out, gv_out
):
    gate_out[...] = dot(xt[...], gg[...])
    up_out[...] = dot(xt[...], ug[...])
    down_out[...] = dot(act[...], c[...])
    go_out[...] = go[...]
    gq_out[...] = gq[...]
    gk_out[...] = gk[...]
    gv_out[...] = gv[...]


def weight_call(xt, c, gg, ug, act, go, gq, gk, gv, steps):
    width, rows = xt.shape
    hidden = gg.shape[1]
    tile = width // steps
    slice_in = pl.BlockSpec((rows, tile), lambda i: (0, i))
    slice_x = pl.BlockSpec((tile, rows), lambda i: (i, 0))
    whole = pl.BlockSpec((rows, hidden), lambda i: (0, 0))
    whole_t = pl.BlockSpec((hidden, rows), lambda i: (0, 0))
    tall = pl.BlockSpec((tile, hidden), lambda i: (i, 0))

    def banded(v):
        return pl.BlockSpec((v.shape[0] // steps, v.shape[1]), lambda i: (i, 0))

    small = [banded(v) for v in (go, gq, gk, gv)]
    return pl.pallas_call(
        weight_kernel,
        grid=(steps,),
        out_shape=(
            jax.ShapeDtypeStruct((width, hidden), F32),
            jax.ShapeDtypeStruct((width, hidden), F32),
            jax.ShapeDtypeStruct((hidden, width), F32),
        )
        + tuple(jax.ShapeDtypeStruct(v.shape, v.dtype) for v in (go, gq, gk, gv)),
        in_specs=[slice_x, slice_in, whole, whole, whole_t] + small,
        out_specs=[tall, tall, pl.BlockSpec((hidden, tile), lambda i: (0, i))] + small,
        compiler_params=pltpu.CompilerParams(vmem_limit_bytes=62 << 20),
        name="weights",
    )(xt, c, gg, ug, act, go, gq, gk, gv)


def shards(
    moe_input,
    cotangent,
    routes,
    route_weights,
    gate_weight,
    up_weight,
    down_weight,
    out_weight,
    mixer_output,
    queries,
    key_vectors,
    value_vectors,
    log_decay,
    block_states,
):
    outs = expert_call(
        routes.T, route_weights.T, moe_input, cotangent, log_decay.T, block_states,
        gate_weight[0], up_weight[0], down_weight[0], out_weight, mixer_output,
        queries, key_vectors, value_vectors,
    )
    grads = weight_call(*outs, steps=WEIGHT_STEPS)
    return tuple(g[None] for g in grads[:3]) + tuple(grads[3:])


def solution(mesh):
    return jax.shard_map(
        shards,
        mesh=mesh,
        in_specs=(
            P(SP, None),
            P(SP, None),
            P(SP, None),
            P(SP, None),
            P(SP, None, "tp"),
            P(SP, None, "tp"),
            P(SP, "tp", None),
            P(None, "tp"),
            P(SP, "tp"),
            P(SP, "tp"),
            P(SP, "tp"),
            P(SP, "tp"),
            P(SP, "tp"),
            P(SP, "tp", None, None),
        ),
        out_specs=(
            P(SP, None, "tp"),
            P(SP, None, "tp"),
            P(SP, "tp", None),
            P(SP, "tp"),
            P(SP, "tp"),
            P(SP, "tp"),
            P(SP, "tp"),
        ),
        check_vma=False,
    )
```

```python
import jax
import jax.numpy as jnp
from jax import lax
from jax.sharding import PartitionSpec as P
from jax.experimental import pallas as pl
from jax.experimental.pallas import tpu as pltpu

SP = "sp"
WEIGHT_STEPS = 4


clamp_limit = 7.0
sigmoid_sharpness = 1.702


MAIN = 16
LEFT = 4
LANES = 128
BF = jnp.bfloat16
F32 = jnp.float32
MESH_ID = pl.DeviceIdType.MESH


def dot(a, b):
    return jnp.dot(a, b, preferred_element_type=F32)


def dot_t(a, b):
    return lax.dot_general(a, b, (((1,), (1,)), ((), ())), preferred_element_type=F32)


def t_dot(a, b):
    return lax.dot_general(a, b, (((0,), (0,)), ((), ())), preferred_element_type=F32)


def iota(shape, dim):
    return lax.broadcasted_iota(jnp.int32, shape, dim)


def expert_kernel(
    routes_h, weights_h, x_h, cot_h, ld_h, st_h, wg_h, wu_h, wd_h, ow_h, mix_h, q_h, k_h, v_h,
    xt_h, c_h, gg_h, ug_h, act_h, go_out, gq_out, gk_out, gv_out,
    xt_out, act_out, gg_out, ug_out, o_sem, tails, xs, wg, wu, wd, acc, half_out, ip, far_in, near_in, ret_t, ret_q, res,
    w_sem, a_send, a_recv, l_send, l_recv, g_send, g_recv, rs_send, rs_recv, t_send, t_recv, r_send, r_recv,
    ow, mix, qkv, cum, cum_t, decay, score, logs, gm, gmb, outer, local, part, peer, got,
    ybuf, zbuf, lt_send, lt_recv, d_send, d_recv, b_send, b_recv, sc_send, sc_recv,
    sy_send, sy_recv, sz_send, sz_recv, cbuf,
    routes, weights, xq, cq, ld_ref, st_ref, sent, sent_left, stacks, pm_ref, pl_ref, e_sem,
    stack_sem,
):
    n_sp, n_tp = lax.axis_size("sp"), lax.axis_size("tp")
    me, tp = lax.axis_index("sp"), lax.axis_index("tp")
    nxt, prv, far = lax.rem(tp + 1, n_tp), lax.rem(tp + n_tp - 1, n_tp), lax.rem(tp + 2, n_tp)
    share = wg.shape[0] // n_tp
    wide = share + LANES
    hidden = wg.shape[1]
    hs = n_sp // 2 * MAIN
    hx = n_sp // 2 * (MAIN + LEFT)
    hl = n_sp // 2 * LEFT

    def at(k, width):
        return pl.ds(pl.multiple_of(k * width, LANES), width)

    def slab(k):
        return pl.ds(pl.multiple_of(k * MAIN, MAIN), MAIN)

    def main_slab(k):
        return pl.ds(pl.multiple_of(k * MAIN + k // (n_sp // 2) * hl, MAIN), MAIN)

    groups = MAIN // LEFT

    mine_cols = at(tp, share)
    early = [
        pltpu.make_async_copy(src, dst, e_sem.at[i])
        for i, (src, dst) in enumerate(
            (
                (routes_h, routes), (x_h.at[:, mine_cols], xq), (weights_h, weights),
                (cot_h.at[:, mine_cols], cq), (ld_h, ld_ref), (st_h, st_ref),
            )
        )
    ]
    for load in early:
        load.start()
    toks = pm_ref.shape[1]
    stack_loads = [
        pltpu.make_async_copy(
            src.at[:, pl.ds(k * share + g * LANES, LANES)],
            stacks.at[a, pl.ds(g * toks, toks), pl.ds(k * LANES, LANES)],
            stack_sem.at[a, k * groups + g],
        )
        for a, src in enumerate((x_h, cot_h))
        for k in range(n_tp)
        for g in range(groups)
    ]
    for load in stack_loads:
        load.start()
    loads = [
        pltpu.make_async_copy(src, dst, w_sem.at[i])
        for i, (src, dst) in enumerate(
            ((wg_h, wg), (wu_h, wu), (wd_h, wd), (ow_h, ow), (mix_h, mix))
            + tuple((src, qkv.at[j]) for j, src in enumerate((q_h, k_h, v_h)))
        )
    ]
    for load in loads:
        load.start()

    barrier = pltpu.get_barrier_semaphore()

    def greet(i, carry):
        pl.semaphore_signal(
            barrier, inc=1, device_id={"sp": lax.rem(me + i, n_sp)}, device_id_type=MESH_ID
        )
        return carry

    lax.fori_loop(1, n_sp, greet, 0)
    for k in (nxt, prv):
        pl.semaphore_signal(barrier, inc=1, device_id={"tp": k}, device_id_type=MESH_ID)

    rows_all = pm_ref.shape[0]
    e = iota((n_sp, toks), 0)
    early[0].wait()
    first = routes[0:1, :] == e
    second = routes[1:2, :] == e
    chosen = first | second
    before = (iota((toks, toks), 0) < iota((toks, toks), 1)).astype(F32).astype(BF)
    ranks = jnp.where(chosen, dot(chosen.astype(F32).astype(BF), before), -1.0).astype(BF)
    owner = (iota((rows_all, n_sp), 0) // MAIN == iota((rows_all, n_sp), 1)).astype(F32).astype(BF)
    spread = dot(owner, ranks).astype(jnp.int32)
    place = iota((rows_all, toks), 0) % MAIN
    is_main = spread == place
    is_left = spread == MAIN + place % LEFT
    pm_ref[...] = is_main.astype(F32).astype(BF)
    pl_ref[...] = is_left.astype(F32).astype(BF)
    early[1].wait()
    sent[0] = dot(pm_ref[...], xq[...]).astype(BF)
    pl.semaphore_wait(barrier, n_sp + 1)

    def spread_out(src, landing, send_sem, recv_sem):
        def deliver(i, carry):
            e = lax.rem(me + i, n_sp)
            pltpu.make_async_remote_copy(
                src_ref=src.at[slab(e), :],
                dst_ref=landing,
                send_sem=send_sem,
                recv_sem=recv_sem,
                device_id={"sp": e},
                device_id_type=MESH_ID,
            ).start()
            return carry

        lax.fori_loop(1, n_sp, deliver, 0)

    def dispatch(a):
        landing = xs.at[a, main_slab(me), at(tp, share)]
        spread_out(sent.at[a], landing, a_send.at[a], a_recv.at[a, me // (n_sp // 2)])
        xs[a, main_slab(me), at(tp, share)] = sent[a, slab(me), :]

    def dispatch_left(a):
        spread_out(sent_left.at[a], tails.at[a, slab(me), :], l_send.at[a], l_recv.at[a])
        tails[a, slab(me), :] = sent_left[a, slab(me), :]

    dispatch(0)
    early[2].wait()
    early[3].wait()
    w = jnp.where(first, weights[0:1, :], 0.0) + jnp.where(second, weights[1:2, :], 0.0)
    w_rows = jnp.zeros((rows_all, toks), F32)
    for _ in range(3):
        piece = w.astype(BF)
        w_rows = w_rows + dot(owner, piece)
        w = w - piece.astype(F32)
    w_main = jnp.sum(jnp.where(is_main, w_rows, 0.0), axis=1, keepdims=True)
    w_left = jnp.sum(jnp.where(is_left, w_rows, 0.0), axis=1, keepdims=True)
    sent[1] = (w_main * dot(pm_ref[...], cq[...])).astype(BF)
    dispatch(1)
    row_group = (iota((rows_all, toks), 0) % MAIN) // LEFT
    p_left = pl_ref[...]
    p_wide = jnp.concatenate(
        [jnp.where(row_group == g, p_left, jnp.zeros_like(p_left)) for g in range(groups)], axis=1
    )
    for load in stack_loads:
        load.wait()
    sent_left[0] = dot(p_wide, stacks[0]).astype(BF)
    dispatch_left(0)
    sent_left[1] = (w_left * dot(p_wide, stacks[1])).astype(BF)
    dispatch_left(1)
    early[4].wait()
    early[5].wait()

    blk = toks // 2
    pairs = share // LANES
    core, y_at, z_at = lax.rem(me, 2), lax.rem(me // 2, 4), me // 8

    def pieces(v):
        out = []
        for _ in range(3):
            p = v.astype(BF)
            out.append(p)
            v = v - p.astype(F32)
        return out

    heads = ld_ref.shape[0]
    lane_head = (iota((heads, share), 1) // (share // heads) == iota((heads, share), 0)).astype(
        F32
    ).astype(BF)
    lower = (iota((blk, blk), 0) >= iota((blk, blk), 1)).astype(F32).astype(BF)
    upper = (iota((blk, blk), 0) <= iota((blk, blk), 1)).astype(F32).astype(BF)
    for b in range(2):
        steps = pieces(ld_ref[:, b * blk : (b + 1) * blk])
        cum_t[b * heads : (b + 1) * heads, :] = sum(dot(p, upper) for p in steps)
        cum[b * blk : (b + 1) * blk, :] = sum(
            dot(lower, t_dot(p, lane_head).astype(BF)) for p in steps
        )
    ends = [cum[(b + 1) * blk - 1 : (b + 1) * blk, :] for b in range(2)]

    def by_pair(row):
        return jnp.concatenate(
            [row[:, p * LANES : (p + 1) * LANES] for p in range(pairs)], axis=0
        )

    both_ends = by_pair(ends[0] + ends[1])
    logs[me] = jnp.concatenate([both_ends, jnp.zeros_like(both_ends)], axis=0)

    def tell(i, carry):
        pltpu.make_async_remote_copy(
            src_ref=logs.at[me],
            dst_ref=logs.at[me],
            send_sem=lt_send.at[0],
            recv_sem=lt_recv.at[0],
            device_id={"sp": lax.rem(me + i, n_sp)},
            device_id_type=MESH_ID,
        ).start()
        return carry

    lax.fori_loop(1, n_sp, tell, 0)
    for load in loads[4:]:
        load.wait()
    low_lane = iota((1, LANES), 1) < LANES // 2
    causal = iota((blk, blk), 0) >= iota((blk, blk), 1)

    def spot(i):
        b, p = i // pairs, lax.rem(i, pairs)
        return pl.ds(pl.multiple_of(b * blk, blk), blk), at(p, LANES), b, p

    def side(v, hh):
        return jnp.where(low_lane if hh == 0 else ~low_lane, v, jnp.zeros_like(v))

    @pl.loop(0, 2 * pairs)
    def _(i):
        rows, cols, b, p = spot(i)
        q, k = qkv[0, rows, cols], qkv[1, rows, cols]
        c = cum[rows, cols]
        for hh in range(2):
            column = c[:, hh * (LANES // 2) : hh * (LANES // 2) + 1]
            row = cum_t[pl.ds(b * heads + p * 2 + hh, 1), :]
            d = jnp.where(causal, jnp.exp(jnp.minimum(column - row, 0.0)), 0.0)
            decay[i * 2 + hh] = d
            score[i * 2 + hh] = (dot_t(q, side(k, hh)) * d).astype(BF)

    def tp_copy(ref, dst, sends, recvs, i, k):
        return pltpu.make_async_remote_copy(
            src_ref=ref, dst_ref=dst, send_sem=sends.at[i], recv_sem=recvs.at[i],
            device_id={"tp": k}, device_id_type=MESH_ID,
        )

    def ring_copies(view, sends, recvs):
        def move(h, k, i, to):
            return tp_copy(view(h, k), view(h, k), sends, recvs, i, to)

        return [
            move(0, tp, 0, nxt), move(1, tp, 1, nxt), move(0, tp, 2, prv), move(1, tp, 3, prv),
            move(0, prv, 4, nxt), move(1, nxt, 5, prv),
        ]

    jj = iota((hs, hs), 0)
    qq = iota((hs, hs), 1)
    unpick = (
        qq == ((jj % hl) // LEFT) * MAIN + (jj // hl) * LEFT + jj % LEFT
    ).astype(F32).astype(BF)
    pick = (
        qq == ((jj % MAIN) // LEFT) * hl + (jj // MAIN) * LEFT + jj % LEFT
    ).astype(F32).astype(BF)
    def unpack(a):
        ref = tails.at[a, pl.ds(0, (n_sp - 1) * MAIN), :]
        pltpu.make_async_copy(ref, ref, l_recv.at[a]).wait()
        for h in range(2):
            spread = dot(unpick, tails[a, h * hs : (h + 1) * hs, :]).astype(BF)
            for k in range(n_tp):
                for g in range(groups):
                    lanes = pl.ds(k * share + g * LANES, LANES)
                    xs[a, h * hx + hs : (h + 1) * hx, lanes] = spread[
                        g * hl : (g + 1) * hl, k * LANES : (k + 1) * LANES
                    ]

    def piece_in(k, h):
        rows = pl.ds(h * hx, hs)
        x = xs[0, rows, at(k, share)]
        for i, w in ((0, wg), (1, wu)):
            y = dot(x, w[at(k, share), :])
            acc[i, rows, :] = y if k is tp else acc[i, rows, :] + y

    def left_in():
        unpack(0)
        for h in range(2):
            rows = pl.ds(h * hx + hs, hl)
            x = xs[0, rows, :]
            acc[0, rows, :] = dot(x, wg[...])
            acc[1, rows, :] = dot(x, wu[...])

    def piece_gr(k, h):
        rows = pl.ds(h * hx, hs)
        y = dot_t(xs[1, rows, at(k, share)], wd[:, at(k, share)])
        acc[2, rows, :] = y if k is tp else acc[2, rows, :] + y

    def left_gr():
        unpack(1)
        for h in range(2):
            rows = pl.ds(h * hx + hs, hl)
            acc[2, rows, :] = dot_t(xs[1, rows, :], wd[...])

    rings = [
        [
            ring_copies(
                lambda sub, k, a=a, h=h: xs.at[
                    a, pl.ds(h * hx + sub * (hs // 2), hs // 2), at(k, share)
                ],
                g_send.at[a, h], g_recv.at[a, h],
            )
            for h in range(2)
        ]
        for a in range(2)
    ]

    def wait_arrivals(a, h):
        for inside in range(2):

            @pl.when((me // (n_sp // 2) == h) == (inside == 1))
            def _():
                ref = xs.at[a, pl.ds(h * hx, hs - inside * MAIN), at(tp, share)]
                pltpu.make_async_copy(ref, ref, a_recv.at[a, h]).wait()

    def ring_begin(ring):
        for i in (0, 3, 1, 2):
            ring[i].start()

    def ring_relay(ring):
        ring[0].wait_recv()
        ring[4].start()
        ring[3].wait_recv()
        ring[5].start()

    def begin(a, h):
        wait_arrivals(a, h)
        ring_begin(rings[a][h])

    def near_pieces(a, h):
        rings[a][h][1].wait_recv()
        (piece_in, piece_gr)[a](prv, h)
        rings[a][h][2].wait_recv()
        (piece_in, piece_gr)[a](nxt, h)

    def far_piece(a, h):
        rings[a][h][4].wait_recv()
        rings[a][h][5].wait_recv()
        (piece_in, piece_gr)[a](far, h)

    step = 2 * MAIN

    def forward_half(h):
        @pl.loop(0, hx // step)
        def _(i):
            rows = pl.ds(pl.multiple_of(h * hx + i * step, step), step)
            gate, up = acc[0, rows, :], acc[1, rows, :]
            clamped = jnp.minimum(gate, clamp_limit)
            logistic = 1.0 / (1.0 + jnp.exp(-sigmoid_sharpness * clamped))
            linear = jnp.clip(up, -clamp_limit, clamp_limit) + 1.0
            swish = clamped * logistic
            half_out[rows, :] = (swish * linear).astype(BF)
            slope = logistic + sigmoid_sharpness * swish * (1.0 - logistic)
            acc[0, rows, :] = jnp.where(gate < clamp_limit, linear * slope, 0.0)
            acc[1, rows, :] = jnp.where(jnp.abs(up) < clamp_limit, swish, 0.0)

    def backward_half(h):
        @pl.loop(0, hx // step)
        def _(i):
            rows = pl.ds(pl.multiple_of(h * hx + i * step, step), step)
            act_grad = acc[2, rows, :]
            gg_out[rows, :] = (act_grad * acc[0, rows, :]).astype(BF)
            ug_out[rows, :] = (act_grad * acc[1, rows, :]).astype(BF)

    def expert_part(k, slot, h):
        rows = pl.ds(h * hx, hx)
        y = dot_t(gg_out[rows, :], wg[at(k, share), :])
        y = y + dot_t(ug_out[rows, :], wu[at(k, share), :])
        ip[slot, rows, :] = y.astype(BF)

    def sums(h):
        subs = [pl.ds(h * hx + sub * (hx // 2), hx // 2) for sub in range(2)]

        def rs_copy(src, dst, i, k):
            return tp_copy(src, dst, rs_send.at[h], rs_recv.at[h], i, k)

        return subs, [
            rs_copy(ip.at[0, subs[0]], far_in.at[h, 0], 0, nxt),
            rs_copy(ip.at[0, subs[1]], far_in.at[h, 1], 1, prv),
            rs_copy(ip.at[1, subs[1]], near_in.at[0, subs[1]], 2, nxt),
            rs_copy(ip.at[2, subs[0]], near_in.at[1, subs[0]], 3, prv),
            rs_copy(ip.at[1, subs[0]], near_in.at[0, subs[0]], 4, nxt),
            rs_copy(ip.at[2, subs[1]], near_in.at[1, subs[1]], 5, prv),
        ]

    reduces = [sums(h) for h in range(2)]

    def parts(h):
        for slot, k in enumerate((far, nxt, prv)):
            expert_part(k, slot, h)

    def send_parts(h):
        for copy in reduces[h][1][:4]:
            copy.start()

    def augment(h):
        subs, rs = reduces[h]
        for i in range(2):
            rs[i].wait_recv()
            ip[1 + i, subs[i], :] = (
                ip[1 + i, subs[i], :].astype(F32) + far_in[h, i].astype(F32)
            ).astype(BF)
            rs[4 + i].start()

    def finish(h):
        for i in range(2, 6):
            reduces[h][1][i].wait_recv()
        rows = pl.ds(h * hx, hx)
        total = (
            ip[3, rows, :].astype(F32)
            + near_in[0, rows, :].astype(F32)
            + near_in[1, rows, :].astype(F32)
        ).astype(BF)
        ret_t[h * hs : (h + 1) * hs, :share] = total[:hs]
        stacked = jnp.concatenate(
            [total[hs:, g * LANES : (g + 1) * LANES] for g in range(groups)], axis=0
        )
        ret_t[h * hs : (h + 1) * hs, share:] = dot(pick, stacked).astype(BF)

        def give_back(i, carry):
            s = h * (n_sp // 2) + lax.rem(me + i, n_sp // 2)

            @pl.when(s != me)
            def _():
                pltpu.make_async_remote_copy(
                    src_ref=ret_t.at[slab(s), :],
                    dst_ref=ret_q.at[slab(me), :],
                    send_sem=t_send.at[0],
                    recv_sem=t_recv.at[0],
                    device_id={"sp": s},
                    device_id_type=MESH_ID,
                ).start()

            return carry

        lax.fori_loop(0, n_sp // 2, give_back, 0)

    begin(0, 0)
    loads[0].wait()
    loads[1].wait()
    piece_in(tp, 0)
    ring_relay(rings[0][0])
    begin(1, 0)
    loads[2].wait()
    piece_gr(tp, 0)
    near_pieces(0, 0)
    ring_relay(rings[1][0])
    begin(0, 1)
    far_piece(0, 0)
    piece_in(tp, 1)
    left_in()
    forward_half(0)
    ring_relay(rings[0][1])
    begin(1, 1)
    near_pieces(1, 0)
    left_gr()
    far_piece(1, 0)
    backward_half(0)
    parts(0)
    ring_relay(rings[1][1])
    send_parts(0)
    piece_gr(tp, 1)
    near_pieces(0, 1)
    far_piece(0, 1)
    forward_half(1)
    expert_part(tp, 3, 0)
    near_pieces(1, 1)
    far_piece(1, 1)
    backward_half(1)
    parts(1)
    augment(0)
    send_parts(1)
    expert_part(tp, 3, 1)

    @pl.loop(0, hidden // LANES)
    def _(i):
        act_out[at(i, LANES), :] = half_out[:, at(i, LANES)].T

    finish(0)

    @pl.loop(0, n_tp * groups)
    def _(i):
        xt_out[at(i, LANES), :] = xs[0, :, at(i, LANES)].T

    augment(1)
    saves = [
        pltpu.make_async_copy(src, dst, o_sem.at[i])
        for i, (src, dst) in enumerate(
            ((xt_out, xt_h), (xs.at[1], c_h), (gg_out, gg_h), (ug_out, ug_h), (act_out, act_h))
        )
    ]
    for save in saves:
        save.start()
    finish(1)
    ret_q[slab(me), :] = ret_t[slab(me), :]
    others = pl.ds(0, (n_sp - 1) * MAIN)
    pltpu.make_async_copy(ret_q.at[others, :], ret_q.at[others, :], t_recv.at[0]).wait()

    p_left = pl_ref[...]
    y = t_dot(pm_ref[...], ret_q[:, :share])
    back = ret_q[:, share:]
    group = (iota(p_left.shape, 0) % MAIN) // LEFT
    y = y + jnp.concatenate(
        [t_dot(jnp.where(group == g, p_left, jnp.zeros_like(p_left)), back) for g in range(groups)],
        axis=1,
    )
    res[:, at(tp, share)] = (cq[...].astype(F32) + y).astype(BF)
    ring = ring_copies(
        lambda h, k: res.at[pl.ds(h * (toks // 2), toks // 2), at(k, share)], r_send, r_recv
    )
    ring_begin(ring)
    block = share // (2 * pairs)
    plane = pairs * block
    partner = me + 1 - 2 * core

    def sp_copy(src, dst, send_sem, recv_sem, e):
        return pltpu.make_async_remote_copy(
            src_ref=src, dst_ref=dst, send_sem=send_sem, recv_sem=recv_sem,
            device_id={"sp": e}, device_id_type=MESH_ID,
        )

    order = (tp, prv, nxt, far)

    def plane_rows(k):
        return pl.ds(pl.multiple_of(k * plane, plane), plane)

    swaps = [
        sp_copy(
            part.at[1 - core, plane_rows(k), :], peer.at[plane_rows(k), :],
            d_send.at[i], d_recv.at[i], partner,
        )
        for i, k in enumerate(order)
    ]

    def piece_mix(i):
        k = order[i]
        y = dot(res[:, at(k, share)], ow[at(k, share), :])
        gm[...] = y if i == 0 else gm[...] + y

    def piece_out(i):
        k = order[i]
        r = res[:, at(k, share)]
        for j in range(pairs):
            g = t_dot(r[:, j * LANES : (j + 1) * LANES], mix[...]).astype(BF)
            for c in range(2):
                part[c, pl.ds(pl.multiple_of(k * plane + j * block, block), block), :] = g[
                    c * block : (c + 1) * block
                ]
        swaps[i].start()

    def piece_res(i):
        piece_out(i)
        piece_mix(i)

    my_block = me // 2

    def send_plane(i):
        k = order[i]
        swaps[i].wait_recv()
        rows = plane_rows(k)
        part[core, rows, :] = (
            part[core, rows, :].astype(F32) + peer[rows, :].astype(F32)
        ).astype(BF)
        for j in range(4):
            zy = k * 4 + lax.rem(y_at + j, 4)

            @pl.when(zy != my_block)
            def _():
                sp_copy(
                    part.at[core, pl.ds(pl.multiple_of(zy * block, block), block), :],
                    got.at[my_block], b_send.at[0], b_recv.at[0], zy * 2 + core,
                ).start()

    loads[3].wait()
    piece_res(0)
    ring_relay(ring)
    ring[1].wait_recv()
    piece_res(1)
    send_plane(0)
    ring[2].wait_recv()
    piece_res(2)
    send_plane(1)
    ring[4].wait_recv()
    ring[5].wait_recv()
    piece_mix(3)
    gmb[...] = gm[...].astype(BF)

    half = LANES // 2

    @pl.loop(0, 2 * pairs)
    def _(i):
        rows, cols, b, p = spot(i)
        q = (qkv[0, rows, cols].astype(F32) * jnp.exp(cum[rows, cols])).astype(BF)
        o = t_dot(q, gmb[rows, cols])
        outer[b, p] = jnp.where(low_lane, o[:half], o[half:])

    def pair_rows(tile):
        return tile[:pairs][:, None, :]

    block_factor = [jnp.exp(by_pair(e))[:, None, :] for e in ends]
    total = block_factor[0] * outer[1] + outer[0]
    local[0] = total.astype(BF)
    swap_state = sp_copy(local.at[0], cbuf, sc_send.at[0], sc_recv.at[0], partner)
    swap_state.start()
    piece_out(3)
    tiles = pl.ds(0, n_sp - 1)
    pltpu.make_async_copy(logs.at[tiles], logs.at[tiles], lt_recv.at[0]).wait()

    def chip_log(z, y):
        return logs[z * 8 + y * 2] + logs[z * 8 + y * 2 + 1]

    later_core_log = logs[me - core + 1]
    earlier_core_log = logs[me - core]

    swap_state.wait_recv()
    mine, others_total = local[0].astype(F32), cbuf[...].astype(F32)
    early = jnp.where(core == 0, mine, others_total)
    late = jnp.where(core == 0, others_total, mine)
    chip_total = jnp.exp(pair_rows(earlier_core_log)) * late + early
    ybuf[y_at] = chip_total.astype(BF)
    y_sends = [
        sp_copy(
            ybuf.at[y_at], ybuf.at[y_at], sy_send.at[i - 1], sy_recv.at[i - 1],
            z_at * 8 + lax.rem(y_at + i, 4) * 2 + core,
        )
        for i in range(1, 4)
    ]
    for copy in y_sends:
        copy.start()
    send_plane(2)

    send_plane(3)
    for copy in y_sends:
        copy.wait_recv()
    inside_y = jnp.zeros_like(total)
    plane_total = jnp.zeros_like(total)
    later_y = jnp.zeros((2 * pairs, LANES), F32)
    for y in (3, 2, 1, 0):
        log = chip_log(z_at, y)
        factor = jnp.exp(pair_rows(log))
        t = ybuf[y].astype(F32)
        inside_y = jnp.where(y > y_at, factor * inside_y + t, inside_y)
        later_y = jnp.where(y > y_at, later_y + log, later_y)
        plane_total = factor * plane_total + t
    local[1] = plane_total.astype(BF)
    z_sends = [
        sp_copy(local.at[1], zbuf.at[i - 1], sz_send.at[i - 1], sz_recv.at[i - 1], me - i * 8)
        for i in range(1, 4)
    ]
    for i, copy in enumerate(z_sends, 1):

        @pl.when(z_at >= i)
        def _():
            copy.start()

    @pl.loop(0, 2 * pairs)
    def _(i):
        rows, cols, b, p = spot(i)
        q, k, v, g = qkv[0, rows, cols], qkv[1, rows, cols], qkv[2, rows, cols], gmb[rows, cols]
        outs = []
        for hh in range(2):
            wg_ts = (dot_t(g, side(v, hh)) * decay[i * 2 + hh]).astype(BF)
            outs.append((dot(wg_ts, k), t_dot(wg_ts, q), t_dot(score[i * 2 + hh], g)))
        intra = [jnp.where(low_lane, lo, hi) for lo, hi in zip(*outs)]
        st = [st_ref[b, 2 * p + hh] for hh in range(2)]
        none = jnp.zeros_like(st[0])
        full = jnp.concatenate(
            [
                jnp.concatenate([st[0], none], axis=1),
                jnp.concatenate([none, st[1]], axis=1),
            ],
            axis=0,
        )
        carry = dot_t(g, full) * jnp.exp(cum[rows, cols])
        gq_out[rows, cols] = (intra[0] + carry).astype(BF)
        gm[rows, cols] = intra[1]
        acc[0, rows, cols] = intra[2]

    beyond = jnp.zeros_like(total)
    local_state = acc.at[1, pl.ds(0, pairs * half), pl.ds(0, LANES)]
    local_state[...] = jnp.zeros((pairs * half, LANES), F32)
    for i in (3, 2, 1):

        @pl.when(z_at + i < 4)
        def _():
            z_sends[i - 1].wait_recv()
            log = sum(chip_log(z_at + i, y) for y in range(4))
            now = local_state[...].reshape(pairs, half, LANES)
            now = jnp.exp(pair_rows(log)) * now + zbuf[i - 1].astype(F32)
            local_state[...] = now.reshape(pairs * half, LANES)

    beyond = local_state[...].reshape(pairs, half, LANES)
    entering_state = jnp.exp(pair_rows(later_y)) * beyond + inside_y
    entering_state = jnp.where(
        core == 0, jnp.exp(pair_rows(later_core_log)) * entering_state + late, entering_state
    )
    carried = (block_factor[1] * entering_state + outer[1], entering_state)
    for b in range(2):
        outer[b] = carried[b]

    @pl.loop(0, 2 * pairs)
    def _(i):
        rows, cols, b, p = spot(i)
        k, v = qkv[1, rows, cols], qkv[2, rows, cols]
        st = outer[b, p].astype(BF)
        full = jnp.concatenate([side(st, 0), side(st, 1)], axis=0)
        c = cum[rows, cols]
        to_end = jnp.exp(c[blk - 1 : blk, :] - c)
        gk_out[rows, cols] = (gm[rows, cols] + dot_t(v, full) * to_end).astype(BF)
        gv_out[rows, cols] = (acc[0, rows, cols] + dot(k, full) * to_end).astype(BF)

    blocks = pl.ds(0, 15)
    pltpu.make_async_copy(got.at[blocks], got.at[blocks], b_recv.at[0]).wait()
    got[my_block] = part[core, pl.ds(pl.multiple_of(my_block * block, block), block), :]
    sums = got[0].astype(F32)
    for i in range(1, 16):
        sums = sums + got[i].astype(F32)
    go_out[...] = sums

    pltpu.make_async_copy(got.at[blocks], got.at[blocks], b_send.at[0]).wait()
    pltpu.make_async_copy(logs.at[tiles], logs.at[tiles], lt_send.at[0]).wait()
    for copy in swaps + [swap_state] + y_sends:
        copy.wait_send()
    for i, copy in enumerate(z_sends, 1):

        @pl.when(z_at >= i)
        def _():
            copy.wait_send()

    for a in range(2):
        for ref, sem in ((sent.at[a, others, :], a_send), (sent_left.at[a, others, :], l_send)):
            pltpu.make_async_copy(ref, ref, sem.at[a]).wait()
        for copy in rings[a][0] + rings[a][1]:
            copy.wait_send()
    for copy in reduces[0][1] + reduces[1][1] + ring:
        copy.wait_send()
    for save in saves:
        save.wait()
    pltpu.make_async_copy(ret_q.at[others, :], ret_q.at[others, :], t_send.at[0]).wait()


def expert_call(
    routes, weights, x, cotangent, log_decay, states, w_gate, w_up, w_down, w_out, mixer,
    queries, key_vectors, value_vectors,
):
    n_sp, n_tp = lax.axis_size("sp"), lax.axis_size("tp")
    width, hidden = w_gate.shape
    share = width // n_tp
    wide = share + LANES
    rows = n_sp * MAIN
    full = n_sp * (MAIN + LEFT)
    toks = cotangent.shape[0]
    anyspace = pl.BlockSpec(memory_space=pl.ANY)
    vmem = pl.BlockSpec(memory_space=pltpu.VMEM)
    dma = pltpu.SemaphoreType.DMA
    return pl.pallas_call(
        expert_kernel,
        out_shape=(
            jax.ShapeDtypeStruct((width, full), BF),
            jax.ShapeDtypeStruct((full, width), BF),
            jax.ShapeDtypeStruct((full, hidden), BF),
            jax.ShapeDtypeStruct((full, hidden), BF),
            jax.ShapeDtypeStruct((hidden, full), BF),
            jax.ShapeDtypeStruct((width // n_sp, share), F32),
            jax.ShapeDtypeStruct((toks, share), BF),
            jax.ShapeDtypeStruct((toks, share), BF),
            jax.ShapeDtypeStruct((toks, share), BF),
        ),
        in_specs=[anyspace] * 14,
        out_specs=[anyspace] * 5 + [vmem] * 4,
        scratch_shapes=[
            pltpu.VMEM((width, full), BF),
            pltpu.VMEM((hidden, full), BF),
            pltpu.VMEM((full, hidden), BF),
            pltpu.VMEM((full, hidden), BF),
            dma((5,)),
            pltpu.VMEM((2, rows, n_tp * LANES), BF),
            pltpu.VMEM((2, full, width), BF),
            pltpu.VMEM(w_gate.shape, BF),
            pltpu.VMEM(w_up.shape, BF),
            pltpu.VMEM(w_down.shape, BF),
            pltpu.VMEM((3, full, hidden), F32),
            pltpu.VMEM((full, hidden), BF),
            pltpu.VMEM((4, full, share), BF),
            pltpu.VMEM((2, 2, full // 4, share), BF),
            pltpu.VMEM((2, full, share), BF),
            pltpu.VMEM((rows, wide), BF),
            pltpu.VMEM((rows, wide), BF),
            pltpu.VMEM((toks, width), BF),
            dma((8,)), dma((2,)), dma((2, 2)), dma((2,)), dma((2,)), dma((2, 2, 6)), dma((2, 2, 6)),
            dma((2, 6)), dma((2, 6)), dma((1,)), dma((1,)), dma((6,)), dma((6,)),
            pltpu.VMEM(w_out.shape, BF),
            pltpu.VMEM(mixer.shape, BF),
            pltpu.VMEM((3, toks, share), BF),
            pltpu.VMEM((toks, share), F32),
            pltpu.VMEM((2 * log_decay.shape[0], toks // 2), F32),
            pltpu.VMEM((16, toks // 2, toks // 2), F32),
            pltpu.VMEM((16, toks // 2, toks // 2), BF),
            pltpu.VMEM((n_sp, 8, LANES), F32),
            pltpu.VMEM((toks, share), F32),
            pltpu.VMEM((toks, share), BF),
            pltpu.VMEM((2, 4, 64, LANES), F32),
            pltpu.VMEM((2, 4, 64, LANES), BF),
            pltpu.VMEM((2, width // 2, share), BF),
            pltpu.VMEM((width // 2, share), BF),
            pltpu.VMEM((16, width // n_sp, share), BF),
            pltpu.VMEM((4, 4, 64, LANES), BF),
            pltpu.VMEM((3, 4, 64, LANES), BF),
            dma((1,)), dma((1,)), dma((4,)), dma((4,)), dma((1,)), dma((1,)), dma((1,)),
            dma((1,)), dma((3,)), dma((3,)), dma((3,)), dma((3,)),
            pltpu.VMEM((4, 64, LANES), BF),
            pltpu.VMEM(routes.shape, jnp.int32),
            pltpu.VMEM(weights.shape, F32),
            pltpu.VMEM((toks, share), BF),
            pltpu.VMEM((toks, share), BF),
            pltpu.VMEM(log_decay.shape, F32),
            pltpu.VMEM(states.shape, BF),
            pltpu.VMEM((2, rows, share), BF),
            pltpu.VMEM((2, rows, n_tp * LANES), BF),
            pltpu.VMEM((2, MAIN // LEFT * toks, n_tp * LANES), BF),
            pltpu.VMEM((rows, toks), BF),
            pltpu.VMEM((rows, toks), BF),
            dma((6,)),
            dma((2, 16)),
        ],
        compiler_params=pltpu.CompilerParams(
            collective_id=0, has_side_effects=True, vmem_limit_bytes=62 << 20
        ),
        cost_estimate=pl.CostEstimate(flops=10**10, bytes_accessed=20 << 20, transcendentals=0),
        name="experts",
    )(
        routes, weights, x, cotangent, log_decay, states, w_gate, w_up, w_down, w_out, mixer,
        queries, key_vectors, value_vectors,
    )


def weight_kernel(
    xt, c, gg, ug, act, go, gq, gk, gv, gate_out, up_out, down_out, go_out, gq_out, gk_out, gv_out
):
    gate_out[...] = dot(xt[...], gg[...])
    up_out[...] = dot(xt[...], ug[...])
    down_out[...] = dot(act[...], c[...])
    go_out[...] = go[...]
    gq_out[...] = gq[...]
    gk_out[...] = gk[...]
    gv_out[...] = gv[...]


def weight_call(xt, c, gg, ug, act, go, gq, gk, gv, steps):
    width, rows = xt.shape
    hidden = gg.shape[1]
    tile = width // steps
    slice_in = pl.BlockSpec((rows, tile), lambda i: (0, i))
    slice_x = pl.BlockSpec((tile, rows), lambda i: (i, 0))
    whole = pl.BlockSpec((rows, hidden), lambda i: (0, 0))
    whole_t = pl.BlockSpec((hidden, rows), lambda i: (0, 0))
    tall = pl.BlockSpec((tile, hidden), lambda i: (i, 0))

    def banded(v):
        return pl.BlockSpec((v.shape[0] // steps, v.shape[1]), lambda i: (i, 0))

    small = [banded(v) for v in (go, gq, gk, gv)]
    return pl.pallas_call(
        weight_kernel,
        grid=(steps,),
        out_shape=(
            jax.ShapeDtypeStruct((width, hidden), F32),
            jax.ShapeDtypeStruct((width, hidden), F32),
            jax.ShapeDtypeStruct((hidden, width), F32),
        )
        + tuple(jax.ShapeDtypeStruct(v.shape, v.dtype) for v in (go, gq, gk, gv)),
        in_specs=[slice_x, slice_in, whole, whole, whole_t] + small,
        out_specs=[tall, tall, pl.BlockSpec((hidden, tile), lambda i: (0, i))] + small,
        compiler_params=pltpu.CompilerParams(vmem_limit_bytes=62 << 20),
        name="weights",
    )(xt, c, gg, ug, act, go, gq, gk, gv)


def shards(
    moe_input,
    cotangent,
    routes,
    route_weights,
    gate_weight,
    up_weight,
    down_weight,
    out_weight,
    mixer_output,
    queries,
    key_vectors,
    value_vectors,
    log_decay,
    block_states,
):
    outs = expert_call(
        routes.T, route_weights.T, moe_input, cotangent, log_decay.T, block_states,
        gate_weight[0], up_weight[0], down_weight[0], out_weight, mixer_output,
        queries, key_vectors, value_vectors,
    )
    grads = weight_call(*outs, steps=WEIGHT_STEPS)
    return tuple(g[None] for g in grads[:3]) + tuple(grads[3:])


def solution(mesh):
    return jax.shard_map(
        shards,
        mesh=mesh,
        in_specs=(
            P(SP, None),
            P(SP, None),
            P(SP, None),
            P(SP, None),
            P(SP, None, "tp"),
            P(SP, None, "tp"),
            P(SP, "tp", None),
            P(None, "tp"),
            P(SP, "tp"),
            P(SP, "tp"),
            P(SP, "tp"),
            P(SP, "tp"),
            P(SP, "tp"),
            P(SP, "tp", None, None),
        ),
        out_specs=(
            P(SP, None, "tp"),
            P(SP, None, "tp"),
            P(SP, "tp", None),
            P(SP, "tp"),
            P(SP, "tp"),
            P(SP, "tp"),
            P(SP, "tp"),
        ),
        check_vma=False,
    )
```

```python
import jax
import jax.numpy as jnp
from jax import lax
from jax.sharding import PartitionSpec as P
from jax.experimental import pallas as pl
from jax.experimental.pallas import tpu as pltpu

SP = "sp"
WEIGHT_STEPS = 2


clamp_limit = 7.0
sigmoid_sharpness = 1.702


MAIN = 16
LEFT = 4
LANES = 128
BF = jnp.bfloat16
F32 = jnp.float32
MESH_ID = pl.DeviceIdType.MESH


def dot(a, b):
    return jnp.dot(a, b, preferred_element_type=F32)


def dot_t(a, b):
    return lax.dot_general(a, b, (((1,), (1,)), ((), ())), preferred_element_type=F32)


def t_dot(a, b):
    return lax.dot_general(a, b, (((0,), (0,)), ((), ())), preferred_element_type=F32)


def iota(shape, dim):
    return lax.broadcasted_iota(jnp.int32, shape, dim)


def expert_kernel(
    routes_h, weights_h, x_h, cot_h, ld_h, st_h, wg_h, wu_h, wd_h, ow_h, mix_h, q_h, k_h, v_h,
    xt_h, c_h, gg_h, ug_h, act_h, go_out, gq_out, gk_out, gv_out,
    xt_out, act_out, gg_out, ug_out, o_sem, tails, xs, wg, wu, wd, acc, half_out, ip, far_in, near_in, ret_t, ret_q, res,
    w_sem, a_send, a_recv, l_send, l_recv, g_send, g_recv, rs_send, rs_recv, t_send, t_recv, r_send, r_recv,
    ow, mix, qkv, cum, cum_t, decay, score, logs, gm, gmb, outer, local, part, peer, got,
    ybuf, zbuf, lt_send, lt_recv, d_send, d_recv, b_send, b_recv, sc_send, sc_recv,
    sy_send, sy_recv, sz_send, sz_recv, cbuf,
    routes, weights, xq, cq, ld_ref, st_ref, sent, sent_left, stacks, pm_ref, pl_ref, e_sem,
    stack_sem,
):
    n_sp, n_tp = lax.axis_size("sp"), lax.axis_size("tp")
    me, tp = lax.axis_index("sp"), lax.axis_index("tp")
    nxt, prv, far = lax.rem(tp + 1, n_tp), lax.rem(tp + n_tp - 1, n_tp), lax.rem(tp + 2, n_tp)
    share = wg.shape[0] // n_tp
    wide = share + LANES
    hidden = wg.shape[1]
    hs = n_sp // 2 * MAIN
    hx = n_sp // 2 * (MAIN + LEFT)
    hl = n_sp // 2 * LEFT

    def at(k, width):
        return pl.ds(pl.multiple_of(k * width, LANES), width)

    def slab(k):
        return pl.ds(pl.multiple_of(k * MAIN, MAIN), MAIN)

    def main_slab(k):
        return pl.ds(pl.multiple_of(k * MAIN + k // (n_sp // 2) * hl, MAIN), MAIN)

    groups = MAIN // LEFT

    mine_cols = at(tp, share)
    early = [
        pltpu.make_async_copy(src, dst, e_sem.at[i])
        for i, (src, dst) in enumerate(
            (
                (routes_h, routes), (x_h.at[:, mine_cols], xq), (weights_h, weights),
                (cot_h.at[:, mine_cols], cq), (ld_h, ld_ref), (st_h, st_ref),
            )
        )
    ]
    for load in early:
        load.start()
    toks = pm_ref.shape[1]
    stack_loads = [
        pltpu.make_async_copy(
            src.at[:, pl.ds(k * share + g * LANES, LANES)],
            stacks.at[a, pl.ds(g * toks, toks), pl.ds(k * LANES, LANES)],
            stack_sem.at[a, k * groups + g],
        )
        for a, src in enumerate((x_h, cot_h))
        for k in range(n_tp)
        for g in range(groups)
    ]
    for load in stack_loads:
        load.start()
    loads = [
        pltpu.make_async_copy(src, dst, w_sem.at[i])
        for i, (src, dst) in enumerate(
            ((wg_h, wg), (wu_h, wu), (wd_h, wd), (ow_h, ow), (mix_h, mix))
            + tuple((src, qkv.at[j]) for j, src in enumerate((q_h, k_h, v_h)))
        )
    ]
    for load in loads:
        load.start()

    barrier = pltpu.get_barrier_semaphore()

    def greet(i, carry):
        pl.semaphore_signal(
            barrier, inc=1, device_id={"sp": lax.rem(me + i, n_sp)}, device_id_type=MESH_ID
        )
        return carry

    lax.fori_loop(1, n_sp, greet, 0)
    for k in (nxt, prv):
        pl.semaphore_signal(barrier, inc=1, device_id={"tp": k}, device_id_type=MESH_ID)

    rows_all = pm_ref.shape[0]
    e = iota((n_sp, toks), 0)
    early[0].wait()
    first = routes[0:1, :] == e
    second = routes[1:2, :] == e
    chosen = first | second
    before = (iota((toks, toks), 0) < iota((toks, toks), 1)).astype(F32).astype(BF)
    ranks = jnp.where(chosen, dot(chosen.astype(F32).astype(BF), before), -1.0).astype(BF)
    owner = (iota((rows_all, n_sp), 0) // MAIN == iota((rows_all, n_sp), 1)).astype(F32).astype(BF)
    spread = dot(owner, ranks).astype(jnp.int32)
    place = iota((rows_all, toks), 0) % MAIN
    is_main = spread == place
    is_left = spread == MAIN + place % LEFT
    pm_ref[...] = is_main.astype(F32).astype(BF)
    pl_ref[...] = is_left.astype(F32).astype(BF)
    early[1].wait()
    sent[0] = dot(pm_ref[...], xq[...]).astype(BF)
    pl.semaphore_wait(barrier, n_sp + 1)

    def spread_out(src, landing, send_sem, recv_sem):
        def deliver(i, carry):
            e = lax.rem(me + i, n_sp)
            pltpu.make_async_remote_copy(
                src_ref=src.at[slab(e), :],
                dst_ref=landing,
                send_sem=send_sem,
                recv_sem=recv_sem,
                device_id={"sp": e},
                device_id_type=MESH_ID,
            ).start()
            return carry

        lax.fori_loop(1, n_sp, deliver, 0)

    def dispatch(a):
        landing = xs.at[a, main_slab(me), at(tp, share)]
        spread_out(sent.at[a], landing, a_send.at[a], a_recv.at[a, me // (n_sp // 2)])
        xs[a, main_slab(me), at(tp, share)] = sent[a, slab(me), :]

    def dispatch_left(a):
        spread_out(sent_left.at[a], tails.at[a, slab(me), :], l_send.at[a], l_recv.at[a])
        tails[a, slab(me), :] = sent_left[a, slab(me), :]

    dispatch(0)
    early[2].wait()
    early[3].wait()
    w = jnp.where(first, weights[0:1, :], 0.0) + jnp.where(second, weights[1:2, :], 0.0)
    w_rows = jnp.zeros((rows_all, toks), F32)
    for _ in range(3):
        piece = w.astype(BF)
        w_rows = w_rows + dot(owner, piece)
        w = w - piece.astype(F32)
    w_main = jnp.sum(jnp.where(is_main, w_rows, 0.0), axis=1, keepdims=True)
    w_left = jnp.sum(jnp.where(is_left, w_rows, 0.0), axis=1, keepdims=True)
    sent[1] = (w_main * dot(pm_ref[...], cq[...])).astype(BF)
    dispatch(1)
    row_group = (iota((rows_all, toks), 0) % MAIN) // LEFT
    p_left = pl_ref[...]
    p_wide = jnp.concatenate(
        [jnp.where(row_group == g, p_left, jnp.zeros_like(p_left)) for g in range(groups)], axis=1
    )
    for load in stack_loads:
        load.wait()
    sent_left[0] = dot(p_wide, stacks[0]).astype(BF)
    dispatch_left(0)
    sent_left[1] = (w_left * dot(p_wide, stacks[1])).astype(BF)
    dispatch_left(1)
    early[4].wait()
    early[5].wait()

    blk = toks // 2
    pairs = share // LANES
    core, y_at, z_at = lax.rem(me, 2), lax.rem(me // 2, 4), me // 8

    def pieces(v):
        out = []
        for _ in range(3):
            p = v.astype(BF)
            out.append(p)
            v = v - p.astype(F32)
        return out

    heads = ld_ref.shape[0]
    lane_head = (iota((heads, share), 1) // (share // heads) == iota((heads, share), 0)).astype(
        F32
    ).astype(BF)
    lower = (iota((blk, blk), 0) >= iota((blk, blk), 1)).astype(F32).astype(BF)
    upper = (iota((blk, blk), 0) <= iota((blk, blk), 1)).astype(F32).astype(BF)
    for b in range(2):
        steps = pieces(ld_ref[:, b * blk : (b + 1) * blk])
        cum_t[b * heads : (b + 1) * heads, :] = sum(dot(p, upper) for p in steps)
        cum[b * blk : (b + 1) * blk, :] = sum(
            dot(lower, t_dot(p, lane_head).astype(BF)) for p in steps
        )
    ends = [cum[(b + 1) * blk - 1 : (b + 1) * blk, :] for b in range(2)]

    def by_pair(row):
        return jnp.concatenate(
            [row[:, p * LANES : (p + 1) * LANES] for p in range(pairs)], axis=0
        )

    both_ends = by_pair(ends[0] + ends[1])
    logs[me] = jnp.concatenate([both_ends, jnp.zeros_like(both_ends)], axis=0)

    def tell(i, carry):
        pltpu.make_async_remote_copy(
            src_ref=logs.at[me],
            dst_ref=logs.at[me],
            send_sem=lt_send.at[0],
            recv_sem=lt_recv.at[0],
            device_id={"sp": lax.rem(me + i, n_sp)},
            device_id_type=MESH_ID,
        ).start()
        return carry

    lax.fori_loop(1, n_sp, tell, 0)
    for load in loads[4:]:
        load.wait()
    low_lane = iota((1, LANES), 1) < LANES // 2
    causal = iota((blk, blk), 0) >= iota((blk, blk), 1)

    def spot(i):
        b, p = i // pairs, lax.rem(i, pairs)
        return pl.ds(pl.multiple_of(b * blk, blk), blk), at(p, LANES), b, p

    def side(v, hh):
        return jnp.where(low_lane if hh == 0 else ~low_lane, v, jnp.zeros_like(v))

    @pl.loop(0, 2 * pairs)
    def _(i):
        rows, cols, b, p = spot(i)
        q, k = qkv[0, rows, cols], qkv[1, rows, cols]
        c = cum[rows, cols]
        for hh in range(2):
            column = c[:, hh * (LANES // 2) : hh * (LANES // 2) + 1]
            row = cum_t[pl.ds(b * heads + p * 2 + hh, 1), :]
            d = jnp.where(causal, jnp.exp(jnp.minimum(column - row, 0.0)), 0.0)
            decay[i * 2 + hh] = d
            score[i * 2 + hh] = (dot_t(q, side(k, hh)) * d).astype(BF)

    def tp_copy(ref, dst, sends, recvs, i, k):
        return pltpu.make_async_remote_copy(
            src_ref=ref, dst_ref=dst, send_sem=sends.at[i], recv_sem=recvs.at[i],
            device_id={"tp": k}, device_id_type=MESH_ID,
        )

    def ring_copies(view, sends, recvs):
        def move(h, k, i, to):
            return tp_copy(view(h, k), view(h, k), sends, recvs, i, to)

        return [
            move(0, tp, 0, nxt), move(1, tp, 1, nxt), move(0, tp, 2, prv), move(1, tp, 3, prv),
            move(0, prv, 4, nxt), move(1, nxt, 5, prv),
        ]

    jj = iota((hs, hs), 0)
    qq = iota((hs, hs), 1)
    unpick = (
        qq == ((jj % hl) // LEFT) * MAIN + (jj // hl) * LEFT + jj % LEFT
    ).astype(F32).astype(BF)
    pick = (
        qq == ((jj % MAIN) // LEFT) * hl + (jj // MAIN) * LEFT + jj % LEFT
    ).astype(F32).astype(BF)
    def unpack(a):
        ref = tails.at[a, pl.ds(0, (n_sp - 1) * MAIN), :]
        pltpu.make_async_copy(ref, ref, l_recv.at[a]).wait()
        for h in range(2):
            spread = dot(unpick, tails[a, h * hs : (h + 1) * hs, :]).astype(BF)
            for k in range(n_tp):
                for g in range(groups):
                    lanes = pl.ds(k * share + g * LANES, LANES)
                    xs[a, h * hx + hs : (h + 1) * hx, lanes] = spread[
                        g * hl : (g + 1) * hl, k * LANES : (k + 1) * LANES
                    ]

    def piece_in(k, h):
        rows = pl.ds(h * hx, hs)
        x = xs[0, rows, at(k, share)]
        for i, w in ((0, wg), (1, wu)):
            y = dot(x, w[at(k, share), :])
            acc[i, rows, :] = y if k is tp else acc[i, rows, :] + y

    def left_in():
        unpack(0)
        for h in range(2):
            rows = pl.ds(h * hx + hs, hl)
            x = xs[0, rows, :]
            acc[0, rows, :] = dot(x, wg[...])
            acc[1, rows, :] = dot(x, wu[...])

    def piece_gr(k, h):
        rows = pl.ds(h * hx, hs)
        y = dot_t(xs[1, rows, at(k, share)], wd[:, at(k, share)])
        acc[2, rows, :] = y if k is tp else acc[2, rows, :] + y

    def left_gr():
        unpack(1)
        for h in range(2):
            rows = pl.ds(h * hx + hs, hl)
            acc[2, rows, :] = dot_t(xs[1, rows, :], wd[...])

    rings = [
        [
            ring_copies(
                lambda sub, k, a=a, h=h: xs.at[
                    a, pl.ds(h * hx + sub * (hs // 2), hs // 2), at(k, share)
                ],
                g_send.at[a, h], g_recv.at[a, h],
            )
            for h in range(2)
        ]
        for a in range(2)
    ]

    def wait_arrivals(a, h):
        for inside in range(2):

            @pl.when((me // (n_sp // 2) == h) == (inside == 1))
            def _():
                ref = xs.at[a, pl.ds(h * hx, hs - inside * MAIN), at(tp, share)]
                pltpu.make_async_copy(ref, ref, a_recv.at[a, h]).wait()

    def ring_begin(ring):
        for i in (0, 3, 1, 2):
            ring[i].start()

    def ring_relay(ring):
        ring[0].wait_recv()
        ring[4].start()
        ring[3].wait_recv()
        ring[5].start()

    def begin(a, h):
        wait_arrivals(a, h)
        ring_begin(rings[a][h])

    def near_pieces(a, h):
        rings[a][h][1].wait_recv()
        (piece_in, piece_gr)[a](prv, h)
        rings[a][h][2].wait_recv()
        (piece_in, piece_gr)[a](nxt, h)

    def far_piece(a, h):
        rings[a][h][4].wait_recv()
        rings[a][h][5].wait_recv()
        (piece_in, piece_gr)[a](far, h)

    step = 2 * MAIN

    def forward_half(h):
        @pl.loop(0, hx // step)
        def _(i):
            rows = pl.ds(pl.multiple_of(h * hx + i * step, step), step)
            gate, up = acc[0, rows, :], acc[1, rows, :]
            clamped = jnp.minimum(gate, clamp_limit)
            logistic = 1.0 / (1.0 + jnp.exp(-sigmoid_sharpness * clamped))
            linear = jnp.clip(up, -clamp_limit, clamp_limit) + 1.0
            swish = clamped * logistic
            half_out[rows, :] = (swish * linear).astype(BF)
            slope = logistic + sigmoid_sharpness * swish * (1.0 - logistic)
            acc[0, rows, :] = jnp.where(gate < clamp_limit, linear * slope, 0.0)
            acc[1, rows, :] = jnp.where(jnp.abs(up) < clamp_limit, swish, 0.0)

    def backward_half(h):
        @pl.loop(0, hx // step)
        def _(i):
            rows = pl.ds(pl.multiple_of(h * hx + i * step, step), step)
            act_grad = acc[2, rows, :]
            gg_out[rows, :] = (act_grad * acc[0, rows, :]).astype(BF)
            ug_out[rows, :] = (act_grad * acc[1, rows, :]).astype(BF)

    def expert_part(k, slot, h):
        rows = pl.ds(h * hx, hx)
        y = dot_t(gg_out[rows, :], wg[at(k, share), :])
        y = y + dot_t(ug_out[rows, :], wu[at(k, share), :])
        ip[slot, rows, :] = y.astype(BF)

    def sums(h):
        subs = [pl.ds(h * hx + sub * (hx // 2), hx // 2) for sub in range(2)]

        def rs_copy(src, dst, i, k):
            return tp_copy(src, dst, rs_send.at[h], rs_recv.at[h], i, k)

        return subs, [
            rs_copy(ip.at[0, subs[0]], far_in.at[h, 0], 0, nxt),
            rs_copy(ip.at[0, subs[1]], far_in.at[h, 1], 1, prv),
            rs_copy(ip.at[1, subs[1]], near_in.at[0, subs[1]], 2, nxt),
            rs_copy(ip.at[2, subs[0]], near_in.at[1, subs[0]], 3, prv),
            rs_copy(ip.at[1, subs[0]], near_in.at[0, subs[0]], 4, nxt),
            rs_copy(ip.at[2, subs[1]], near_in.at[1, subs[1]], 5, prv),
        ]

    reduces = [sums(h) for h in range(2)]

    def parts(h):
        for slot, k in enumerate((far, nxt, prv)):
            expert_part(k, slot, h)

    def send_parts(h):
        for copy in reduces[h][1][:4]:
            copy.start()

    def augment(h):
        subs, rs = reduces[h]
        for i in range(2):
            rs[i].wait_recv()
            ip[1 + i, subs[i], :] = (
                ip[1 + i, subs[i], :].astype(F32) + far_in[h, i].astype(F32)
            ).astype(BF)
            rs[4 + i].start()

    def finish(h):
        for i in range(2, 6):
            reduces[h][1][i].wait_recv()
        rows = pl.ds(h * hx, hx)
        total = (
            ip[3, rows, :].astype(F32)
            + near_in[0, rows, :].astype(F32)
            + near_in[1, rows, :].astype(F32)
        ).astype(BF)
        ret_t[h * hs : (h + 1) * hs, :share] = total[:hs]
        stacked = jnp.concatenate(
            [total[hs:, g * LANES : (g + 1) * LANES] for g in range(groups)], axis=0
        )
        ret_t[h * hs : (h + 1) * hs, share:] = dot(pick, stacked).astype(BF)

        def give_back(i, carry):
            s = h * (n_sp // 2) + lax.rem(me + i, n_sp // 2)

            @pl.when(s != me)
            def _():
                pltpu.make_async_remote_copy(
                    src_ref=ret_t.at[slab(s), :],
                    dst_ref=ret_q.at[slab(me), :],
                    send_sem=t_send.at[0],
                    recv_sem=t_recv.at[0],
                    device_id={"sp": s},
                    device_id_type=MESH_ID,
                ).start()

            return carry

        lax.fori_loop(0, n_sp // 2, give_back, 0)

    begin(0, 0)
    loads[0].wait()
    loads[1].wait()
    piece_in(tp, 0)
    ring_relay(rings[0][0])
    begin(1, 0)
    loads[2].wait()
    piece_gr(tp, 0)
    near_pieces(0, 0)
    ring_relay(rings[1][0])
    begin(0, 1)
    far_piece(0, 0)
    piece_in(tp, 1)
    left_in()
    forward_half(0)
    ring_relay(rings[0][1])
    begin(1, 1)
    near_pieces(1, 0)
    left_gr()
    far_piece(1, 0)
    backward_half(0)
    parts(0)
    ring_relay(rings[1][1])
    send_parts(0)
    piece_gr(tp, 1)
    near_pieces(0, 1)
    far_piece(0, 1)
    forward_half(1)
    expert_part(tp, 3, 0)
    near_pieces(1, 1)
    far_piece(1, 1)
    backward_half(1)
    parts(1)
    augment(0)
    send_parts(1)
    expert_part(tp, 3, 1)

    @pl.loop(0, hidden // LANES)
    def _(i):
        act_out[at(i, LANES), :] = half_out[:, at(i, LANES)].T

    finish(0)

    @pl.loop(0, n_tp * groups)
    def _(i):
        xt_out[at(i, LANES), :] = xs[0, :, at(i, LANES)].T

    augment(1)
    saves = [
        pltpu.make_async_copy(src, dst, o_sem.at[i])
        for i, (src, dst) in enumerate(
            ((xt_out, xt_h), (xs.at[1], c_h), (gg_out, gg_h), (ug_out, ug_h), (act_out, act_h))
        )
    ]
    for save in saves:
        save.start()
    finish(1)
    ret_q[slab(me), :] = ret_t[slab(me), :]
    others = pl.ds(0, (n_sp - 1) * MAIN)
    pltpu.make_async_copy(ret_q.at[others, :], ret_q.at[others, :], t_recv.at[0]).wait()

    p_left = pl_ref[...]
    y = t_dot(pm_ref[...], ret_q[:, :share])
    back = ret_q[:, share:]
    group = (iota(p_left.shape, 0) % MAIN) // LEFT
    y = y + jnp.concatenate(
        [t_dot(jnp.where(group == g, p_left, jnp.zeros_like(p_left)), back) for g in range(groups)],
        axis=1,
    )
    res[:, at(tp, share)] = (cq[...].astype(F32) + y).astype(BF)
    ring = ring_copies(
        lambda h, k: res.at[pl.ds(h * (toks // 2), toks // 2), at(k, share)], r_send, r_recv
    )
    ring_begin(ring)
    block = share // (2 * pairs)
    plane = pairs * block
    partner = me + 1 - 2 * core

    def sp_copy(src, dst, send_sem, recv_sem, e):
        return pltpu.make_async_remote_copy(
            src_ref=src, dst_ref=dst, send_sem=send_sem, recv_sem=recv_sem,
            device_id={"sp": e}, device_id_type=MESH_ID,
        )

    order = (tp, prv, nxt, far)

    def plane_rows(k):
        return pl.ds(pl.multiple_of(k * plane, plane), plane)

    swaps = [
        sp_copy(
            part.at[1 - core, plane_rows(k), :], peer.at[plane_rows(k), :],
            d_send.at[i], d_recv.at[i], partner,
        )
        for i, k in enumerate(order)
    ]

    def piece_mix(i):
        k = order[i]
        y = dot(res[:, at(k, share)], ow[at(k, share), :])
        gm[...] = y if i == 0 else gm[...] + y

    def piece_out(i):
        k = order[i]
        r = res[:, at(k, share)]
        for j in range(pairs):
            g = t_dot(r[:, j * LANES : (j + 1) * LANES], mix[...]).astype(BF)
            for c in range(2):
                part[c, pl.ds(pl.multiple_of(k * plane + j * block, block), block), :] = g[
                    c * block : (c + 1) * block
                ]
        swaps[i].start()

    def piece_res(i):
        piece_out(i)
        piece_mix(i)

    my_block = me // 2

    def send_plane(i):
        k = order[i]
        swaps[i].wait_recv()
        rows = plane_rows(k)
        part[core, rows, :] = (
            part[core, rows, :].astype(F32) + peer[rows, :].astype(F32)
        ).astype(BF)
        for j in range(4):
            zy = k * 4 + lax.rem(y_at + j, 4)

            @pl.when(zy != my_block)
            def _():
                sp_copy(
                    part.at[core, pl.ds(pl.multiple_of(zy * block, block), block), :],
                    got.at[my_block], b_send.at[0], b_recv.at[0], zy * 2 + core,
                ).start()

    loads[3].wait()
    piece_res(0)
    ring_relay(ring)
    ring[1].wait_recv()
    piece_res(1)
    send_plane(0)
    ring[2].wait_recv()
    piece_res(2)
    send_plane(1)
    ring[4].wait_recv()
    ring[5].wait_recv()
    piece_mix(3)
    gmb[...] = gm[...].astype(BF)

    half = LANES // 2

    @pl.loop(0, 2 * pairs)
    def _(i):
        rows, cols, b, p = spot(i)
        q = (qkv[0, rows, cols].astype(F32) * jnp.exp(cum[rows, cols])).astype(BF)
        o = t_dot(q, gmb[rows, cols])
        outer[b, p] = jnp.where(low_lane, o[:half], o[half:])

    def pair_rows(tile):
        return tile[:pairs][:, None, :]

    block_factor = [jnp.exp(by_pair(e))[:, None, :] for e in ends]
    total = block_factor[0] * outer[1] + outer[0]
    local[0] = total.astype(BF)
    swap_state = sp_copy(local.at[0], cbuf, sc_send.at[0], sc_recv.at[0], partner)
    swap_state.start()
    piece_out(3)
    tiles = pl.ds(0, n_sp - 1)
    pltpu.make_async_copy(logs.at[tiles], logs.at[tiles], lt_recv.at[0]).wait()

    def chip_log(z, y):
        return logs[z * 8 + y * 2] + logs[z * 8 + y * 2 + 1]

    later_core_log = logs[me - core + 1]
    earlier_core_log = logs[me - core]

    swap_state.wait_recv()
    mine, others_total = local[0].astype(F32), cbuf[...].astype(F32)
    early = jnp.where(core == 0, mine, others_total)
    late = jnp.where(core == 0, others_total, mine)
    chip_total = jnp.exp(pair_rows(earlier_core_log)) * late + early
    ybuf[y_at] = chip_total.astype(BF)
    y_sends = [
        sp_copy(
            ybuf.at[y_at], ybuf.at[y_at], sy_send.at[i - 1], sy_recv.at[i - 1],
            z_at * 8 + lax.rem(y_at + i, 4) * 2 + core,
        )
        for i in range(1, 4)
    ]
    for copy in y_sends:
        copy.start()
    send_plane(2)

    send_plane(3)
    for copy in y_sends:
        copy.wait_recv()
    inside_y = jnp.zeros_like(total)
    plane_total = jnp.zeros_like(total)
    later_y = jnp.zeros((2 * pairs, LANES), F32)
    for y in (3, 2, 1, 0):
        log = chip_log(z_at, y)
        factor = jnp.exp(pair_rows(log))
        t = ybuf[y].astype(F32)
        inside_y = jnp.where(y > y_at, factor * inside_y + t, inside_y)
        later_y = jnp.where(y > y_at, later_y + log, later_y)
        plane_total = factor * plane_total + t
    local[1] = plane_total.astype(BF)
    z_sends = [
        sp_copy(local.at[1], zbuf.at[i - 1], sz_send.at[i - 1], sz_recv.at[i - 1], me - i * 8)
        for i in range(1, 4)
    ]
    for i, copy in enumerate(z_sends, 1):

        @pl.when(z_at >= i)
        def _():
            copy.start()

    @pl.loop(0, 2 * pairs)
    def _(i):
        rows, cols, b, p = spot(i)
        q, k, v, g = qkv[0, rows, cols], qkv[1, rows, cols], qkv[2, rows, cols], gmb[rows, cols]
        outs = []
        for hh in range(2):
            wg_ts = (dot_t(g, side(v, hh)) * decay[i * 2 + hh]).astype(BF)
            outs.append((dot(wg_ts, k), t_dot(wg_ts, q), t_dot(score[i * 2 + hh], g)))
        intra = [jnp.where(low_lane, lo, hi) for lo, hi in zip(*outs)]
        st = [st_ref[b, 2 * p + hh] for hh in range(2)]
        none = jnp.zeros_like(st[0])
        full = jnp.concatenate(
            [
                jnp.concatenate([st[0], none], axis=1),
                jnp.concatenate([none, st[1]], axis=1),
            ],
            axis=0,
        )
        carry = dot_t(g, full) * jnp.exp(cum[rows, cols])
        gq_out[rows, cols] = (intra[0] + carry).astype(BF)
        gm[rows, cols] = intra[1]
        acc[0, rows, cols] = intra[2]

    beyond = jnp.zeros_like(total)
    local_state = acc.at[1, pl.ds(0, pairs * half), pl.ds(0, LANES)]
    local_state[...] = jnp.zeros((pairs * half, LANES), F32)
    for i in (3, 2, 1):

        @pl.when(z_at + i < 4)
        def _():
            z_sends[i - 1].wait_recv()
            log = sum(chip_log(z_at + i, y) for y in range(4))
            now = local_state[...].reshape(pairs, half, LANES)
            now = jnp.exp(pair_rows(log)) * now + zbuf[i - 1].astype(F32)
            local_state[...] = now.reshape(pairs * half, LANES)

    beyond = local_state[...].reshape(pairs, half, LANES)
    entering_state = jnp.exp(pair_rows(later_y)) * beyond + inside_y
    entering_state = jnp.where(
        core == 0, jnp.exp(pair_rows(later_core_log)) * entering_state + late, entering_state
    )
    carried = (block_factor[1] * entering_state + outer[1], entering_state)
    for b in range(2):
        outer[b] = carried[b]

    @pl.loop(0, 2 * pairs)
    def _(i):
        rows, cols, b, p = spot(i)
        k, v = qkv[1, rows, cols], qkv[2, rows, cols]
        st = outer[b, p].astype(BF)
        full = jnp.concatenate([side(st, 0), side(st, 1)], axis=0)
        c = cum[rows, cols]
        to_end = jnp.exp(c[blk - 1 : blk, :] - c)
        gk_out[rows, cols] = (gm[rows, cols] + dot_t(v, full) * to_end).astype(BF)
        gv_out[rows, cols] = (acc[0, rows, cols] + dot(k, full) * to_end).astype(BF)

    blocks = pl.ds(0, 15)
    pltpu.make_async_copy(got.at[blocks], got.at[blocks], b_recv.at[0]).wait()
    got[my_block] = part[core, pl.ds(pl.multiple_of(my_block * block, block), block), :]
    sums = got[0].astype(F32)
    for i in range(1, 16):
        sums = sums + got[i].astype(F32)
    go_out[...] = sums

    pltpu.make_async_copy(got.at[blocks], got.at[blocks], b_send.at[0]).wait()
    pltpu.make_async_copy(logs.at[tiles], logs.at[tiles], lt_send.at[0]).wait()
    for copy in swaps + [swap_state] + y_sends:
        copy.wait_send()
    for i, copy in enumerate(z_sends, 1):

        @pl.when(z_at >= i)
        def _():
            copy.wait_send()

    for a in range(2):
        for ref, sem in ((sent.at[a, others, :], a_send), (sent_left.at[a, others, :], l_send)):
            pltpu.make_async_copy(ref, ref, sem.at[a]).wait()
        for copy in rings[a][0] + rings[a][1]:
            copy.wait_send()
    for copy in reduces[0][1] + reduces[1][1] + ring:
        copy.wait_send()
    for save in saves:
        save.wait()
    pltpu.make_async_copy(ret_q.at[others, :], ret_q.at[others, :], t_send.at[0]).wait()


def expert_call(
    routes, weights, x, cotangent, log_decay, states, w_gate, w_up, w_down, w_out, mixer,
    queries, key_vectors, value_vectors,
):
    n_sp, n_tp = lax.axis_size("sp"), lax.axis_size("tp")
    width, hidden = w_gate.shape
    share = width // n_tp
    wide = share + LANES
    rows = n_sp * MAIN
    full = n_sp * (MAIN + LEFT)
    toks = cotangent.shape[0]
    anyspace = pl.BlockSpec(memory_space=pl.ANY)
    vmem = pl.BlockSpec(memory_space=pltpu.VMEM)
    dma = pltpu.SemaphoreType.DMA
    return pl.pallas_call(
        expert_kernel,
        out_shape=(
            jax.ShapeDtypeStruct((width, full), BF),
            jax.ShapeDtypeStruct((full, width), BF),
            jax.ShapeDtypeStruct((full, hidden), BF),
            jax.ShapeDtypeStruct((full, hidden), BF),
            jax.ShapeDtypeStruct((hidden, full), BF),
            jax.ShapeDtypeStruct((width // n_sp, share), F32),
            jax.ShapeDtypeStruct((toks, share), BF),
            jax.ShapeDtypeStruct((toks, share), BF),
            jax.ShapeDtypeStruct((toks, share), BF),
        ),
        in_specs=[anyspace] * 14,
        out_specs=[anyspace] * 5 + [vmem] * 4,
        scratch_shapes=[
            pltpu.VMEM((width, full), BF),
            pltpu.VMEM((hidden, full), BF),
            pltpu.VMEM((full, hidden), BF),
            pltpu.VMEM((full, hidden), BF),
            dma((5,)),
            pltpu.VMEM((2, rows, n_tp * LANES), BF),
            pltpu.VMEM((2, full, width), BF),
            pltpu.VMEM(w_gate.shape, BF),
            pltpu.VMEM(w_up.shape, BF),
            pltpu.VMEM(w_down.shape, BF),
            pltpu.VMEM((3, full, hidden), F32),
            pltpu.VMEM((full, hidden), BF),
            pltpu.VMEM((4, full, share), BF),
            pltpu.VMEM((2, 2, full // 4, share), BF),
            pltpu.VMEM((2, full, share), BF),
            pltpu.VMEM((rows, wide), BF),
            pltpu.VMEM((rows, wide), BF),
            pltpu.VMEM((toks, width), BF),
            dma((8,)), dma((2,)), dma((2, 2)), dma((2,)), dma((2,)), dma((2, 2, 6)), dma((2, 2, 6)),
            dma((2, 6)), dma((2, 6)), dma((1,)), dma((1,)), dma((6,)), dma((6,)),
            pltpu.VMEM(w_out.shape, BF),
            pltpu.VMEM(mixer.shape, BF),
            pltpu.VMEM((3, toks, share), BF),
            pltpu.VMEM((toks, share), F32),
            pltpu.VMEM((2 * log_decay.shape[0], toks // 2), F32),
            pltpu.VMEM((16, toks // 2, toks // 2), F32),
            pltpu.VMEM((16, toks // 2, toks // 2), BF),
            pltpu.VMEM((n_sp, 8, LANES), F32),
            pltpu.VMEM((toks, share), F32),
            pltpu.VMEM((toks, share), BF),
            pltpu.VMEM((2, 4, 64, LANES), F32),
            pltpu.VMEM((2, 4, 64, LANES), BF),
            pltpu.VMEM((2, width // 2, share), BF),
            pltpu.VMEM((width // 2, share), BF),
            pltpu.VMEM((16, width // n_sp, share), BF),
            pltpu.VMEM((4, 4, 64, LANES), BF),
            pltpu.VMEM((3, 4, 64, LANES), BF),
            dma((1,)), dma((1,)), dma((4,)), dma((4,)), dma((1,)), dma((1,)), dma((1,)),
            dma((1,)), dma((3,)), dma((3,)), dma((3,)), dma((3,)),
            pltpu.VMEM((4, 64, LANES), BF),
            pltpu.VMEM(routes.shape, jnp.int32),
            pltpu.VMEM(weights.shape, F32),
            pltpu.VMEM((toks, share), BF),
            pltpu.VMEM((toks, share), BF),
            pltpu.VMEM(log_decay.shape, F32),
            pltpu.VMEM(states.shape, BF),
            pltpu.VMEM((2, rows, share), BF),
            pltpu.VMEM((2, rows, n_tp * LANES), BF),
            pltpu.VMEM((2, MAIN // LEFT * toks, n_tp * LANES), BF),
            pltpu.VMEM((rows, toks), BF),
            pltpu.VMEM((rows, toks), BF),
            dma((6,)),
            dma((2, 16)),
        ],
        compiler_params=pltpu.CompilerParams(
            collective_id=0, has_side_effects=True, vmem_limit_bytes=62 << 20
        ),
        cost_estimate=pl.CostEstimate(flops=10**10, bytes_accessed=20 << 20, transcendentals=0),
        name="experts",
    )(
        routes, weights, x, cotangent, log_decay, states, w_gate, w_up, w_down, w_out, mixer,
        queries, key_vectors, value_vectors,
    )


def weight_kernel(
    xt, c, gg, ug, act, go, gq, gk, gv, gate_out, up_out, down_out, go_out, gq_out, gk_out, gv_out
):
    gate_out[...] = dot(xt[...], gg[...])
    up_out[...] = dot(xt[...], ug[...])
    down_out[...] = dot(act[...], c[...])
    go_out[...] = go[...]
    gq_out[...] = gq[...]
    gk_out[...] = gk[...]
    gv_out[...] = gv[...]


def weight_call(xt, c, gg, ug, act, go, gq, gk, gv, steps):
    width, rows = xt.shape
    hidden = gg.shape[1]
    tile = width // steps
    slice_in = pl.BlockSpec((rows, tile), lambda i: (0, i))
    slice_x = pl.BlockSpec((tile, rows), lambda i: (i, 0))
    whole = pl.BlockSpec((rows, hidden), lambda i: (0, 0))
    whole_t = pl.BlockSpec((hidden, rows), lambda i: (0, 0))
    tall = pl.BlockSpec((tile, hidden), lambda i: (i, 0))

    def banded(v):
        return pl.BlockSpec((v.shape[0] // steps, v.shape[1]), lambda i: (i, 0))

    small = [banded(v) for v in (go, gq, gk, gv)]
    return pl.pallas_call(
        weight_kernel,
        grid=(steps,),
        out_shape=(
            jax.ShapeDtypeStruct((width, hidden), F32),
            jax.ShapeDtypeStruct((width, hidden), F32),
            jax.ShapeDtypeStruct((hidden, width), F32),
        )
        + tuple(jax.ShapeDtypeStruct(v.shape, v.dtype) for v in (go, gq, gk, gv)),
        in_specs=[slice_x, slice_in, whole, whole, whole_t] + small,
        out_specs=[tall, tall, pl.BlockSpec((hidden, tile), lambda i: (0, i))] + small,
        compiler_params=pltpu.CompilerParams(vmem_limit_bytes=62 << 20),
        name="weights",
    )(xt, c, gg, ug, act, go, gq, gk, gv)


def shards(
    moe_input,
    cotangent,
    routes,
    route_weights,
    gate_weight,
    up_weight,
    down_weight,
    out_weight,
    mixer_output,
    queries,
    key_vectors,
    value_vectors,
    log_decay,
    block_states,
):
    outs = expert_call(
        routes.T, route_weights.T, moe_input, cotangent, log_decay.T, block_states,
        gate_weight[0], up_weight[0], down_weight[0], out_weight, mixer_output,
        queries, key_vectors, value_vectors,
    )
    grads = weight_call(*outs, steps=WEIGHT_STEPS)
    return tuple(g[None] for g in grads[:3]) + tuple(grads[3:])


def solution(mesh):
    return jax.shard_map(
        shards,
        mesh=mesh,
        in_specs=(
            P(SP, None),
            P(SP, None),
            P(SP, None),
            P(SP, None),
            P(SP, None, "tp"),
            P(SP, None, "tp"),
            P(SP, "tp", None),
            P(None, "tp"),
            P(SP, "tp"),
            P(SP, "tp"),
            P(SP, "tp"),
            P(SP, "tp"),
            P(SP, "tp"),
            P(SP, "tp", None, None),
        ),
        out_specs=(
            P(SP, None, "tp"),
            P(SP, None, "tp"),
            P(SP, "tp", None),
            P(SP, "tp"),
            P(SP, "tp"),
            P(SP, "tp"),
            P(SP, "tp"),
        ),
        check_vma=False,
    )
```
